128 devices in a mesh: sp: 16 (over z, x), tp: 8 (over y, core).
Axes of the slice: x: 4, y: 4, z: 4, core: 2. Of those that a mesh axis runs over, the one named last changes fastest.
Arguments:
- latent: bfloat16 [8192, 4096], P('sp'), may hold values from -64 to 64
- context: bfloat16 [1024, 4096], P('sp'), may hold values from -6 to 6
- condition: bfloat16 [4096], P('sp'), may hold values from -6 to 6
- context_condition: bfloat16 [4096], P('sp'), may hold values from -6 to 6
- shift_weight: bfloat16 [4096, 4096], P('sp', 'tp'), may hold values from -0.125 to 0.125
- scale_weight: bfloat16 [4096, 4096], P('sp', 'tp'), may hold values from -0.125 to 0.125
- gate_weight: bfloat16 [4096, 4096], P('sp', 'tp'), may hold values from -0.25 to 0.25
- norm_gain: float32 [4096], replicated, may hold values from 0.1 to 1.9
- query_weight: bfloat16 [4096, 2048], P(None, 'tp'), may hold values from -0.09375 to 0.09375
- key_weight: bfloat16 [4096, 2048], P(None, 'tp'), may hold values from -0.09375 to 0.09375
- value_weight: bfloat16 [4096, 2048], P(None, 'tp'), may hold values from -0.09375 to 0.09375
- write_weight: bfloat16 [4096, 2, 16], replicated, may hold values from -0.09375 to 0.09375
- decay_weight: bfloat16 [4096, 2, 16], replicated, may hold values from -0.09375 to 0.09375
- write_bias: float32 [2, 16], replicated, may hold values from -12 to 1
- decay_bias: float32 [2, 16], replicated, may hold values from -16 to -4
- log_rate: float32 [2, 16], replicated, may hold values from 0 to 1.4
- head_gain: float32 [128], replicated, may hold values from 0.1 to 1.9
- out_weight: bfloat16 [2048, 4096], P(None, 'tp'), may hold values from -0.125 to 0.125
Outputs:
- updated: bfloat16 [8192, 4096], P('sp', 'tp')
The draws below stay inside these ranges and needn't reach their ends.
All inputs are finite; a program needn't handle non-finite values.
Results may differ from the reference program's by a relative error of at most 0.013.
Values may be sent and summed in bfloat16 or wider, within the bound.
A program may use at most 128 MiB of HBM per device.

```python
import math
import jax
import jax.numpy as jnp
from jax import lax

D = 4096
HEADS = 16
HEAD_DIM = 128
BLOCK = 64
TOKENS = 8192
CTX = 1024


def draw_latent(key, part):
    segment_count = (TOKENS + 127) // 128
    offsets = jnp.clip(jax.random.normal(jax.random.fold_in(key, 22), (segment_count, D), jnp.float32), -3.0, 3.0)
    segment_index = jnp.arange(TOKENS) // 128
    noise = jnp.clip(jax.random.normal(jax.random.fold_in(key, 21), (TOKENS, D), jnp.float32), -6.0, 6.0)
    return (noise + offsets[segment_index]).astype(jnp.bfloat16)


def head_speeds(key):
    chooser = jax.random.uniform(jax.random.fold_in(key, 31), (2, HEADS), jnp.float32)
    return chooser < 0.7


def draw_decay_bias(key, part):
    keeping = head_speeds(key)
    spread = jax.random.uniform(jax.random.fold_in(key, 32), (2, HEADS), jnp.float32, -0.5, 0.5)
    slow_value = math.log(0.05 / (TOKENS + CTX)) + spread
    fast_value = -5.0 + spread
    return jnp.where(keeping, slow_value, fast_value).astype(jnp.float32)


def draw_write_bias(key, part):
    keeping = head_speeds(key)
    spread = jax.random.uniform(jax.random.fold_in(key, 33), (2, HEADS), jnp.float32, -0.5, 0.5)
    slow_value = math.log(HEAD_DIM / (TOKENS + CTX)) - 1.5 + spread
    fast_value = spread
    return jnp.where(keeping, slow_value, fast_value).astype(jnp.float32)


def block_levels(rng, shape, cuts, least, high):
    level = 1.0
    for position, blocks in cuts:
        draws = jax.random.uniform(jax.random.fold_in(jax.random.fold_in(rng, 6), position), (blocks,), jnp.float32, least / len(cuts), high / len(cuts))
        level = level * jnp.repeat(jnp.exp(draws), shape[position] // blocks).reshape((-1,) + (1,) * (len(shape) - 1 - position))
    return level


def gaussian(key, extent, scale, most, split=(), held_as=jnp.bfloat16):
    drawn = jax.random.normal(key, extent, jnp.float32) * scale
    if len(split) > 0:
        drawn = block_levels(key, extent, split, -0.22, 0.18) * drawn
    return jnp.clip(drawn, min=-most, max=most).astype(held_as)


def setup_inputs(seed: int = 0) -> dict:
    keys = jax.random.split(jax.random.key(seed), 19)
    return {
        "latent": draw_latent(jax.random.fold_in(keys[18], 71), 0),
        "context": gaussian(keys[1], (CTX, D), 1.0, 6.0, ((0, 16),)),
        "condition": gaussian(keys[2], (D,), 1.0, 6.0, ((0, 16),)),
        "context_condition": gaussian(keys[3], (D,), 1.0, 6.0, ((0, 16),)),
        "shift_weight": gaussian(keys[4], (D, D), (D // 2) ** -0.5, 0.125, ((0, 16), (1, 8))),
        "scale_weight": gaussian(keys[5], (D, D), (D // 2) ** -0.5, 0.125, ((0, 16), (1, 8))),
        "gate_weight": gaussian(keys[6], (D, D), (D // 8) ** -0.5, 0.25, ((0, 16), (1, 8))),
        "norm_gain": jnp.clip(1.0 + 0.18 * jax.random.normal(keys[7], (D,), jnp.float32), 0.1, 1.9),
        "query_weight": gaussian(keys[8], (D, HEADS * HEAD_DIM), D ** -0.5, 0.09375, ((1, 8),)),
        "key_weight": gaussian(keys[9], (D, HEADS * HEAD_DIM), D ** -0.5, 0.09375, ((1, 8),)),
        "value_weight": gaussian(keys[10], (D, HEADS * HEAD_DIM), D ** -0.5, 0.09375, ((1, 8),)),
        "write_weight": gaussian(keys[11], (D, 2, HEADS), D ** -0.5, 0.09375),
        "decay_weight": gaussian(keys[12], (D, 2, HEADS), D ** -0.5, 0.09375),
        "write_bias": draw_write_bias(jax.random.fold_in(keys[18], 71), 0),
        "decay_bias": draw_decay_bias(jax.random.fold_in(keys[18], 71), 0),
        "log_rate": jnp.clip(jax.random.uniform(keys[15], (2, HEADS), jnp.float32, 0.0, 1.4), 0.0, 1.4),
        "head_gain": jnp.clip(1.0 + 0.18 * jax.random.normal(keys[16], (HEAD_DIM,), jnp.float32), 0.1, 1.9),
        "out_weight": gaussian(keys[17], (HEADS * HEAD_DIM, D), (HEADS * HEAD_DIM) ** -0.5, 0.125, ((1, 8),)),
    }


epsilon = 0.0001
highest = lax.Precision.HIGHEST

def rms_rows(row_data, row_gain):
    values = row_data.astype(jnp.float32)
    scaled = values * lax.rsqrt(lax.optimization_barrier(jnp.mean(values * values, axis=-1, keepdims=True)) + epsilon)
    return scaled * row_gain.astype(jnp.float32)

def unit_heads(matrix, head_count):
    split_heads = matrix.astype(jnp.float32).reshape(matrix.shape[0], head_count, -1)
    return split_heads * lax.rsqrt(lax.optimization_barrier(jnp.sum(split_heads * split_heads, axis=-1, keepdims=True)) + epsilon)

def head_gates(write_pre, decay_pre, write_bias, decay_bias, log_rate):
    write_rate = jax.nn.sigmoid(write_pre.astype(jnp.float32) + write_bias)
    log_decay = -jnp.exp(log_rate) * jax.nn.softplus(decay_pre.astype(jnp.float32) + decay_bias)
    return (write_rate, log_decay)

def project(matrix, weight):
    return jnp.dot(matrix.astype(jnp.float32), weight.astype(jnp.float32), preferred_element_type=jnp.float32).astype(jnp.bfloat16)

def to_blocks(source):
    heads_first = jnp.moveaxis(source, 1, 0)
    block_count = heads_first.shape[1] // BLOCK
    return heads_first.reshape((heads_first.shape[0], block_count, BLOCK) + heads_first.shape[2:])

def prepare_keys(key_vecs, value_vecs, log_decay, write_rate):
    block_keys = to_blocks(key_vecs)
    block_values = to_blocks(value_vecs)
    running = jnp.cumsum(to_blocks(log_decay), axis=-1)
    block_rates = to_blocks(write_rate)
    offsets = jnp.arange(BLOCK)
    lower_mask = offsets[:, None] >= offsets[None, :]
    strict_mask = offsets[:, None] > offsets[None, :]
    spread = running[..., :, None] - running[..., None, :]
    decay_mat = jnp.where(lower_mask, jnp.exp(jnp.where(lower_mask, spread, 0.0)), 0.0)
    scaled = block_keys * block_rates[..., None]
    system = jnp.einsum('hnid,hnjd->hnij', scaled, block_keys, precision=highest) * decay_mat
    system = jnp.where(strict_mask, system, 0.0) + jnp.eye(BLOCK, dtype=system.dtype)
    fresh_values = jax.scipy.linalg.solve_triangular(system, block_values * block_rates[..., None], lower=True, unit_diagonal=True)
    key_weights = jax.scipy.linalg.solve_triangular(system, scaled * jnp.exp(running)[..., None], lower=True, unit_diagonal=True)
    last_gate = running[..., -1]
    late_keys = block_keys * jnp.exp(last_gate[..., None] - running)[..., None]
    return (block_keys, running, decay_mat, fresh_values, key_weights, last_gate, late_keys)

def prepare_queries(query_vecs, prepared):
    block_queries = to_blocks(query_vecs)
    query_keys = jnp.einsum('hnid,hnjd->hnij', block_queries, prepared[0], precision=highest) * prepared[2]
    early_queries = block_queries * jnp.exp(prepared[1])[..., None]
    return (query_keys, early_queries)

def run_blocks(prepared, queried, start):
    inputs = tuple((jnp.moveaxis(item, 1, 0) for item in (prepared[3], prepared[4], queried[0], queried[1], prepared[6], prepared[5])))

    def advance(carried, pieces):
        new_in, key_in, score_in, query_in, late_in, gate_in = pieces
        corrected = new_in - jnp.einsum('hcd,hde->hce', key_in, carried, precision=highest)
        output = jnp.einsum('hcd,hde->hce', query_in, carried, precision=highest)
        output = output + jnp.einsum('hij,hje->hie', score_in, corrected, precision=highest)
        carried = carried * jnp.exp(gate_in)[:, None, None] + jnp.einsum('hcd,hce->hde', late_in, corrected, precision=highest)
        return (carried, output)
    closing, outputs = lax.scan(advance, start, inputs)
    merged = jnp.transpose(outputs, (0, 2, 1, 3))
    return merged.reshape(-1, merged.shape[2], merged.shape[3])

def final_state(prepared, start):
    inputs = tuple((jnp.moveaxis(item, 1, 0) for item in (prepared[3], prepared[4], prepared[6], prepared[5])))

    def advance(carried, pieces):
        new_in, key_in, late_in, gate_in = pieces
        corrected = new_in - jnp.einsum('hcd,hde->hce', key_in, carried, precision=highest)
        carried = carried * jnp.exp(gate_in)[:, None, None] + jnp.einsum('hcd,hce->hde', late_in, corrected, precision=highest)
        return (carried, None)
    closing, unused = lax.scan(advance, start, inputs)
    return closing

def reference(latent, context, condition, context_condition, shift_weight, scale_weight, gate_weight, norm_gain, query_weight, key_weight, value_weight, write_weight, decay_weight, write_bias, decay_bias, log_rate, head_gain, out_weight):
    head_count = write_bias.shape[1]
    width = write_weight.shape[0]
    stacked = jnp.stack([condition, context_condition]).astype(jnp.float32)
    silu_rows = jax.nn.silu(stacked).astype(jnp.bfloat16)
    shift_rows = jnp.dot(silu_rows.astype(jnp.float32), shift_weight.astype(jnp.float32), preferred_element_type=jnp.float32)
    scale_rows = jnp.dot(silu_rows.astype(jnp.float32), scale_weight.astype(jnp.float32), preferred_element_type=jnp.float32)
    gate_row = jnp.dot(silu_rows[0].astype(jnp.float32), gate_weight.astype(jnp.float32), preferred_element_type=jnp.float32)
    modulated = (rms_rows(latent, norm_gain) * (1.0 + scale_rows[0]) + shift_rows[0]).astype(jnp.bfloat16)
    ctx_modulated = (rms_rows(context, norm_gain) * (1.0 + scale_rows[1]) + shift_rows[1]).astype(jnp.bfloat16)
    write_flat = write_weight.reshape(width, -1)
    decay_flat = decay_weight.reshape(width, -1)
    ctx_keys = unit_heads(project(ctx_modulated, key_weight), head_count)
    ctx_values = project(ctx_modulated, value_weight).astype(jnp.float32).reshape(-1, head_count, HEAD_DIM)
    ctx_rate, ctx_log = head_gates(project(ctx_modulated, write_flat).reshape(-1, 2, head_count), project(ctx_modulated, decay_flat).reshape(-1, 2, head_count), write_bias, decay_bias, log_rate)
    start_zero = jnp.zeros((head_count, HEAD_DIM, HEAD_DIM), jnp.float32)
    ctx_forward = final_state(prepare_keys(ctx_keys, ctx_values, ctx_log[:, 0], ctx_rate[:, 0]), start_zero)
    ctx_backward = final_state(prepare_keys(jnp.flip(ctx_keys, 0), jnp.flip(ctx_values, 0), jnp.flip(ctx_log[:, 1], 0), jnp.flip(ctx_rate[:, 1], 0)), start_zero)
    queries = unit_heads(project(modulated, query_weight), head_count) * HEAD_DIM ** (-0.5)
    key_vecs = unit_heads(project(modulated, key_weight), head_count)
    value_vecs = project(modulated, value_weight).astype(jnp.float32).reshape(-1, head_count, HEAD_DIM)
    write_rate, log_decay = head_gates(project(modulated, write_flat).reshape(-1, 2, head_count), project(modulated, decay_flat).reshape(-1, 2, head_count), write_bias, decay_bias, log_rate)
    forward_prep = prepare_keys(key_vecs, value_vecs, log_decay[:, 0], write_rate[:, 0])
    forward_out = run_blocks(forward_prep, prepare_queries(queries, forward_prep), ctx_forward)
    backward_prep = prepare_keys(jnp.flip(key_vecs, 0), jnp.flip(value_vecs, 0), jnp.flip(log_decay[:, 1], 0), jnp.flip(write_rate[:, 1], 0))
    backward_out = jnp.flip(run_blocks(backward_prep, prepare_queries(jnp.flip(queries, 0), backward_prep), ctx_backward), 0)
    combined = forward_out + backward_out
    head_out = combined * lax.rsqrt(lax.optimization_barrier(jnp.mean(combined * combined, axis=-1, keepdims=True)) + epsilon) * head_gain.astype(jnp.float32)
    head_out = head_out.astype(jnp.bfloat16).reshape(combined.shape[0], -1)
    branch = jnp.dot(head_out.astype(jnp.float32), out_weight.astype(jnp.float32), preferred_element_type=jnp.float32)
    return (latent.astype(jnp.float32) + gate_row * branch).astype(jnp.bfloat16)
```

```python
import functools

import jax
import jax.numpy as jnp
from jax import lax
from jax.experimental import pallas as pl
from jax.experimental.pallas import tpu as pltpu
from jax.sharding import PartitionSpec as P

HEAD_DIM = 128
CHUNK = 128
epsilon = 0.0001
bf16 = jnp.bfloat16
f32 = jnp.float32


def mm(a, b):
    return jnp.dot(a.astype(bf16), b.astype(bf16), preferred_element_type=f32)


def mm_t(a, b):
    return lax.dot_general(a, b, (((1,), (1,)), ((), ())), preferred_element_type=f32)


def spans(tokens, ctx_tokens):
    size = min(CHUNK, tokens)
    lat = [(at, size) for at in range(0, tokens, size)]
    ctx_size = min(CHUNK, ctx_tokens)
    ctx = [(tokens + at, ctx_size) for at in range(0, ctx_tokens, ctx_size)]
    return lat, ctx


def iotas(size):
    rows = lax.broadcasted_iota(jnp.int32, (size, size), 0)
    cols = lax.broadcasted_iota(jnp.int32, (size, size), 1)
    return rows, cols


def prepare(groups):
    items = []
    for group in groups:
        size = group["size"]
        rows, cols = iotas(size)
        keys = group["k"]
        keys_t = keys.astype(f32).T
        gram = jnp.dot(keys, keys_t.astype(bf16), preferred_element_type=f32)
        diag = jnp.where(rows == cols, gram, 0.0)
        s_col = lax.rsqrt(jnp.sum(diag, axis=1, keepdims=True) + epsilon)
        s_row = lax.rsqrt(jnp.sum(diag, axis=0, keepdims=True) + epsilon)
        gram = gram * s_col * s_row
        group["keys"] = keys.astype(f32) * s_col
        group["keys_t"] = keys_t * s_row
        group["values"] = group["v"].astype(f32)
        if group["q"] is not None:
            queries = group["q"].astype(f32)
            q_scale = lax.rsqrt(jnp.sum(queries * queries, axis=1, keepdims=True) + epsilon) * HEAD_DIM**-0.5
            group["queries"] = queries * q_scale
            group["score"] = (
                jnp.dot(group["q"], keys_t.astype(bf16), preferred_element_type=f32) * q_scale * s_row
            )
        for d in range(2):
            rate_col, run_col, run_row = group["gates"][d]
            inside = rows >= cols if d == 0 else rows <= cols
            strict = rows > cols if d == 0 else rows < cols
            decay = jnp.where(inside, jnp.exp(jnp.minimum(run_col - run_row, 0.0)), 0.0)
            system = jnp.where(strict, gram * decay * rate_col, 0.0)
            item = dict(group=group, size=size, d=d, rate_col=rate_col, run_col=run_col, run_row=run_row)
            item["system"] = system
            if group["q"] is not None:
                item["score"] = group["score"] * decay
            near = (rows // 2) == (cols // 2)
            item["inv"] = jnp.where(rows == cols, 1.0, jnp.where(near, -system, 0.0))
            items.append(item)
    span = 2
    while span < max(item["size"] for item in items):
        firsts = []
        for item in items:
            if span >= item["size"]:
                firsts.append(None)
                continue
            rows, cols = iotas(item["size"])
            rows, cols = rows // span, cols // span
            if item["d"] == 0:
                mask = ((rows % 2) == 1) & (cols == rows - 1)
            else:
                mask = ((cols % 2) == 1) & (rows == cols - 1)
            firsts.append(mm(jnp.where(mask, item["system"], 0.0), item["inv"]))
        for item, first in zip(items, firsts):
            if first is not None:
                item["inv"] = item["inv"] - mm(item["inv"], first)
        span *= 2
    for item in items:
        group = item["group"]
        growth = jnp.exp(item["run_col"])
        both = jnp.concatenate(
            [group["values"] * item["rate_col"], group["keys"] * (item["rate_col"] * growth)], axis=1
        )
        item["solved"] = mm(item["inv"], both)
        last = item["run_row"][:, item["size"] - 1 :] if item["d"] == 0 else item["run_row"][:, :1]
        item["gate"] = jnp.exp(last)
        late_t = group["keys_t"] * jnp.exp(last - item["run_row"])
        item["late"] = mm(late_t, item["solved"])
        if group["q"] is not None:
            weighed = mm(item["score"], item["solved"])
            item["local"] = weighed[:, :HEAD_DIM]
            item["early"] = group["queries"] * growth - weighed[:, HEAD_DIM:]
    return items


def chain(items, d, e_ref):
    rows, cols = iotas(HEAD_DIM)
    eye = (rows == cols).astype(f32)
    carry = None
    for item in items if d == 0 else items[::-1]:
        if e_ref is not None:
            if carry is None:
                out, early = item["local"], item["early"]
            else:
                moved = mm(item["early"], carry)
                out = item["local"] + moved[:, :HEAD_DIM]
                early = item["early"] + moved[:, HEAD_DIM:]
            at, size = item["group"]["at"], item["size"]
            e_ref[at : at + size, d * HEAD_DIM : (d + 1) * HEAD_DIM] = early.astype(bf16)
            item["out"] = out
        late, gate = item["late"], item["gate"]
        fresh = jnp.concatenate([late[:, :HEAD_DIM], (gate - 1.0) * eye - late[:, HEAD_DIM:]], axis=1)
        if carry is None:
            carry = fresh
        else:
            carry = gate * carry + fresh - mm(late[:, HEAD_DIM:], carry)
    return carry


def on_mesh(sp=None, tp=None):
    return (lax.axis_index("sp") if sp is None else sp, lax.axis_index("tp") if tp is None else tp)


def send(src, dst, send_sem, recv_sem, device):
    return pltpu.make_async_remote_copy(
        src_ref=src,
        dst_ref=dst,
        send_sem=send_sem,
        recv_sem=recv_sem,
        device_id=device,
        device_id_type=pl.DeviceIdType.MESH,
    )


def greet(devices):
    barrier = pltpu.get_barrier_semaphore()
    for device in devices:
        pl.semaphore_signal(barrier, inc=1, device_id=device, device_id_type=pl.DeviceIdType.MESH)


def split_three(x):
    high = x.astype(bf16)
    rest = x - high.astype(f32)
    mid = rest.astype(bf16)
    low = (rest - mid.astype(f32)).astype(bf16)
    return jnp.concatenate([high, mid, low], axis=1)


def advance(state, move, add):
    high = state.astype(bf16)
    low = (state - high.astype(f32)).astype(bf16)
    both = jnp.concatenate([high, low], axis=0)
    moved = jnp.dot(both, move, preferred_element_type=f32)
    rows = state.shape[0]
    return state + add.astype(f32) + moved[:rows] + moved[rows:]


def mixer_kernel(
    sp, tp, heads, tokens, ctx_tokens,
    cond_ref, ctx_cond_ref, gain_ref, head_gain_ref, write_bias_ref, decay_bias_ref, log_rate_ref,
    latent_hbm, context_hbm, shift_hbm, scale_hbm, gate_hbm, query_hbm, key_hbm, value_hbm,
    write_hbm, decay_hbm, out_hbm,
    out_ref,
    rows_v, mod_w, q_w, k_w, v_w, gate_w, out_w, st, stats, mod_v, q_v, k_v, v_v, rate_v, run_v, run_t,
    got_p, blocks, gate_row, o_v, e_v, maps_m, maps_b, got_m, got_b, starts, back, got_o, acc,
    load, sent_p, recv_p, sent_t, recv_t, sent_m, recv_m, sent_b, recv_b, sent_s, recv_s,
    sent_up, recv_dn, sent_dn, recv_up, sent_f, recv_f, sent_c, recv_c,
):
    me, col = lax.axis_index("sp"), lax.axis_index("tp")
    items = 2 * heads
    split = sp // items
    part_rows = HEAD_DIM // split
    half_owners = sp // heads
    width = mod_w.shape[2]
    half = width // 2
    total_tokens = tokens + ctx_tokens
    rings = [lax.rem(me + r, sp) for r in range(1, sp)]
    cross = [lax.rem(col + r, tp) for r in range(1, tp)]
    greet([on_mesh(sp=place) for place in rings] + [on_mesh(tp=place) for place in cross])

    def fetch(n, src, dst):
        copy = pltpu.make_async_copy(src, dst, load.at[n])
        copy.start()
        return copy

    gates_rows = write_hbm.shape[0]
    mod_loads = [fetch(n, src, mod_w.at[n]) for n, src in enumerate((shift_hbm, scale_hbm, gate_hbm))]
    row_loads = [
        fetch(3, latent_hbm, rows_v.at[pl.ds(0, tokens)]),
        fetch(4, context_hbm, rows_v.at[pl.ds(tokens, ctx_tokens)]),
    ]
    weight_loads = [
        fetch(5, key_hbm, k_w),
        fetch(6, value_hbm, v_w),
        fetch(7, write_hbm, gate_w.at[pl.ds(0, gates_rows)]),
        fetch(8, decay_hbm, gate_w.at[pl.ds(gates_rows, gates_rows)]),
        fetch(9, query_hbm, q_w),
    ]
    out_load = fetch(10, out_hbm, out_w)

    def silu(ref):
        value = ref[...].astype(f32)
        return value / (1.0 + jnp.exp(-value))

    silus = (silu(cond_ref), silu(ctx_cond_ref))
    quarter = silus[0].shape[0]
    lefts = []
    for part in range(quarter):
        lefts.append(
            jnp.concatenate(
                [silus[0][part : part + 1], silus[1][part : part + 1], jnp.zeros((6, silus[0].shape[1]), f32)], axis=0
            ).astype(bf16)
        )
    left = jnp.concatenate(lefts, axis=1)
    for copy in mod_loads:
        copy.wait()
    shift = jnp.dot(left, mod_w[0], preferred_element_type=f32)
    scale = jnp.dot(left, mod_w[1], preferred_element_type=f32)
    gate = jnp.dot(left, mod_w[2], preferred_element_type=f32)
    partial = jnp.concatenate([shift[0:2], scale[0:2], gate[0:1], jnp.zeros((3, width), f32)], axis=0)
    got_p[me] = jnp.concatenate([partial[:, :half], partial[:, half:]], axis=0).astype(bf16)
    pl.semaphore_wait(pltpu.get_barrier_semaphore(), len(rings) + len(cross))
    out = []
    for r, place in enumerate(rings):
        out.append(send(got_p.at[me], got_p.at[me], sent_p.at[r], recv_p.at[me], on_mesh(sp=place)))
        out[-1].start()

    gate_w[2 * gates_rows :, :] = jnp.zeros((gate_w.shape[0] - 2 * gates_rows, gate_w.shape[1]), bf16)
    for copy in row_loads:
        copy.wait()

    def measure_rows(i, unused):
        at = pl.ds(pl.multiple_of(i * 32, 32), 32)
        values = rows_v[at, :].astype(f32)
        mean = jnp.mean(values * values, axis=1, keepdims=True)
        stats[at, :] = jnp.broadcast_to(lax.rsqrt(mean + epsilon), (32, HEAD_DIM))
        return unused

    lax.fori_loop(0, total_tokens // 32, measure_rows, 0)

    for place in rings:
        spot = got_p.at[place]
        send(spot, spot, sent_p.at[0], recv_p.at[place], on_mesh(sp=place)).wait_recv()
    total = got_p[0].astype(f32)
    for place in range(1, sp):
        total = total + got_p[place].astype(f32)
    blocks[col] = jnp.concatenate([total[0:4], total[8:12]], axis=0)
    gate_row[...] = jnp.concatenate([total[4:5], total[12:13]], axis=1)
    for r, place in enumerate(cross):
        out.append(send(blocks.at[col], blocks.at[col], sent_t.at[r], recv_t.at[col], on_mesh(tp=place)))
        out[-1].start()
    for place in cross:
        spot = blocks.at[place]
        send(spot, spot, sent_t.at[0], recv_t.at[place], on_mesh(tp=place)).wait_recv()
    for place in range(tp):
        at = place * width
        for part in range(2):
            lanes = slice(at + part * half, at + (part + 1) * half)
            four = blocks[place, 4 * part : 4 * part + 4, :]
            st[0:2, lanes] = four[0:2]
            st[2:4, lanes] = (1.0 + four[2:4]) * gain_ref[:, lanes]

    def modulate(first, count, which):
        def step(i, unused):
            at = pl.ds(pl.multiple_of(first + i * 16, 16), 16)
            values = rows_v[at, :].astype(f32) * stats[at, 0:1]
            mod_v[at, :] = (values * st[2 + which : 3 + which, :] + st[which : which + 1, :]).astype(bf16)
            return unused

        lax.fori_loop(0, count // 16, step, 0)

    modulate(tokens, ctx_tokens, 1)
    modulate(0, tokens, 0)
    for copy in weight_loads:
        copy.wait()
    pre = mm_t(mod_v[...], gate_w[...]).astype(bf16).astype(f32)
    k_v[...] = jnp.dot(mod_v[...], k_w[...], preferred_element_type=f32).astype(bf16)
    v_v[...] = jnp.dot(mod_v[...], v_w[...], preferred_element_type=f32).astype(bf16)
    q_v[...] = jnp.dot(mod_v[0:tokens, :], q_w[...], preferred_element_type=f32).astype(bf16)

    all_heads = gates_rows // 2
    first_head = col * heads
    pre = pltpu.roll(pre, HEAD_DIM - first_head, 1)
    lane = lax.broadcasted_iota(jnp.int32, (1, HEAD_DIM), 1)
    write_bias = jnp.zeros((1, HEAD_DIM), f32)
    decay_bias = jnp.zeros((1, HEAD_DIM), f32)
    log_rate = jnp.zeros((1, HEAD_DIM), f32)
    for d in range(2):
        for head in range(heads):
            spot = d * all_heads + head
            write_bias = jnp.where(lane == spot, write_bias_ref[d, first_head + head], write_bias)
            decay_bias = jnp.where(lane == spot + gates_rows, decay_bias_ref[d, first_head + head], decay_bias)
            log_rate = jnp.where(lane == spot + gates_rows, log_rate_ref[d, first_head + head], log_rate)
    rate_v[...] = jax.nn.sigmoid(pre + write_bias)
    raised = pre + decay_bias
    soft = jnp.maximum(raised, 0.0) + jnp.log1p(jnp.exp(-jnp.abs(raised)))
    log_decay = -jnp.exp(log_rate) * soft
    lat, ctx = spans(tokens, ctx_tokens)
    for n, (at, size) in enumerate(lat + ctx):
        rows, cols = iotas(size)
        lower = (rows >= cols).astype(f32)
        upper = (rows <= cols).astype(f32)
        sums = jnp.dot(
            jnp.concatenate([lower, upper], axis=0).astype(bf16),
            split_three(log_decay[at : at + size]),
            preferred_element_type=f32,
        )
        sums = sums[:, :HEAD_DIM] + sums[:, HEAD_DIM : 2 * HEAD_DIM] + sums[:, 2 * HEAD_DIM :]
        running = jnp.where(lane < gates_rows + all_heads, sums[:size], sums[size:])
        run_v[at : at + size, :] = running
        run_t[n, :, :size] = running.T

    def group_of(n, at, size, head, latent):
        lanes = slice(head * HEAD_DIM, (head + 1) * HEAD_DIM)
        gates = []
        for d in range(2):
            spot = d * all_heads + head
            deep = spot + gates_rows
            gates.append(
                (
                    rate_v[at : at + size, spot : spot + 1],
                    run_v[at : at + size, deep : deep + 1],
                    run_t[n, deep : deep + 1, :size],
                )
            )
        return dict(
            at=at,
            size=size,
            k=k_v[at : at + size, lanes],
            v=v_v[at : at + size, lanes],
            q=q_v[at : at + size, lanes] if latent else None,
            gates=gates,
        )

    def keep(part, item, carry):
        maps_b[part, item] = carry[:, :HEAD_DIM].T.astype(bf16)
        maps_m[part, item] = carry[:, HEAD_DIM:].T.astype(bf16)

    my_item, my_part = me // split, lax.rem(me, split)

    def ship(part, owner):
        item, piece = owner // split, lax.rem(owner, split)
        return (
            send(
                maps_m.at[part, item], got_m.at[part, me], sent_m.at[part, owner], recv_m.at[part, me],
                on_mesh(sp=owner),
            ),
            send(
                maps_b.at[part, item, pl.ds(pl.multiple_of(piece * part_rows, part_rows), part_rows)],
                got_b.at[part, me], sent_b.at[part, owner], recv_b.at[part, me], on_mesh(sp=owner),
            ),
        )

    def ship_head(part, head):
        base = head * half_owners
        for r in range(1, half_owners):
            for copy in ship(part, base + lax.rem(me + r, half_owners)):
                copy.start()

        @pl.when(me // half_owners != head)
        def _():
            for copy in ship(part, base + lax.rem(me, half_owners)):
                copy.start()

    def keep_own(part):
        got_m[part, me] = maps_m[part, my_item]
        got_b[part, me] = maps_b[part, my_item, pl.ds(pl.multiple_of(my_part * part_rows, part_rows), part_rows), :]

    ctx_items = {}
    ctx_groups = []
    for head in range(heads):
        for n, (at, size) in enumerate(ctx):
            ctx_groups.append(group_of(len(lat) + n, at, size, head, False))
    done = prepare(ctx_groups)
    each = 2 * len(ctx)
    for head in range(heads):
        for d in range(2):
            chosen = [i for i in done[head * each : (head + 1) * each] if i["d"] == d]
            keep(0, 2 * head + d, chain(chosen, d, None))
    for head in range(heads):
        ship_head(0, head)
    for head in range(heads):
        done = prepare([group_of(n, at, size, head, True) for n, (at, size) in enumerate(lat)])
        for d in range(2):
            keep(1, 2 * head + d, chain([i for i in done if i["d"] == d], d, e_v.at[head]))
        for at, size in lat:
            pair = [i for i in done if i["group"]["at"] == at]
            o_v[head, at : at + size, :] = pair[0]["out"] + pair[1]["out"]
        ship_head(1, head)
    keep_own(0)
    keep_own(1)

    reverse = lax.rem(my_item, 2)

    def arrive(part):
        for place in rings:
            spot = got_m.at[part, place]
            send(spot, spot, sent_m.at[part, 0], recv_m.at[part, place], on_mesh(sp=place)).wait_recv()
            spot = got_b.at[part, place]
            send(spot, spot, sent_b.at[part, 0], recv_b.at[part, place], on_mesh(sp=place)).wait_recv()

    arrive(0)
    state = jnp.zeros((part_rows, HEAD_DIM), f32)
    for step in range(sp):
        place = step + reverse * (sp - 1 - 2 * step)
        state = advance(state, got_m[0, place], got_b[0, place])
    arrive(1)
    for step in range(sp):
        place = step + reverse * (sp - 1 - 2 * step)
        starts[place] = state.astype(bf16)
        if step < sp - 1:
            state = advance(state, got_m[1, place], got_b[1, place])
    back[me] = starts[me]

    def give_back(place):
        return send(starts.at[place], back.at[me], sent_s.at[place], recv_s.at[me], on_mesh(sp=place))

    for place in rings:
        give_back(place).start()

    core = lax.rem(col, 2)
    chips = tp // 2
    chip = col // 2
    partner = col + 1 - 2 * core
    up = lax.rem(chip + 1, chips) * 2 + core
    down = lax.rem(chip + chips - 1, chips) * 2 + core
    far = lax.rem(chip + 2, chips) * 2 + core
    mid = tokens // 2

    def piece(head, place, part):
        return got_o.at[head, place, pl.ds(part * mid, mid)]

    def to_up(head, part):
        return send(
            piece(head, col, part), piece(head, col, part), sent_up.at[head, part], recv_dn.at[head, part],
            on_mesh(tp=up),
        )

    def to_down(head, part):
        return send(
            piece(head, col, part), piece(head, col, part), sent_dn.at[head, part], recv_up.at[head, part],
            on_mesh(tp=down),
        )

    def forward(head, part):
        src, dst = (down, up) if part == 0 else (up, down)
        return send(
            piece(head, src, part), piece(head, src, part), sent_f.at[head, part], recv_f.at[head, part],
            on_mesh(tp=dst),
        )

    def relay(head, n, spot):
        return send(spot, spot, sent_c.at[head, n], recv_c.at[head, n], on_mesh(tp=partner))

    def finish_head(head):
        half_items = [2 * head, 2 * head + 1]
        for owner in range(2 * head * split, 2 * (head + 1) * split):

            @pl.when(owner != me)
            def _():
                spot = back.at[owner]
                send(spot, spot, sent_s.at[owner], recv_s.at[owner], on_mesh(sp=owner)).wait_recv()

        pair = [back[item * split : (item + 1) * split].reshape(HEAD_DIM, HEAD_DIM) for item in half_items]
        combined = o_v[head] + mm_t(e_v[head], jnp.concatenate(pair, axis=1))
        norm = lax.rsqrt(jnp.mean(combined * combined, axis=1, keepdims=True) + epsilon)
        got_o[head, col] = (combined * norm * head_gain_ref[...]).astype(bf16)
        for copy in (to_up(head, 0), to_down(head, 1), to_up(head, 1), to_down(head, 0)):
            out.append(copy)
            copy.start()
        out.append(relay(head, 0, got_o.at[head, col]))
        out[-1].start()

    def near_arrivals(head):
        waits = ((down, 0, recv_dn, True), (up, 1, recv_up, True), (down, 1, recv_dn, False), (up, 0, recv_up, False))
        for n, (place, part, sems, onward) in enumerate(waits):
            spot = piece(head, place, part)
            send(spot, spot, sent_up.at[head, part], sems.at[head, part], on_mesh(tp=place)).wait_recv()
            if onward:
                out.append(forward(head, part))
                out[-1].start()
            out.append(relay(head, 1 + n, spot))
            out[-1].start()

    def far_arrivals(head):
        for part in range(2):
            spot = piece(head, far, part)
            send(spot, spot, sent_f.at[head, part], recv_f.at[head, part], on_mesh(tp=up)).wait_recv()
            out.append(relay(head, 5 + part, spot))
            out[-1].start()

    def from_partner(head, n, spot):
        send(spot, spot, sent_c.at[head, n], recv_c.at[head, n], on_mesh(tp=partner)).wait_recv()

    def add(head, place, first=False):
        even = place - core
        lanes = jnp.concatenate([got_o[head, even], got_o[head, even + 1]], axis=1)
        depth = heads * HEAD_DIM
        weights = jnp.concatenate(
            [
                out_w[pl.ds(pl.multiple_of((even + n) * depth + head * HEAD_DIM, HEAD_DIM), HEAD_DIM), :]
                for n in range(2)
            ],
            axis=0,
        )
        part = jnp.dot(lanes, weights, preferred_element_type=f32)
        acc[...] = part if first else acc[...] + part

    def near_matmuls(head):
        from_partner(head, 0, got_o.at[head, partner])
        add(head, col, head == 0)
        other = 1 - 2 * core
        for n, (place, part) in enumerate(((down, 0), (up, 1), (down, 1), (up, 0))):
            from_partner(head, 1 + n, piece(head, place + other, part))
        add(head, down)
        add(head, up)

    def far_matmuls(head):
        other = 1 - 2 * core
        for part in range(2):
            from_partner(head, 5 + part, piece(head, far + other, part))
        add(head, far)

    out_load.wait()
    finish_head(0)
    near_arrivals(0)
    for head in range(1, heads):
        finish_head(head)
        far_arrivals(head - 1)
        near_matmuls(head - 1)
        far_matmuls(head - 1)
        near_arrivals(head)
    far_arrivals(heads - 1)
    near_matmuls(heads - 1)
    far_matmuls(heads - 1)
    lanes = pl.ds(pl.multiple_of(col * width, width), width)
    out_ref[...] = rows_v[0:tokens, lanes].astype(f32) + gate_row[...] * acc[...]
    for copy in out:
        copy.wait_send()
    for part in range(2):
        for r in range(1, sp):
            for copy in ship(part, lax.rem(me + r, sp)):
                copy.wait_send()
    for place in rings:
        give_back(place).wait_send()


def body(
    latent,
    context,
    condition,
    context_condition,
    shift_weight,
    scale_weight,
    gate_weight,
    norm_gain,
    query_weight,
    key_weight,
    value_weight,
    write_weight,
    decay_weight,
    write_bias,
    decay_bias,
    log_rate,
    head_gain,
    out_weight,
):
    sp, tp = lax.axis_size("sp"), lax.axis_size("tp")
    inner = query_weight.shape[1]
    heads = inner // HEAD_DIM
    tokens, ctx_tokens = latent.shape[0], context.shape[0]
    total = tokens + ctx_tokens
    features = latent.shape[1]
    width = shift_weight.shape[1]
    items = 2 * heads
    split = sp // items
    rows = HEAD_DIM // split
    chunks = sum(len(part) for part in spans(tokens, ctx_tokens))
    vmem = pl.BlockSpec(memory_space=pltpu.VMEM)
    smem = pl.BlockSpec(memory_space=pltpu.SMEM)
    anywhere = pl.BlockSpec(memory_space=pl.ANY)
    dma = pltpu.SemaphoreType.DMA
    flat = [jnp.transpose(w, (1, 2, 0)).reshape(-1, features) for w in (write_weight, decay_weight)]
    updated = pl.pallas_call(
        functools.partial(mixer_kernel, sp, tp, heads, tokens, ctx_tokens),
        in_specs=[vmem] * 4 + [smem] * 3 + [anywhere] * 11,
        out_specs=vmem,
        out_shape=jax.ShapeDtypeStruct((tokens, width), f32),
        scratch_shapes=[
            pltpu.VMEM((total, features), bf16),
            pltpu.VMEM((3,) + shift_weight.shape, bf16),
            pltpu.VMEM(query_weight.shape, bf16),
            pltpu.VMEM(key_weight.shape, bf16),
            pltpu.VMEM(value_weight.shape, bf16),
            pltpu.VMEM((HEAD_DIM, features), bf16),
            pltpu.VMEM(out_weight.shape, bf16),
            pltpu.VMEM((4, features), f32),
            pltpu.VMEM((total, HEAD_DIM), f32),
            pltpu.VMEM((total, features), bf16),
            pltpu.VMEM((tokens, inner), bf16),
            pltpu.VMEM((total, inner), bf16),
            pltpu.VMEM((total, inner), bf16),
            pltpu.VMEM((total, HEAD_DIM), f32),
            pltpu.VMEM((total, HEAD_DIM), f32),
            pltpu.VMEM((chunks, HEAD_DIM, CHUNK), f32),
            pltpu.VMEM((sp, 16, width // 2), bf16),
            pltpu.VMEM((tp, 8, width // 2), f32),
            pltpu.VMEM((1, width), f32),
            pltpu.VMEM((heads, tokens, HEAD_DIM), f32),
            pltpu.VMEM((heads, tokens, 2 * HEAD_DIM), bf16),
            pltpu.VMEM((2, items, HEAD_DIM, HEAD_DIM), bf16),
            pltpu.VMEM((2, items, HEAD_DIM, HEAD_DIM), bf16),
            pltpu.VMEM((2, sp, HEAD_DIM, HEAD_DIM), bf16),
            pltpu.VMEM((2, sp, rows, HEAD_DIM), bf16),
            pltpu.VMEM((sp, rows, HEAD_DIM), bf16),
            pltpu.VMEM((sp, rows, HEAD_DIM), bf16),
            pltpu.VMEM((heads, tp, tokens, HEAD_DIM), bf16),
            pltpu.VMEM((tokens, width), f32),
            dma((11,)),
            dma((sp,)),
            dma((sp,)),
            dma((tp,)),
            dma((tp,)),
            dma((2, sp)),
            dma((2, sp)),
            dma((2, sp)),
            dma((2, sp)),
            dma((sp,)),
            dma((sp,)),
            dma((heads, 2)),
            dma((heads, 2)),
            dma((heads, 2)),
            dma((heads, 2)),
            dma((heads, 2)),
            dma((heads, 2)),
            dma((heads, 7)),
            dma((heads, 7)),
        ],
        compiler_params=pltpu.CompilerParams(
            collective_id=0, has_side_effects=True, vmem_limit_bytes=56 * 1024 * 1024
        ),
        name="mixer",
    )(
        condition.reshape(-1, HEAD_DIM),
        context_condition.reshape(-1, HEAD_DIM),
        norm_gain[None, :],
        head_gain[None, :],
        write_bias,
        decay_bias,
        log_rate,
        latent,
        context,
        shift_weight,
        scale_weight,
        gate_weight,
        query_weight,
        key_weight,
        value_weight,
        flat[0],
        flat[1],
        out_weight,
    )
    return updated.astype(bf16)


def solution(mesh):
    placed = (
        P("sp", None),
        P("sp", None),
        P("sp"),
        P("sp"),
        P("sp", "tp"),
        P("sp", "tp"),
        P("sp", "tp"),
        P(),
        P(None, "tp"),
        P(None, "tp"),
        P(None, "tp"),
        P(),
        P(),
        P(),
        P(),
        P(),
        P(),
        P(None, "tp"),
    )
    return jax.shard_map(body, mesh=mesh, in_specs=placed, out_specs=P("sp", "tp"), check_vma=False)
```

```python
import functools

import jax
import jax.numpy as jnp
from jax import lax
from jax.experimental import pallas as pl
from jax.experimental.pallas import tpu as pltpu
from jax.sharding import PartitionSpec as P

HEAD_DIM = 128
CHUNK = 128
epsilon = 0.0001
bf16 = jnp.bfloat16
f32 = jnp.float32


def mm(a, b):
    return jnp.dot(a.astype(bf16), b.astype(bf16), preferred_element_type=f32)


def mm_t(a, b):
    return lax.dot_general(a, b, (((1,), (1,)), ((), ())), preferred_element_type=f32)


def spans(tokens, ctx_tokens):
    size = min(CHUNK, tokens)
    lat = [(at, size) for at in range(0, tokens, size)]
    ctx_size = min(CHUNK, ctx_tokens)
    ctx = [(tokens + at, ctx_size) for at in range(0, ctx_tokens, ctx_size)]
    return lat, ctx


def iotas(size):
    rows = lax.broadcasted_iota(jnp.int32, (size, size), 0)
    cols = lax.broadcasted_iota(jnp.int32, (size, size), 1)
    return rows, cols


def prepare(groups):
    items = []
    for group in groups:
        size = group["size"]
        rows, cols = iotas(size)
        keys = group["k"]
        keys_t = keys.astype(f32).T
        gram = jnp.dot(keys, keys_t.astype(bf16), preferred_element_type=f32)
        diag = jnp.where(rows == cols, gram, 0.0)
        s_col = lax.rsqrt(jnp.sum(diag, axis=1, keepdims=True) + epsilon)
        s_row = lax.rsqrt(jnp.sum(diag, axis=0, keepdims=True) + epsilon)
        gram = gram * s_col * s_row
        group["keys"] = keys.astype(f32) * s_col
        group["keys_t"] = keys_t * s_row
        group["values"] = group["v"].astype(f32)
        if group["q"] is not None:
            queries = group["q"].astype(f32)
            q_scale = lax.rsqrt(jnp.sum(queries * queries, axis=1, keepdims=True) + epsilon) * HEAD_DIM**-0.5
            group["queries"] = queries * q_scale
            group["score"] = (
                jnp.dot(group["q"], keys_t.astype(bf16), preferred_element_type=f32) * q_scale * s_row
            )
        for d in range(2):
            rate_col, run_col, run_row = group["gates"][d]
            inside = rows >= cols if d == 0 else rows <= cols
            strict = rows > cols if d == 0 else rows < cols
            decay = jnp.where(inside, jnp.exp(jnp.minimum(run_col - run_row, 0.0)), 0.0)
            system = jnp.where(strict, gram * decay * rate_col, 0.0)
            item = dict(group=group, size=size, d=d, rate_col=rate_col, run_col=run_col, run_row=run_row)
            item["system"] = system
            if group["q"] is not None:
                item["score"] = group["score"] * decay
            near = (rows // 2) == (cols // 2)
            item["inv"] = jnp.where(rows == cols, 1.0, jnp.where(near, -system, 0.0))
            items.append(item)
    span = 2
    while span < max(item["size"] for item in items):
        firsts = []
        for item in items:
            if span >= item["size"]:
                firsts.append(None)
                continue
            rows, cols = iotas(item["size"])
            rows, cols = rows // span, cols // span
            if item["d"] == 0:
                mask = ((rows % 2) == 1) & (cols == rows - 1)
            else:
                mask = ((cols % 2) == 1) & (rows == cols - 1)
            firsts.append(mm(jnp.where(mask, item["system"], 0.0), item["inv"]))
        for item, first in zip(items, firsts):
            if first is not None:
                item["inv"] = item["inv"] - mm(item["inv"], first)
        span *= 2
    for item in items:
        group = item["group"]
        growth = jnp.exp(item["run_col"])
        both = jnp.concatenate(
            [group["values"] * item["rate_col"], group["keys"] * (item["rate_col"] * growth)], axis=1
        )
        item["solved"] = mm(item["inv"], both)
        last = item["run_row"][:, item["size"] - 1 :] if item["d"] == 0 else item["run_row"][:, :1]
        item["gate"] = jnp.exp(last)
        late_t = group["keys_t"] * jnp.exp(last - item["run_row"])
        item["late"] = mm(late_t, item["solved"])
        if group["q"] is not None:
            weighed = mm(item["score"], item["solved"])
            item["local"] = weighed[:, :HEAD_DIM]
            item["early"] = group["queries"] * growth - weighed[:, HEAD_DIM:]
    return items


def chain(items, d, e_ref):
    rows, cols = iotas(HEAD_DIM)
    eye = (rows == cols).astype(f32)
    carry = None
    for item in items if d == 0 else items[::-1]:
        if e_ref is not None:
            if carry is None:
                out, early = item["local"], item["early"]
            else:
                moved = mm(item["early"], carry)
                out = item["local"] + moved[:, :HEAD_DIM]
                early = item["early"] + moved[:, HEAD_DIM:]
            at, size = item["group"]["at"], item["size"]
            e_ref[at : at + size, d * HEAD_DIM : (d + 1) * HEAD_DIM] = early.astype(bf16)
            item["out"] = out
        late, gate = item["late"], item["gate"]
        fresh = jnp.concatenate([late[:, :HEAD_DIM], (gate - 1.0) * eye - late[:, HEAD_DIM:]], axis=1)
        if carry is None:
            carry = fresh
        else:
            carry = gate * carry + fresh - mm(late[:, HEAD_DIM:], carry)
    return carry


def on_mesh(sp=None, tp=None):
    return (lax.axis_index("sp") if sp is None else sp, lax.axis_index("tp") if tp is None else tp)


def send(src, dst, send_sem, recv_sem, device):
    return pltpu.make_async_remote_copy(
        src_ref=src,
        dst_ref=dst,
        send_sem=send_sem,
        recv_sem=recv_sem,
        device_id=device,
        device_id_type=pl.DeviceIdType.MESH,
    )


def greet(devices):
    barrier = pltpu.get_barrier_semaphore()
    for device in devices:
        pl.semaphore_signal(barrier, inc=1, device_id=device, device_id_type=pl.DeviceIdType.MESH)


def split_three(x):
    high = x.astype(bf16)
    rest = x - high.astype(f32)
    mid = rest.astype(bf16)
    low = (rest - mid.astype(f32)).astype(bf16)
    return jnp.concatenate([high, mid, low], axis=1)


def advance(state, move, add):
    high = state.astype(bf16)
    low = (state - high.astype(f32)).astype(bf16)
    both = jnp.concatenate([high, low], axis=0)
    moved = jnp.dot(both, move, preferred_element_type=f32)
    rows = state.shape[0]
    return state + add.astype(f32) + moved[:rows] + moved[rows:]


def mixer_kernel(
    sp, tp, heads, tokens, ctx_tokens,
    cond_ref, ctx_cond_ref, gain_ref, head_gain_ref, write_bias_ref, decay_bias_ref, log_rate_ref,
    latent_hbm, context_hbm, shift_hbm, scale_hbm, gate_hbm, query_hbm, key_hbm, value_hbm,
    write_hbm, decay_hbm, out_hbm,
    out_ref,
    rows_v, mod_w, q_w, k_w, v_w, gate_w, out_w, st, stats, mod_v, q_v, k_v, v_v, rate_v, run_v, run_t,
    got_p, blocks, gate_row, o_v, e_v, maps_m, maps_b, got_m, got_b, starts, back, got_o, acc,
    load, sent_p, recv_p, sent_t, recv_t, sent_m, recv_m, sent_b, recv_b, sent_s, recv_s,
    sent_o, recv_dn, recv_up, recv_f, recv_c,
):
    me, col = lax.axis_index("sp"), lax.axis_index("tp")
    items = 2 * heads
    split = sp // items
    part_rows = HEAD_DIM // split
    half_owners = sp // heads
    width = mod_w.shape[2]
    half = width // 2
    total_tokens = tokens + ctx_tokens
    rings = [lax.rem(me + r, sp) for r in range(1, sp)]
    near = on_mesh(sp=rings[0])
    cross = [lax.rem(col + r, tp) for r in range(1, tp)]
    greet([on_mesh(sp=place) for place in rings] + [on_mesh(tp=place) for place in cross])

    def arrived(spot, sem):
        send(spot, spot, sem, sem, near).wait_recv()

    def left(spot, sem):
        send(spot, spot, sem, sem, near).wait_send()

    def fetch(n, src, dst):
        copy = pltpu.make_async_copy(src, dst, load.at[n])
        copy.start()
        return copy

    gates_rows = write_hbm.shape[0]
    mod_loads = [fetch(n, src, mod_w.at[n]) for n, src in enumerate((shift_hbm, scale_hbm, gate_hbm))]
    row_loads = [
        fetch(3, latent_hbm, rows_v.at[pl.ds(0, tokens)]),
        fetch(4, context_hbm, rows_v.at[pl.ds(tokens, ctx_tokens)]),
    ]
    weight_loads = [
        fetch(5, key_hbm, k_w),
        fetch(6, value_hbm, v_w),
        fetch(7, write_hbm, gate_w.at[pl.ds(0, gates_rows)]),
        fetch(8, decay_hbm, gate_w.at[pl.ds(gates_rows, gates_rows)]),
        fetch(9, query_hbm, q_w),
    ]
    out_load = fetch(10, out_hbm, out_w)

    def silu(ref):
        value = ref[...].astype(f32)
        return value / (1.0 + jnp.exp(-value))

    silus = (silu(cond_ref), silu(ctx_cond_ref))
    quarter = silus[0].shape[0]
    lefts = []
    for part in range(quarter):
        lefts.append(
            jnp.concatenate(
                [silus[0][part : part + 1], silus[1][part : part + 1], jnp.zeros((6, silus[0].shape[1]), f32)], axis=0
            ).astype(bf16)
        )
    silu_rows = jnp.concatenate(lefts, axis=1)
    for copy in mod_loads:
        copy.wait()
    shift = jnp.dot(silu_rows, mod_w[0], preferred_element_type=f32)
    scale = jnp.dot(silu_rows, mod_w[1], preferred_element_type=f32)
    gate = jnp.dot(silu_rows, mod_w[2], preferred_element_type=f32)
    partial = jnp.concatenate([shift[0:2], scale[0:2], gate[0:1], jnp.zeros((3, width), f32)], axis=0)
    got_p[me] = jnp.concatenate([partial[:, :half], partial[:, half:]], axis=0).astype(bf16)
    pl.semaphore_wait(pltpu.get_barrier_semaphore(), len(rings) + len(cross))
    for place in rings:
        send(got_p.at[me], got_p.at[me], sent_p, recv_p, on_mesh(sp=place)).start()

    gate_w[2 * gates_rows :, :] = jnp.zeros((gate_w.shape[0] - 2 * gates_rows, gate_w.shape[1]), bf16)
    for copy in row_loads:
        copy.wait()

    def measure_rows(i, unused):
        at = pl.ds(pl.multiple_of(i * 32, 32), 32)
        values = rows_v[at, :].astype(f32)
        mean = jnp.mean(values * values, axis=1, keepdims=True)
        stats[at, :] = jnp.broadcast_to(lax.rsqrt(mean + epsilon), (32, HEAD_DIM))
        return unused

    lax.fori_loop(0, total_tokens // 32, measure_rows, 0)

    arrived(got_p.at[pl.ds(0, sp - 1)], recv_p)
    total = got_p[0].astype(f32)
    for place in range(1, sp):
        total = total + got_p[place].astype(f32)
    blocks[col] = jnp.concatenate([total[0:4], total[8:12]], axis=0)
    gate_row[...] = jnp.concatenate([total[4:5], total[12:13]], axis=1)
    for place in cross:
        send(blocks.at[col], blocks.at[col], sent_t, recv_t, on_mesh(tp=place)).start()
    arrived(blocks.at[pl.ds(0, tp - 1)], recv_t)
    for place in range(tp):
        at = place * width
        for part in range(2):
            lanes = slice(at + part * half, at + (part + 1) * half)
            four = blocks[place, 4 * part : 4 * part + 4, :]
            scaled = (1.0 + four[2:4]) * gain_ref[:, lanes]
            for which in range(2):
                st[which, :, lanes] = jnp.broadcast_to(four[which : which + 1], (8, half))
                st[2 + which, :, lanes] = jnp.broadcast_to(scaled[which : which + 1], (8, half))

    def modulate(first, count, which):
        def step(i, unused):
            at = pl.ds(pl.multiple_of(first + i * 32, 32), 32)
            root = stats[at, :]
            for lane_at in range(0, rows_v.shape[1], HEAD_DIM):
                lanes = slice(lane_at, lane_at + HEAD_DIM)
                values = rows_v[at, lanes].astype(f32) * root
                shift, scale = st[which, :, lanes], st[2 + which, :, lanes]
                parts = [values[n : n + 8] * scale + shift for n in range(0, 32, 8)]
                mod_v[at, lanes] = jnp.concatenate(parts, axis=0).astype(bf16)
            return unused

        lax.fori_loop(0, count // 32, step, 0)

    modulate(tokens, ctx_tokens, 1)
    modulate(0, tokens, 0)
    for copy in weight_loads:
        copy.wait()
    pre = mm_t(mod_v[...], gate_w[...]).astype(bf16).astype(f32)
    k_v[...] = jnp.dot(mod_v[...], k_w[...], preferred_element_type=f32).astype(bf16)
    v_v[...] = jnp.dot(mod_v[...], v_w[...], preferred_element_type=f32).astype(bf16)
    q_v[...] = jnp.dot(mod_v[0:tokens, :], q_w[...], preferred_element_type=f32).astype(bf16)

    all_heads = gates_rows // 2
    first_head = col * heads
    pre = pltpu.roll(pre, HEAD_DIM - first_head, 1)
    lane = lax.broadcasted_iota(jnp.int32, (1, HEAD_DIM), 1)
    write_bias = jnp.zeros((1, HEAD_DIM), f32)
    decay_bias = jnp.zeros((1, HEAD_DIM), f32)
    log_rate = jnp.zeros((1, HEAD_DIM), f32)
    for d in range(2):
        for head in range(heads):
            spot = d * all_heads + head
            write_bias = jnp.where(lane == spot, write_bias_ref[d, first_head + head], write_bias)
            decay_bias = jnp.where(lane == spot + gates_rows, decay_bias_ref[d, first_head + head], decay_bias)
            log_rate = jnp.where(lane == spot + gates_rows, log_rate_ref[d, first_head + head], log_rate)
    rate_v[...] = jax.nn.sigmoid(pre + write_bias)
    raised = pre + decay_bias
    soft = jnp.maximum(raised, 0.0) + jnp.log1p(jnp.exp(-jnp.abs(raised)))
    log_decay = -jnp.exp(log_rate) * soft
    lat, ctx = spans(tokens, ctx_tokens)
    for n, (at, size) in enumerate(lat + ctx):
        rows, cols = iotas(size)
        lower = (rows >= cols).astype(f32)
        upper = (rows <= cols).astype(f32)
        sums = jnp.dot(
            jnp.concatenate([lower, upper], axis=0).astype(bf16),
            split_three(log_decay[at : at + size]),
            preferred_element_type=f32,
        )
        sums = sums[:, :HEAD_DIM] + sums[:, HEAD_DIM : 2 * HEAD_DIM] + sums[:, 2 * HEAD_DIM :]
        running = jnp.where(lane < gates_rows + all_heads, sums[:size], sums[size:])
        run_v[at : at + size, :] = running
        run_t[n, :, :size] = running.T

    def group_of(n, at, size, head, latent):
        lanes = slice(head * HEAD_DIM, (head + 1) * HEAD_DIM)
        gates = []
        for d in range(2):
            spot = d * all_heads + head
            deep = spot + gates_rows
            gates.append(
                (
                    rate_v[at : at + size, spot : spot + 1],
                    run_v[at : at + size, deep : deep + 1],
                    run_t[n, deep : deep + 1, :size],
                )
            )
        return dict(
            at=at,
            size=size,
            k=k_v[at : at + size, lanes],
            v=v_v[at : at + size, lanes],
            q=q_v[at : at + size, lanes] if latent else None,
            gates=gates,
        )

    def keep(part, item, carry):
        maps_b[part, item] = carry[:, :HEAD_DIM].T.astype(bf16)
        maps_m[part, item] = carry[:, HEAD_DIM:].T.astype(bf16)

    my_item, my_part = me // split, lax.rem(me, split)

    def ship(part, owner):
        item, piece = owner // split, lax.rem(owner, split)
        return (
            send(
                maps_m.at[part, item], got_m.at[part, me], sent_m.at[part], recv_m.at[part],
                on_mesh(sp=owner),
            ),
            send(
                maps_b.at[part, item, pl.ds(pl.multiple_of(piece * part_rows, part_rows), part_rows)],
                got_b.at[part, me], sent_b.at[part], recv_b.at[part], on_mesh(sp=owner),
            ),
        )

    def ship_head(part, head):
        base = head * half_owners
        for r in range(1, half_owners):
            for copy in ship(part, base + lax.rem(me + r, half_owners)):
                copy.start()

        @pl.when(me // half_owners != head)
        def _():
            for copy in ship(part, base + lax.rem(me, half_owners)):
                copy.start()

    def keep_own(part):
        got_m[part, me] = maps_m[part, my_item]
        got_b[part, me] = maps_b[part, my_item, pl.ds(pl.multiple_of(my_part * part_rows, part_rows), part_rows), :]

    ctx_items = {}
    ctx_groups = []
    for head in range(heads):
        for n, (at, size) in enumerate(ctx):
            ctx_groups.append(group_of(len(lat) + n, at, size, head, False))
    done = prepare(ctx_groups)
    each = 2 * len(ctx)
    for head in range(heads):
        for d in range(2):
            chosen = [i for i in done[head * each : (head + 1) * each] if i["d"] == d]
            keep(0, 2 * head + d, chain(chosen, d, None))
    for head in range(heads):
        ship_head(0, head)
    for head in range(heads):
        done = prepare([group_of(n, at, size, head, True) for n, (at, size) in enumerate(lat)])
        for d in range(2):
            keep(1, 2 * head + d, chain([i for i in done if i["d"] == d], d, e_v.at[head]))
        for at, size in lat:
            pair = [i for i in done if i["group"]["at"] == at]
            o_v[head, at : at + size, :] = pair[0]["out"] + pair[1]["out"]
        ship_head(1, head)
    keep_own(0)
    keep_own(1)

    reverse = lax.rem(my_item, 2)

    def arrive(part):
        arrived(got_m.at[part, pl.ds(0, sp - 1)], recv_m.at[part])
        arrived(got_b.at[part, pl.ds(0, sp - 1)], recv_b.at[part])

    arrive(0)
    state = jnp.zeros((part_rows, HEAD_DIM), f32)
    for step in range(sp):
        place = step + reverse * (sp - 1 - 2 * step)
        state = advance(state, got_m[0, place], got_b[0, place])
    arrive(1)
    for step in range(sp):
        place = step + reverse * (sp - 1 - 2 * step)
        starts[place] = state.astype(bf16)
        if step < sp - 1:
            state = advance(state, got_m[1, place], got_b[1, place])
    back[me] = starts[me]

    def give_back(place):
        return send(starts.at[place], back.at[me], sent_s, recv_s.at[my_item // 2], on_mesh(sp=place))

    for place in rings:
        give_back(place).start()

    core = lax.rem(col, 2)
    chips = tp // 2
    chip = col // 2
    partner = col + 1 - 2 * core
    up = lax.rem(chip + 1, chips) * 2 + core
    down = lax.rem(chip + chips - 1, chips) * 2 + core
    far = lax.rem(chip + 2, chips) * 2 + core
    mid = tokens // 2

    def piece(head, place, part):
        return got_o.at[head, place, pl.ds(part * mid, mid)]

    def to_up(head, part):
        return send(
            piece(head, col, part), piece(head, col, part), sent_o.at[head], recv_dn.at[head, part],
            on_mesh(tp=up),
        )

    def to_down(head, part):
        return send(
            piece(head, col, part), piece(head, col, part), sent_o.at[head], recv_up.at[head, part],
            on_mesh(tp=down),
        )

    def forward(head, part):
        src, dst = (down, up) if part == 0 else (up, down)
        return send(
            piece(head, src, part), piece(head, src, part), sent_o.at[head], recv_f.at[head, part],
            on_mesh(tp=dst),
        )

    def relay(head, n, spot):
        return send(spot, spot, sent_o.at[head], recv_c.at[head, n], on_mesh(tp=partner))

    def finish_head(head):
        half_items = [2 * head, 2 * head + 1]
        @pl.when(me // half_owners == head)
        def _():
            arrived(back.at[pl.ds(0, half_owners - 1)], recv_s.at[head])

        @pl.when(me // half_owners != head)
        def _():
            arrived(back.at[pl.ds(0, half_owners)], recv_s.at[head])

        pair = [back[item * split : (item + 1) * split].reshape(HEAD_DIM, HEAD_DIM) for item in half_items]
        combined = o_v[head] + mm_t(e_v[head], jnp.concatenate(pair, axis=1))
        norm = lax.rsqrt(jnp.mean(combined * combined, axis=1, keepdims=True) + epsilon)
        got_o[head, col] = (combined * norm * head_gain_ref[...]).astype(bf16)
        for copy in (to_up(head, 0), to_down(head, 1), to_up(head, 1), to_down(head, 0)):
            copy.start()
        relay(head, 0, got_o.at[head, col]).start()

    def near_arrivals(head):
        waits = (
            (down, 0, recv_dn, 1, True),
            (up, 1, recv_up, 2, True),
            (down, 1, recv_dn, 1, False),
            (up, 0, recv_up, 2, False),
        )
        for place, part, sems, n, onward in waits:
            spot = piece(head, place, part)
            arrived(spot, sems.at[head, part])
            if onward:
                forward(head, part).start()
            relay(head, n, spot).start()

    def far_arrivals(head):
        for part in range(2):
            spot = piece(head, far, part)
            arrived(spot, recv_f.at[head, part])
            relay(head, 3, spot).start()

    def from_partner(head, n):
        arrived(got_o.at[head, 0], recv_c.at[head, n])

    def add(head, place, first=False):
        even = place - core
        lanes = jnp.concatenate([got_o[head, even], got_o[head, even + 1]], axis=1)
        depth = heads * HEAD_DIM
        weights = jnp.concatenate(
            [
                out_w[pl.ds(pl.multiple_of((even + n) * depth + head * HEAD_DIM, HEAD_DIM), HEAD_DIM), :]
                for n in range(2)
            ],
            axis=0,
        )
        part = jnp.dot(lanes, weights, preferred_element_type=f32)
        acc[...] = part if first else acc[...] + part

    def near_matmuls(head):
        from_partner(head, 0)
        add(head, col, head == 0)
        from_partner(head, 1)
        add(head, down)
        from_partner(head, 2)
        add(head, up)

    def far_matmuls(head):
        from_partner(head, 3)
        add(head, far)

    out_load.wait()
    finish_head(0)
    near_arrivals(0)
    for head in range(1, heads):
        finish_head(head)
        far_arrivals(head - 1)
        near_matmuls(head - 1)
        far_matmuls(head - 1)
        near_arrivals(head)
    far_arrivals(heads - 1)
    near_matmuls(heads - 1)
    far_matmuls(heads - 1)
    lanes = pl.ds(pl.multiple_of(col * width, width), width)
    out_ref[...] = rows_v[0:tokens, lanes].astype(f32) + gate_row[...] * acc[...]
    left(got_p.at[pl.ds(0, sp - 1)], sent_p)
    left(blocks.at[pl.ds(0, tp - 1)], sent_t)
    for part in range(2):
        left(got_m.at[part, pl.ds(0, sp - 1)], sent_m.at[part])
        left(got_b.at[part, pl.ds(0, sp - 1)], sent_b.at[part])
    left(starts.at[pl.ds(0, sp - 1)], sent_s)
    for head in range(heads):
        left(got_o.at[head, pl.ds(0, tp - 1)], sent_o.at[head])


def body(
    latent,
    context,
    condition,
    context_condition,
    shift_weight,
    scale_weight,
    gate_weight,
    norm_gain,
    query_weight,
    key_weight,
    value_weight,
    write_weight,
    decay_weight,
    write_bias,
    decay_bias,
    log_rate,
    head_gain,
    out_weight,
):
    sp, tp = lax.axis_size("sp"), lax.axis_size("tp")
    inner = query_weight.shape[1]
    heads = inner // HEAD_DIM
    tokens, ctx_tokens = latent.shape[0], context.shape[0]
    total = tokens + ctx_tokens
    features = latent.shape[1]
    width = shift_weight.shape[1]
    items = 2 * heads
    split = sp // items
    rows = HEAD_DIM // split
    chunks = sum(len(part) for part in spans(tokens, ctx_tokens))
    vmem = pl.BlockSpec(memory_space=pltpu.VMEM)
    smem = pl.BlockSpec(memory_space=pltpu.SMEM)
    anywhere = pl.BlockSpec(memory_space=pltpu.HBM)
    dma = pltpu.SemaphoreType.DMA
    flat = [jnp.transpose(w, (1, 2, 0)).reshape(-1, features) for w in (write_weight, decay_weight)]
    updated = pl.pallas_call(
        functools.partial(mixer_kernel, sp, tp, heads, tokens, ctx_tokens),
        in_specs=[vmem] * 4 + [smem] * 3 + [anywhere] * 11,
        out_specs=vmem,
        out_shape=jax.ShapeDtypeStruct((tokens, width), f32),
        scratch_shapes=[
            pltpu.VMEM((total, features), bf16),
            pltpu.VMEM((3,) + shift_weight.shape, bf16),
            pltpu.VMEM(query_weight.shape, bf16),
            pltpu.VMEM(key_weight.shape, bf16),
            pltpu.VMEM(value_weight.shape, bf16),
            pltpu.VMEM((HEAD_DIM, features), bf16),
            pltpu.VMEM(out_weight.shape, bf16),
            pltpu.VMEM((4, 8, features), f32),
            pltpu.VMEM((total, HEAD_DIM), f32),
            pltpu.VMEM((total, features), bf16),
            pltpu.VMEM((tokens, inner), bf16),
            pltpu.VMEM((total, inner), bf16),
            pltpu.VMEM((total, inner), bf16),
            pltpu.VMEM((total, HEAD_DIM), f32),
            pltpu.VMEM((total, HEAD_DIM), f32),
            pltpu.VMEM((chunks, HEAD_DIM, CHUNK), f32),
            pltpu.VMEM((sp, 16, width // 2), bf16),
            pltpu.VMEM((tp, 8, width // 2), f32),
            pltpu.VMEM((1, width), f32),
            pltpu.VMEM((heads, tokens, HEAD_DIM), f32),
            pltpu.VMEM((heads, tokens, 2 * HEAD_DIM), bf16),
            pltpu.VMEM((2, items, HEAD_DIM, HEAD_DIM), bf16),
            pltpu.VMEM((2, items, HEAD_DIM, HEAD_DIM), bf16),
            pltpu.VMEM((2, sp, HEAD_DIM, HEAD_DIM), bf16),
            pltpu.VMEM((2, sp, rows, HEAD_DIM), bf16),
            pltpu.VMEM((sp, rows, HEAD_DIM), bf16),
            pltpu.VMEM((sp, rows, HEAD_DIM), bf16),
            pltpu.VMEM((heads, tp, tokens, HEAD_DIM), bf16),
            pltpu.VMEM((tokens, width), f32),
            dma((11,)),
            dma,
            dma,
            dma,
            dma,
            dma((2,)),
            dma((2,)),
            dma((2,)),
            dma((2,)),
            dma,
            dma((heads,)),
            dma((heads,)),
            dma((heads, 2)),
            dma((heads, 2)),
            dma((heads, 2)),
            dma((heads, 4)),
        ],
        compiler_params=pltpu.CompilerParams(
            collective_id=0, has_side_effects=True, vmem_limit_bytes=58 * 1024 * 1024
        ),
        name="mixer",
    )(
        condition.reshape(-1, HEAD_DIM),
        context_condition.reshape(-1, HEAD_DIM),
        norm_gain[None, :],
        head_gain[None, :],
        write_bias,
        decay_bias,
        log_rate,
        latent,
        context,
        shift_weight,
        scale_weight,
        gate_weight,
        query_weight,
        key_weight,
        value_weight,
        flat[0],
        flat[1],
        out_weight,
    )
    return updated.astype(bf16)


def solution(mesh):
    placed = (
        P("sp", None),
        P("sp", None),
        P("sp"),
        P("sp"),
        P("sp", "tp"),
        P("sp", "tp"),
        P("sp", "tp"),
        P(),
        P(None, "tp"),
        P(None, "tp"),
        P(None, "tp"),
        P(),
        P(),
        P(),
        P(),
        P(),
        P(),
        P(None, "tp"),
    )
    return jax.shard_map(body, mesh=mesh, in_specs=placed, out_specs=P("sp", "tp"), check_vma=False)
```

```python
import functools

import jax
import jax.numpy as jnp
from jax import lax
from jax.experimental import pallas as pl
from jax.experimental.pallas import tpu as pltpu
from jax.sharding import PartitionSpec as P

HEAD_DIM = 128
CHUNK = 128
epsilon = 0.0001
bf16 = jnp.bfloat16
f32 = jnp.float32


def mm(a, b):
    return jnp.dot(a.astype(bf16), b.astype(bf16), preferred_element_type=f32)


def mm_t(a, b):
    return lax.dot_general(a, b, (((1,), (1,)), ((), ())), preferred_element_type=f32)


def spans(tokens, ctx_tokens):
    size = min(CHUNK, tokens)
    lat = [(at, size) for at in range(0, tokens, size)]
    ctx_size = min(CHUNK, ctx_tokens)
    ctx = [(tokens + at, ctx_size) for at in range(0, ctx_tokens, ctx_size)]
    return lat, ctx


def iotas(size):
    rows = lax.broadcasted_iota(jnp.int32, (size, size), 0)
    cols = lax.broadcasted_iota(jnp.int32, (size, size), 1)
    return rows, cols


def prepare(groups):
    items = []
    for group in groups:
        size = group["size"]
        rows, cols = iotas(size)
        keys = group["k"]
        keys_t = keys.astype(f32).T
        gram = jnp.dot(keys, keys_t.astype(bf16), preferred_element_type=f32)
        diag = jnp.where(rows == cols, gram, 0.0)
        s_col = lax.rsqrt(jnp.sum(diag, axis=1, keepdims=True) + epsilon)
        s_row = lax.rsqrt(jnp.sum(diag, axis=0, keepdims=True) + epsilon)
        gram = gram * s_col * s_row
        group["keys"] = keys.astype(f32) * s_col
        group["keys_t"] = keys_t * s_row
        group["values"] = group["v"].astype(f32)
        for d in range(2):
            rate_col, run_col, run_row = group["gates"][d]
            inside = rows >= cols if d == 0 else rows <= cols
            strict = rows > cols if d == 0 else rows < cols
            decay = jnp.where(inside, jnp.exp(jnp.minimum(run_col - run_row, 0.0)), 0.0)
            system = jnp.where(strict, gram * decay * rate_col, 0.0)
            item = dict(group=group, size=size, d=d, rate_col=rate_col, run_col=run_col, run_row=run_row)
            item["system"] = system
            near = (rows // 2) == (cols // 2)
            item["inv"] = jnp.where(rows == cols, 1.0, jnp.where(near, -system, 0.0))
            items.append(item)
    span = 2
    while span < max(item["size"] for item in items):
        firsts = []
        for item in items:
            if span >= item["size"]:
                firsts.append(None)
                continue
            rows, cols = iotas(item["size"])
            rows, cols = rows // span, cols // span
            if item["d"] == 0:
                mask = ((rows % 2) == 1) & (cols == rows - 1)
            else:
                mask = ((cols % 2) == 1) & (rows == cols - 1)
            firsts.append(mm(jnp.where(mask, item["system"], 0.0), item["inv"]))
        for item, first in zip(items, firsts):
            if first is not None:
                item["inv"] = item["inv"] - mm(item["inv"], first)
        span *= 2
    for item in items:
        group = item["group"]
        growth = jnp.exp(item["run_col"])
        both = jnp.concatenate(
            [group["values"] * item["rate_col"], group["keys"] * (item["rate_col"] * growth)], axis=1
        )
        item["solved"] = mm(item["inv"], both)
        last = item["run_row"][:, item["size"] - 1 :] if item["d"] == 0 else item["run_row"][:, :1]
        item["gate"] = jnp.exp(last)
        late_t = group["keys_t"] * jnp.exp(last - item["run_row"])
        item["late"] = mm(late_t, item["solved"])
    return items


def solve_groups(groups):
    size = groups[0]["size"]
    rows, cols = iotas(size)
    near = (rows // 2) == (cols // 2)
    for group in groups:
        keys = group["k"]
        keys_t = keys.astype(f32).T
        group["plain_t"] = keys_t.astype(bf16)
        gram = jnp.dot(keys, group["plain_t"], preferred_element_type=f32)
        diag = jnp.where(rows == cols, gram, 0.0)
        s_col = lax.rsqrt(jnp.sum(diag, axis=1, keepdims=True) + epsilon)
        s_row = lax.rsqrt(jnp.sum(diag, axis=0, keepdims=True) + epsilon)
        gram = gram * s_col * s_row
        group["s_row"] = s_row
        group["keys"] = keys.astype(f32) * s_col
        group["keys_t"] = keys_t * s_row
        group["decay"], group["system"], group["inv"] = [], [], []
        for d in range(2):
            rate_col, run_col, run_row = group["gates"][d]
            inside = rows >= cols if d == 0 else rows <= cols
            strict = rows > cols if d == 0 else rows < cols
            decay = jnp.where(inside, jnp.exp(jnp.minimum(run_col - run_row, 0.0)), 0.0)
            group["decay"].append(decay)
            system = jnp.where(strict, gram * decay * rate_col, 0.0)
            group["system"].append(system.astype(bf16))
            group["inv"].append(jnp.where(rows == cols, 1.0, jnp.where(near, -system, 0.0)))
    span = 2
    while span < size:
        row_block, col_block = rows // span, cols // span
        masks = (
            ((row_block % 2) == 1) & (col_block == row_block - 1),
            ((col_block % 2) == 1) & (row_block == col_block - 1),
        )
        masks = [jnp.where(mask, 1.0, 0.0).astype(bf16) for mask in masks]
        firsts = []
        for group in groups:
            group["packed"] = [inv.astype(bf16) for inv in group["inv"]]
            firsts.append([mm(group["system"][d] * masks[d], group["packed"][d]) for d in range(2)])
        for group, first in zip(groups, firsts):
            group["inv"] = [group["inv"][d] - mm(group["packed"][d], first[d]) for d in range(2)]
        span *= 2
    for group in groups:
        values = group["v"].astype(f32)
        group["growth"], group["solved"], group["late"], group["gate"] = [], [], [], []
        for d in range(2):
            rate_col, run_col, run_row = group["gates"][d]
            growth = jnp.exp(run_col)
            both = jnp.concatenate([values * rate_col, group["keys"] * (rate_col * growth)], axis=1)
            solved = mm(group["inv"][d], both).astype(bf16)
            last = run_row[:, size - 1 :] if d == 0 else run_row[:, :1]
            group["growth"].append(growth)
            group["solved"].append(solved)
            group["gate"].append(jnp.exp(last))
            group["late"].append(mm(group["keys_t"] * jnp.exp(last - run_row), solved))


def follow(carry, late, gate, eye):
    fresh = jnp.concatenate([late[:, :HEAD_DIM], (gate - 1.0) * eye - late[:, HEAD_DIM:]], axis=1)
    if carry is None:
        return fresh
    return gate * carry + fresh - mm(late[:, HEAD_DIM:], carry)


def identity():
    rows, cols = iotas(HEAD_DIM)
    return (rows == cols).astype(f32)


def chain(items, d):
    eye = identity()
    carry = None
    for item in items if d == 0 else items[::-1]:
        carry = follow(carry, item["late"], item["gate"], eye)
    return carry


def chain_groups(groups, d):
    eye = identity()
    carry = None
    for group in groups if d == 0 else groups[::-1]:
        group["before", d] = None if carry is None else carry.astype(bf16)
        carry = follow(carry, group["late"][d], group["gate"][d], eye)
    return carry


def outputs(groups, q_of, o_ref, e_ref):
    for group in groups:
        at, size = group["at"], group["size"]
        plain = q_of(at, size)
        queries = plain.astype(f32)
        q_scale = lax.rsqrt(jnp.sum(queries * queries, axis=1, keepdims=True) + epsilon) * HEAD_DIM**-0.5
        queries = queries * q_scale
        score = jnp.dot(plain, group["plain_t"], preferred_element_type=f32) * q_scale * group["s_row"]
        total = None
        for d in range(2):
            weighed = mm(score * group["decay"][d], group["solved"][d])
            out = weighed[:, :HEAD_DIM]
            early = queries * group["growth"][d] - weighed[:, HEAD_DIM:]
            before = group["before", d]
            if before is not None:
                moved = mm(early, before)
                out = out + moved[:, :HEAD_DIM]
                early = early + moved[:, HEAD_DIM:]
            e_ref[at : at + size, d * HEAD_DIM : (d + 1) * HEAD_DIM] = early.astype(bf16)
            total = out if total is None else total + out
        o_ref[at : at + size, :] = total


def on_mesh(sp=None, tp=None):
    return (lax.axis_index("sp") if sp is None else sp, lax.axis_index("tp") if tp is None else tp)


def send(src, dst, send_sem, recv_sem, device):
    return pltpu.make_async_remote_copy(
        src_ref=src,
        dst_ref=dst,
        send_sem=send_sem,
        recv_sem=recv_sem,
        device_id=device,
        device_id_type=pl.DeviceIdType.MESH,
    )


def greet(devices):
    barrier = pltpu.get_barrier_semaphore()
    for device in devices:
        pl.semaphore_signal(barrier, inc=1, device_id=device, device_id_type=pl.DeviceIdType.MESH)


def split_three(x):
    high = x.astype(bf16)
    rest = x - high.astype(f32)
    mid = rest.astype(bf16)
    low = (rest - mid.astype(f32)).astype(bf16)
    return jnp.concatenate([high, mid, low], axis=1)


def advance(state, move, add):
    high = state.astype(bf16)
    low = (state - high.astype(f32)).astype(bf16)
    both = jnp.concatenate([high, low], axis=0)
    moved = jnp.dot(both, move, preferred_element_type=f32)
    rows = state.shape[0]
    return state + add.astype(f32) + moved[:rows] + moved[rows:]


def mixer_kernel(
    sp, tp, heads, tokens, ctx_tokens,
    cond_ref, ctx_cond_ref, gain_ref, head_gain_ref, write_bias_ref, decay_bias_ref, log_rate_ref,
    latent_hbm, context_hbm, shift_hbm, scale_hbm, gate_hbm, query_hbm, key_hbm, value_hbm,
    write_hbm, decay_hbm, out_hbm,
    out_ref,
    rows_v, mod_w, q_w, k_w, v_w, gate_w, out_w, st, stats, mod_v, q_v, k_v, v_v, rate_v, run_v, run_t,
    got_p, blocks, gate_row, o_v, e_v, maps_m, maps_b, got_m, got_b, starts, back, got_o, acc,
    load, sent_p, recv_p, sent_t, recv_t, sent_m, recv_m, sent_b, recv_b, sent_s, recv_s,
    sent_o, recv_dn, recv_up, recv_f, recv_c,
):
    me, col = lax.axis_index("sp"), lax.axis_index("tp")
    items = 2 * heads
    quads = sp // items
    split = 2
    part_rows = HEAD_DIM // split
    core = lax.rem(col, 2)
    width = mod_w.shape[2]
    half = width // 2
    total_tokens = tokens + ctx_tokens
    rings = [lax.rem(me + r, sp) for r in range(1, sp)]
    near = on_mesh(sp=rings[0])
    cross = [lax.rem(col + r, tp) for r in range(1, tp)]
    greet([on_mesh(sp=place) for place in rings] + [on_mesh(tp=place) for place in cross])

    def arrived(spot, sem):
        send(spot, spot, sem, sem, near).wait_recv()

    def left(spot, sem):
        send(spot, spot, sem, sem, near).wait_send()

    def fetch(n, src, dst):
        copy = pltpu.make_async_copy(src, dst, load.at[n])
        copy.start()
        return copy

    gates_rows = write_hbm.shape[0]
    mod_loads = [fetch(n, src, mod_w.at[n]) for n, src in enumerate((shift_hbm, scale_hbm, gate_hbm))]
    row_loads = [
        fetch(3, latent_hbm, rows_v.at[pl.ds(0, tokens)]),
        fetch(4, context_hbm, rows_v.at[pl.ds(tokens, ctx_tokens)]),
    ]
    weight_loads = [
        fetch(5, key_hbm, k_w),
        fetch(6, value_hbm, v_w),
        fetch(7, write_hbm, gate_w.at[pl.ds(0, gates_rows)]),
        fetch(8, decay_hbm, gate_w.at[pl.ds(gates_rows, gates_rows)]),
        fetch(9, query_hbm, q_w),
    ]
    out_load = fetch(10, out_hbm, out_w)

    def silu(ref):
        value = ref[...].astype(f32)
        return value / (1.0 + jnp.exp(-value))

    silus = (silu(cond_ref), silu(ctx_cond_ref))
    quarter = silus[0].shape[0]
    lefts = []
    for part in range(quarter):
        lefts.append(
            jnp.concatenate(
                [silus[0][part : part + 1], silus[1][part : part + 1], jnp.zeros((6, silus[0].shape[1]), f32)], axis=0
            ).astype(bf16)
        )
    silu_rows = jnp.concatenate(lefts, axis=1)
    for copy in mod_loads:
        copy.wait()
    shift = jnp.dot(silu_rows, mod_w[0], preferred_element_type=f32)
    scale = jnp.dot(silu_rows, mod_w[1], preferred_element_type=f32)
    gate = jnp.dot(silu_rows, mod_w[2], preferred_element_type=f32)
    partial = jnp.concatenate([shift[0:2], scale[0:2], gate[0:1], jnp.zeros((3, width), f32)], axis=0)
    got_p[me] = jnp.concatenate([partial[:, :half], partial[:, half:]], axis=0).astype(bf16)
    pl.semaphore_wait(pltpu.get_barrier_semaphore(), len(rings) + len(cross))
    for place in rings:
        send(got_p.at[me], got_p.at[me], sent_p, recv_p, on_mesh(sp=place)).start()

    gate_w[2 * gates_rows :, :] = jnp.zeros((gate_w.shape[0] - 2 * gates_rows, gate_w.shape[1]), bf16)
    for copy in row_loads:
        copy.wait()

    def measure_rows(i, unused):
        at = pl.ds(pl.multiple_of(i * 32, 32), 32)
        values = rows_v[at, :].astype(f32)
        mean = jnp.mean(values * values, axis=1, keepdims=True)
        stats[at, :] = jnp.broadcast_to(lax.rsqrt(mean + epsilon), (32, HEAD_DIM))
        return unused

    lax.fori_loop(0, total_tokens // 32, measure_rows, 0)

    arrived(got_p.at[pl.ds(0, sp - 1)], recv_p)
    total = got_p[0].astype(f32)
    for place in range(1, sp):
        total = total + got_p[place].astype(f32)
    blocks[col] = jnp.concatenate([total[0:4], total[8:12]], axis=0)
    gate_row[...] = jnp.concatenate([total[4:5], total[12:13]], axis=1)
    for place in cross:
        send(blocks.at[col], blocks.at[col], sent_t, recv_t, on_mesh(tp=place)).start()
    arrived(blocks.at[pl.ds(0, tp - 1)], recv_t)
    for place in range(tp):
        at = place * width
        for part in range(2):
            lanes = slice(at + part * half, at + (part + 1) * half)
            four = blocks[place, 4 * part : 4 * part + 4, :]
            scaled = (1.0 + four[2:4]) * gain_ref[:, lanes]
            for which in range(2):
                st[which, :, lanes] = jnp.broadcast_to(four[which : which + 1], (8, half))
                st[2 + which, :, lanes] = jnp.broadcast_to(scaled[which : which + 1], (8, half))

    def modulate(first, count, which):
        def step(i, unused):
            at = pl.ds(pl.multiple_of(first + i * 32, 32), 32)
            root = stats[at, :]
            for lane_at in range(0, rows_v.shape[1], HEAD_DIM):
                lanes = slice(lane_at, lane_at + HEAD_DIM)
                values = rows_v[at, lanes].astype(f32) * root
                shift, scale = st[which, :, lanes], st[2 + which, :, lanes]
                parts = [values[n : n + 8] * scale + shift for n in range(0, 32, 8)]
                mod_v[at, lanes] = jnp.concatenate(parts, axis=0).astype(bf16)
            return unused

        lax.fori_loop(0, count // 32, step, 0)

    modulate(tokens, ctx_tokens, 1)
    modulate(0, tokens, 0)
    for copy in weight_loads:
        copy.wait()
    pre = mm_t(mod_v[...], gate_w[...]).astype(bf16).astype(f32)
    k_v[...] = jnp.dot(mod_v[...], k_w[...], preferred_element_type=f32).astype(bf16)
    v_v[...] = jnp.dot(mod_v[...], v_w[...], preferred_element_type=f32).astype(bf16)

    all_heads = gates_rows // 2
    first_head = col * heads
    pre = pltpu.roll(pre, HEAD_DIM - first_head, 1)
    lane = lax.broadcasted_iota(jnp.int32, (1, HEAD_DIM), 1)
    write_bias = jnp.zeros((1, HEAD_DIM), f32)
    decay_bias = jnp.zeros((1, HEAD_DIM), f32)
    log_rate = jnp.zeros((1, HEAD_DIM), f32)
    for d in range(2):
        for head in range(heads):
            spot = d * all_heads + head
            write_bias = jnp.where(lane == spot, write_bias_ref[d, first_head + head], write_bias)
            decay_bias = jnp.where(lane == spot + gates_rows, decay_bias_ref[d, first_head + head], decay_bias)
            log_rate = jnp.where(lane == spot + gates_rows, log_rate_ref[d, first_head + head], log_rate)
    rate_v[...] = jax.nn.sigmoid(pre + write_bias)
    raised = pre + decay_bias
    soft = jnp.maximum(raised, 0.0) + jnp.log1p(jnp.exp(-jnp.abs(raised)))
    log_decay = -jnp.exp(log_rate) * soft
    lat, ctx = spans(tokens, ctx_tokens)
    for n, (at, size) in enumerate(lat + ctx):
        rows, cols = iotas(size)
        lower = (rows >= cols).astype(f32)
        upper = (rows <= cols).astype(f32)
        sums = jnp.dot(
            jnp.concatenate([lower, upper], axis=0).astype(bf16),
            split_three(log_decay[at : at + size]),
            preferred_element_type=f32,
        )
        sums = sums[:, :HEAD_DIM] + sums[:, HEAD_DIM : 2 * HEAD_DIM] + sums[:, 2 * HEAD_DIM :]
        running = jnp.where(lane < gates_rows + all_heads, sums[:size], sums[size:])
        run_v[at : at + size, :] = running
        run_t[n, :, :size] = running.T

    def group_of(n, at, size, head):
        lanes = slice(head * HEAD_DIM, (head + 1) * HEAD_DIM)
        gates = []
        for d in range(2):
            spot = d * all_heads + head
            deep = spot + gates_rows
            gates.append(
                (
                    rate_v[at : at + size, spot : spot + 1],
                    run_v[at : at + size, deep : deep + 1],
                    run_t[n, deep : deep + 1, :size],
                )
            )
        return dict(
            at=at,
            size=size,
            k=k_v[at : at + size, lanes],
            v=v_v[at : at + size, lanes],
            gates=gates,
        )

    def keep(part, item, carry):
        maps_b[part, item] = carry[:, :HEAD_DIM].T.astype(bf16)
        maps_m[part, item] = carry[:, HEAD_DIM:].T.astype(bf16)

    def owner_of(item, piece):
        return item * quads + 2 * piece + lax.rem(item + core, 2)

    my_item, my_part = me // quads, lax.rem(me, quads) // 2
    owning = lax.rem(me, 2) == lax.rem(my_item + core, 2)
    reverse = lax.rem(my_item, 2)

    def ship(part, item, piece):
        owner = owner_of(item, piece)

        @pl.when(owner != me)
        def _():
            send(
                maps_m.at[part, item], got_m.at[part, me], sent_m.at[part], recv_m.at[part], on_mesh(sp=owner)
            ).start()
            send(
                maps_b.at[part, item, pl.ds(piece * part_rows, part_rows)],
                got_b.at[part, me], sent_b.at[part], recv_b.at[part], on_mesh(sp=owner),
            ).start()

    def ship_head(part, head):
        for item in (2 * head, 2 * head + 1):
            for piece in range(split):
                ship(part, item, piece)

    def keep_own(part):
        got_m[part, me] = maps_m[part, my_item]
        got_b[part, me] = maps_b[part, my_item, pl.ds(pl.multiple_of(my_part * part_rows, part_rows), part_rows), :]

    ctx_groups = []
    for head in range(heads):
        for n, (at, size) in enumerate(ctx):
            ctx_groups.append(group_of(len(lat) + n, at, size, head))
    done = prepare(ctx_groups)
    each = 2 * len(ctx)
    for head in range(heads):
        for d in range(2):
            chosen = [i for i in done[head * each : (head + 1) * each] if i["d"] == d]
            keep(0, 2 * head + d, chain(chosen, d))
    for head in range(heads):
        ship_head(0, head)
    latents = []
    for head in range(heads):
        latents.append([group_of(n, at, size, head) for n, (at, size) in enumerate(lat)])
        solve_groups(latents[head])
        for d in range(2):
            keep(1, 2 * head + d, chain_groups(latents[head], d))
        ship_head(1, head)
    q_v[...] = jnp.dot(mod_v[0:tokens, :], q_w[...], preferred_element_type=f32).astype(bf16)
    for head in range(heads):

        def q_of(at, size):
            return q_v[at : at + size, head * HEAD_DIM : (head + 1) * HEAD_DIM]

        outputs(latents[head], q_of, o_v.at[head], e_v.at[head])

    def arrive(part):
        arrived(got_m.at[part, pl.ds(0, sp - 1)], recv_m.at[part])
        arrived(got_b.at[part, pl.ds(0, sp - 1)], recv_b.at[part])

    def give_back(place):
        return send(
            starts.at[place], back.at[my_item * split + my_part], sent_s, recv_s.at[my_item // 2], on_mesh(sp=place)
        )

    @pl.when(owning)
    def _():
        keep_own(0)
        keep_own(1)
        arrive(0)
        state = jnp.zeros((part_rows, HEAD_DIM), f32)
        for step in range(sp):
            place = step + reverse * (sp - 1 - 2 * step)
            state = advance(state, got_m[0, place], got_b[0, place])
        arrive(1)
        for step in range(sp):
            place = step + reverse * (sp - 1 - 2 * step)
            starts[place] = state.astype(bf16)
            if step < sp - 1:
                state = advance(state, got_m[1, place], got_b[1, place])
        for place in rings:
            give_back(place).start()
        back[my_item * split + my_part] = starts[me]

    chips = tp // 2
    chip = col // 2
    partner = col + 1 - 2 * core
    up = lax.rem(chip + 1, chips) * 2 + core
    down = lax.rem(chip + chips - 1, chips) * 2 + core
    far = lax.rem(chip + 2, chips) * 2 + core
    mid = tokens // 2

    def piece(head, place, part):
        return got_o.at[head, place, pl.ds(part * mid, mid)]

    def to_up(head, part):
        return send(
            piece(head, col, part), piece(head, col, part), sent_o.at[head], recv_dn.at[head, part],
            on_mesh(tp=up),
        )

    def to_down(head, part):
        return send(
            piece(head, col, part), piece(head, col, part), sent_o.at[head], recv_up.at[head, part],
            on_mesh(tp=down),
        )

    def forward(head, part):
        src, dst = (down, up) if part == 0 else (up, down)
        return send(
            piece(head, src, part), piece(head, src, part), sent_o.at[head], recv_f.at[head, part],
            on_mesh(tp=dst),
        )

    def relay(head, n, spot):
        return send(spot, spot, sent_o.at[head], recv_c.at[head, n], on_mesh(tp=partner))

    def finish_head(head):
        half_items = [2 * head, 2 * head + 1]
        mine = owning & (my_item // 2 == head)

        @pl.when(mine)
        def _():
            arrived(back.at[pl.ds(0, 2 * split - 1)], recv_s.at[head])

        @pl.when(jnp.logical_not(mine))
        def _():
            arrived(back.at[pl.ds(0, 2 * split)], recv_s.at[head])

        pair = [back[item * split : (item + 1) * split].reshape(HEAD_DIM, HEAD_DIM) for item in half_items]
        combined = o_v[head] + mm_t(e_v[head], jnp.concatenate(pair, axis=1))
        norm = lax.rsqrt(jnp.mean(combined * combined, axis=1, keepdims=True) + epsilon)
        got_o[head, col] = (combined * norm * head_gain_ref[...]).astype(bf16)
        for copy in (to_up(head, 0), to_down(head, 1), to_up(head, 1), to_down(head, 0)):
            copy.start()
        relay(head, 0, got_o.at[head, col]).start()

    def near_arrivals(head):
        waits = (
            (down, 0, recv_dn, 1, True),
            (up, 1, recv_up, 2, True),
            (down, 1, recv_dn, 1, False),
            (up, 0, recv_up, 2, False),
        )
        for place, part, sems, n, onward in waits:
            spot = piece(head, place, part)
            arrived(spot, sems.at[head, part])
            if onward:
                forward(head, part).start()
            relay(head, n, spot).start()

    def far_arrivals(head):
        for part in range(2):
            spot = piece(head, far, part)
            arrived(spot, recv_f.at[head, part])
            relay(head, 3, spot).start()

    def from_partner(head, n):
        arrived(got_o.at[head, 0], recv_c.at[head, n])

    def add(head, place, first=False):
        even = place - core
        lanes = jnp.concatenate([got_o[head, even], got_o[head, even + 1]], axis=1)
        depth = heads * HEAD_DIM
        weights = jnp.concatenate(
            [
                out_w[pl.ds(pl.multiple_of((even + n) * depth + head * HEAD_DIM, HEAD_DIM), HEAD_DIM), :]
                for n in range(2)
            ],
            axis=0,
        )
        part = jnp.dot(lanes, weights, preferred_element_type=f32)
        acc[...] = part if first else acc[...] + part

    def near_matmuls(head):
        from_partner(head, 0)
        add(head, col, head == 0)
        from_partner(head, 1)
        add(head, down)
        from_partner(head, 2)
        add(head, up)

    def far_matmuls(head):
        from_partner(head, 3)
        add(head, far)

    out_load.wait()
    finish_head(0)
    near_arrivals(0)
    for head in range(1, heads):
        finish_head(head)
        far_arrivals(head - 1)
        near_matmuls(head - 1)
        far_matmuls(head - 1)
        near_arrivals(head)
    far_arrivals(heads - 1)
    near_matmuls(heads - 1)
    far_matmuls(heads - 1)
    lanes = pl.ds(pl.multiple_of(col * width, width), width)
    out_ref[...] = rows_v[0:tokens, lanes].astype(f32) + gate_row[...] * acc[...]
    left(got_p.at[pl.ds(0, sp - 1)], sent_p)
    left(blocks.at[pl.ds(0, tp - 1)], sent_t)

    def sent_maps(count):
        for part in range(2):
            left(got_m.at[part, pl.ds(0, count)], sent_m.at[part])
            left(got_b.at[part, pl.ds(0, count)], sent_b.at[part])

    @pl.when(owning)
    def _():
        sent_maps(items * split - 1)
        left(starts.at[pl.ds(0, sp - 1)], sent_s)

    @pl.when(jnp.logical_not(owning))
    def _():
        sent_maps(items * split)

    for head in range(heads):
        left(got_o.at[head, pl.ds(0, tp - 1)], sent_o.at[head])


def body(
    latent,
    context,
    condition,
    context_condition,
    shift_weight,
    scale_weight,
    gate_weight,
    norm_gain,
    query_weight,
    key_weight,
    value_weight,
    write_weight,
    decay_weight,
    write_bias,
    decay_bias,
    log_rate,
    head_gain,
    out_weight,
):
    sp, tp = lax.axis_size("sp"), lax.axis_size("tp")
    inner = query_weight.shape[1]
    heads = inner // HEAD_DIM
    tokens, ctx_tokens = latent.shape[0], context.shape[0]
    total = tokens + ctx_tokens
    features = latent.shape[1]
    width = shift_weight.shape[1]
    items = 2 * heads
    split = 2
    rows = HEAD_DIM // split
    chunks = sum(len(part) for part in spans(tokens, ctx_tokens))
    vmem = pl.BlockSpec(memory_space=pltpu.VMEM)
    smem = pl.BlockSpec(memory_space=pltpu.SMEM)
    anywhere = pl.BlockSpec(memory_space=pltpu.HBM)
    dma = pltpu.SemaphoreType.DMA
    flat = [jnp.transpose(w, (1, 2, 0)).reshape(-1, features) for w in (write_weight, decay_weight)]
    updated = pl.pallas_call(
        functools.partial(mixer_kernel, sp, tp, heads, tokens, ctx_tokens),
        in_specs=[vmem] * 4 + [smem] * 3 + [anywhere] * 11,
        out_specs=vmem,
        out_shape=jax.ShapeDtypeStruct((tokens, width), f32),
        scratch_shapes=[
            pltpu.VMEM((total, features), bf16),
            pltpu.VMEM((3,) + shift_weight.shape, bf16),
            pltpu.VMEM(query_weight.shape, bf16),
            pltpu.VMEM(key_weight.shape, bf16),
            pltpu.VMEM(value_weight.shape, bf16),
            pltpu.VMEM((HEAD_DIM, features), bf16),
            pltpu.VMEM(out_weight.shape, bf16),
            pltpu.VMEM((4, 8, features), f32),
            pltpu.VMEM((total, HEAD_DIM), f32),
            pltpu.VMEM((total, features), bf16),
            pltpu.VMEM((tokens, inner), bf16),
            pltpu.VMEM((total, inner), bf16),
            pltpu.VMEM((total, inner), bf16),
            pltpu.VMEM((total, HEAD_DIM), f32),
            pltpu.VMEM((total, HEAD_DIM), f32),
            pltpu.VMEM((chunks, HEAD_DIM, CHUNK), f32),
            pltpu.VMEM((sp, 16, width // 2), bf16),
            pltpu.VMEM((tp, 8, width // 2), f32),
            pltpu.VMEM((1, width), f32),
            pltpu.VMEM((heads, tokens, HEAD_DIM), f32),
            pltpu.VMEM((heads, tokens, 2 * HEAD_DIM), bf16),
            pltpu.VMEM((2, items, HEAD_DIM, HEAD_DIM), bf16),
            pltpu.VMEM((2, items, HEAD_DIM, HEAD_DIM), bf16),
            pltpu.VMEM((2, sp, HEAD_DIM, HEAD_DIM), bf16),
            pltpu.VMEM((2, sp, rows, HEAD_DIM), bf16),
            pltpu.VMEM((sp, rows, HEAD_DIM), bf16),
            pltpu.VMEM((items * split, rows, HEAD_DIM), bf16),
            pltpu.VMEM((heads, tp, tokens, HEAD_DIM), bf16),
            pltpu.VMEM((tokens, width), f32),
            dma((11,)),
            dma,
            dma,
            dma,
            dma,
            dma((2,)),
            dma((2,)),
            dma((2,)),
            dma((2,)),
            dma,
            dma((heads,)),
            dma((heads,)),
            dma((heads, 2)),
            dma((heads, 2)),
            dma((heads, 2)),
            dma((heads, 4)),
        ],
        compiler_params=pltpu.CompilerParams(
            collective_id=0, has_side_effects=True, vmem_limit_bytes=58 * 1024 * 1024
        ),
        name="mixer",
    )(
        condition.reshape(-1, HEAD_DIM),
        context_condition.reshape(-1, HEAD_DIM),
        norm_gain[None, :],
        head_gain[None, :],
        write_bias,
        decay_bias,
        log_rate,
        latent,
        context,
        shift_weight,
        scale_weight,
        gate_weight,
        query_weight,
        key_weight,
        value_weight,
        flat[0],
        flat[1],
        out_weight,
    )
    return updated.astype(bf16)


def solution(mesh):
    placed = (
        P("sp", None),
        P("sp", None),
        P("sp"),
        P("sp"),
        P("sp", "tp"),
        P("sp", "tp"),
        P("sp", "tp"),
        P(),
        P(None, "tp"),
        P(None, "tp"),
        P(None, "tp"),
        P(),
        P(),
        P(),
        P(),
        P(),
        P(),
        P(None, "tp"),
    )
    return jax.shard_map(body, mesh=mesh, in_specs=placed, out_specs=P("sp", "tp"), check_vma=False)
```

```python
import functools

import jax
import jax.numpy as jnp
from jax import lax
from jax.experimental import pallas as pl
from jax.experimental.pallas import tpu as pltpu
from jax.sharding import PartitionSpec as P

HEAD_DIM = 128
CHUNK = 128
epsilon = 0.0001
bf16 = jnp.bfloat16
f32 = jnp.float32


def mm(a, b):
    return jnp.dot(a.astype(bf16), b.astype(bf16), preferred_element_type=f32)


def mm_t(a, b):
    return lax.dot_general(a, b, (((1,), (1,)), ((), ())), preferred_element_type=f32)


def spans(tokens, ctx_tokens):
    size = min(CHUNK, tokens)
    lat = [(at, size) for at in range(0, tokens, size)]
    ctx_size = min(CHUNK, ctx_tokens)
    ctx = [(tokens + at, ctx_size) for at in range(0, ctx_tokens, ctx_size)]
    return lat, ctx


def iotas(size):
    rows = lax.broadcasted_iota(jnp.int32, (size, size), 0)
    cols = lax.broadcasted_iota(jnp.int32, (size, size), 1)
    return rows, cols


def prepare(groups):
    items = []
    for group in groups:
        size = group["size"]
        rows, cols = iotas(size)
        keys = group["k"]
        keys_t = keys.astype(f32).T
        gram = jnp.dot(keys, keys_t.astype(bf16), preferred_element_type=f32)
        diag = jnp.where(rows == cols, gram, 0.0)
        s_col = lax.rsqrt(jnp.sum(diag, axis=1, keepdims=True) + epsilon)
        s_row = lax.rsqrt(jnp.sum(diag, axis=0, keepdims=True) + epsilon)
        gram = gram * s_col * s_row
        group["keys"] = keys.astype(f32) * s_col
        group["keys_t"] = keys_t * s_row
        group["values"] = group["v"].astype(f32)
        for d in range(2):
            rate_col, run_col, run_row = group["gates"][d]
            inside = rows >= cols if d == 0 else rows <= cols
            strict = rows > cols if d == 0 else rows < cols
            decay = jnp.where(inside, jnp.exp(jnp.minimum(run_col - run_row, 0.0)), 0.0)
            system = jnp.where(strict, gram * decay * rate_col, 0.0)
            item = dict(group=group, size=size, d=d, rate_col=rate_col, run_col=run_col, run_row=run_row)
            item["system"] = system
            near = (rows // 2) == (cols // 2)
            item["inv"] = jnp.where(rows == cols, 1.0, jnp.where(near, -system, 0.0))
            items.append(item)
    span = 2
    while span < max(item["size"] for item in items):
        firsts = []
        for item in items:
            if span >= item["size"]:
                firsts.append(None)
                continue
            rows, cols = iotas(item["size"])
            rows, cols = rows // span, cols // span
            if item["d"] == 0:
                mask = ((rows % 2) == 1) & (cols == rows - 1)
            else:
                mask = ((cols % 2) == 1) & (rows == cols - 1)
            firsts.append(mm(jnp.where(mask, item["system"], 0.0), item["inv"]))
        for item, first in zip(items, firsts):
            if first is not None:
                item["inv"] = item["inv"] - mm(item["inv"], first)
        span *= 2
    for item in items:
        group = item["group"]
        growth = jnp.exp(item["run_col"])
        both = jnp.concatenate(
            [group["values"] * item["rate_col"], group["keys"] * (item["rate_col"] * growth)], axis=1
        )
        item["solved"] = mm(item["inv"], both)
        last = item["run_row"][:, item["size"] - 1 :] if item["d"] == 0 else item["run_row"][:, :1]
        item["gate"] = jnp.exp(last)
        late_t = group["keys_t"] * jnp.exp(last - item["run_row"])
        item["late"] = mm(late_t, item["solved"])
    return items


def solve_groups(groups):
    size = groups[0]["size"]
    rows, cols = iotas(size)
    near = (rows // 2) == (cols // 2)
    for group in groups:
        keys = group["k"]
        keys_t = keys.astype(f32).T
        group["plain_t"] = keys_t.astype(bf16)
        gram = jnp.dot(keys, group["plain_t"], preferred_element_type=f32)
        diag = jnp.where(rows == cols, gram, 0.0)
        s_col = lax.rsqrt(jnp.sum(diag, axis=1, keepdims=True) + epsilon)
        s_row = lax.rsqrt(jnp.sum(diag, axis=0, keepdims=True) + epsilon)
        gram = gram * s_col * s_row
        group["s_row"] = s_row
        group["keys"] = keys.astype(f32) * s_col
        group["keys_t"] = keys_t * s_row
        group["decay"], group["system"], group["inv"] = [], [], []
        for d in range(2):
            rate_col, run_col, run_row = group["gates"][d]
            inside = rows >= cols if d == 0 else rows <= cols
            strict = rows > cols if d == 0 else rows < cols
            decay = jnp.where(inside, jnp.exp(jnp.minimum(run_col - run_row, 0.0)), 0.0)
            group["decay"].append(decay)
            system = jnp.where(strict, gram * decay * rate_col, 0.0)
            group["system"].append(system.astype(bf16))
            group["inv"].append(jnp.where(rows == cols, 1.0, jnp.where(near, -system, 0.0)))
    span = 2
    while span < size:
        row_block, col_block = rows // span, cols // span
        masks = (
            ((row_block % 2) == 1) & (col_block == row_block - 1),
            ((col_block % 2) == 1) & (row_block == col_block - 1),
        )
        masks = [jnp.where(mask, 1.0, 0.0).astype(bf16) for mask in masks]
        firsts = []
        for group in groups:
            group["packed"] = [inv.astype(bf16) for inv in group["inv"]]
            firsts.append([mm(group["system"][d] * masks[d], group["packed"][d]) for d in range(2)])
        for group, first in zip(groups, firsts):
            group["inv"] = [group["inv"][d] - mm(group["packed"][d], first[d]) for d in range(2)]
        span *= 2
    for group in groups:
        values = group["v"].astype(f32)
        group["growth"], group["solved"], group["late"], group["gate"] = [], [], [], []
        for d in range(2):
            rate_col, run_col, run_row = group["gates"][d]
            growth = jnp.exp(run_col)
            both = jnp.concatenate([values * rate_col, group["keys"] * (rate_col * growth)], axis=1)
            solved = mm(group["inv"][d], both).astype(bf16)
            last = run_row[:, size - 1 :] if d == 0 else run_row[:, :1]
            group["growth"].append(growth)
            group["solved"].append(solved)
            group["gate"].append(jnp.exp(last))
            group["late"].append(mm(group["keys_t"] * jnp.exp(last - run_row), solved))


def follow(carry, late, gate, eye):
    fresh = jnp.concatenate([late[:, :HEAD_DIM], (gate - 1.0) * eye - late[:, HEAD_DIM:]], axis=1)
    if carry is None:
        return fresh
    return gate * carry + fresh - mm(late[:, HEAD_DIM:], carry)


def identity():
    rows, cols = iotas(HEAD_DIM)
    return (rows == cols).astype(f32)


def chain(items, d):
    eye = identity()
    carry = None
    for item in items if d == 0 else items[::-1]:
        carry = follow(carry, item["late"], item["gate"], eye)
    return carry


def chain_groups(groups, d):
    eye = identity()
    carry = None
    for group in groups if d == 0 else groups[::-1]:
        group["before", d] = None if carry is None else carry.astype(bf16)
        carry = follow(carry, group["late"][d], group["gate"][d], eye)
    return carry


def outputs(groups, q_of, o_ref, e_ref):
    for group in groups:
        at, size = group["at"], group["size"]
        plain = q_of(at, size)
        queries = plain.astype(f32)
        q_scale = lax.rsqrt(jnp.sum(queries * queries, axis=1, keepdims=True) + epsilon) * HEAD_DIM**-0.5
        queries = queries * q_scale
        score = jnp.dot(plain, group["plain_t"], preferred_element_type=f32) * q_scale * group["s_row"]
        total = None
        for d in range(2):
            weighed = mm(score * group["decay"][d], group["solved"][d])
            out = weighed[:, :HEAD_DIM]
            early = queries * group["growth"][d] - weighed[:, HEAD_DIM:]
            before = group["before", d]
            if before is not None:
                moved = mm(early, before)
                out = out + moved[:, :HEAD_DIM]
                early = early + moved[:, HEAD_DIM:]
            e_ref[at : at + size, d * HEAD_DIM : (d + 1) * HEAD_DIM] = early.astype(bf16)
            total = out if total is None else total + out
        o_ref[at : at + size, :] = total


def on_mesh(sp=None, tp=None):
    return (lax.axis_index("sp") if sp is None else sp, lax.axis_index("tp") if tp is None else tp)


def send(src, dst, send_sem, recv_sem, device):
    return pltpu.make_async_remote_copy(
        src_ref=src,
        dst_ref=dst,
        send_sem=send_sem,
        recv_sem=recv_sem,
        device_id=device,
        device_id_type=pl.DeviceIdType.MESH,
    )


def greet(devices):
    barrier = pltpu.get_barrier_semaphore()
    for device in devices:
        pl.semaphore_signal(barrier, inc=1, device_id=device, device_id_type=pl.DeviceIdType.MESH)


def split_three(x):
    high = x.astype(bf16)
    rest = x - high.astype(f32)
    mid = rest.astype(bf16)
    low = (rest - mid.astype(f32)).astype(bf16)
    return jnp.concatenate([high, mid, low], axis=1)


def advance(state, move, add):
    high = state.astype(bf16)
    low = (state - high.astype(f32)).astype(bf16)
    both = jnp.concatenate([high, low], axis=0)
    moved = jnp.dot(both, move, preferred_element_type=f32)
    rows = state.shape[0]
    return state + add.astype(f32) + moved[:rows] + moved[rows:]


def mixer_kernel(
    sp, tp, heads, tokens, ctx_tokens,
    cond_ref, ctx_cond_ref, gain_ref, head_gain_ref, write_bias_ref, decay_bias_ref, log_rate_ref,
    latent_hbm, context_hbm, shift_hbm, scale_hbm, gate_hbm, query_hbm, key_hbm, value_hbm,
    write_hbm, decay_hbm, out_hbm,
    out_ref,
    rows_v, mod_w, q_w, k_w, v_w, gate_w, out_w, st, stats, mod_v, q_v, k_v, v_v, rate_v, run_v, run_t,
    got_p, blocks, gate_row, ctx_state, o_v, e_v, maps_m, maps_b, got_m, got_b, starts, back, got_o, acc,
    load, sent_p, recv_p, sent_t, recv_t, sent_m, recv_m, sent_b, recv_b, sent_s, recv_s,
    sent_o, recv_dn, recv_up, recv_f, recv_c,
):
    me, col = lax.axis_index("sp"), lax.axis_index("tp")
    items = 2 * heads
    quads = sp // items
    split = 2
    part_rows = HEAD_DIM // split
    core = lax.rem(col, 2)
    chips = tp // 2
    chip = col // 2
    partner = col + 1 - 2 * core
    up = lax.rem(chip + 1, chips) * 2 + core
    down = lax.rem(chip + chips - 1, chips) * 2 + core
    far = lax.rem(chip + 2, chips) * 2 + core
    width = mod_w.shape[2]
    half = width // 2
    total_tokens = tokens + ctx_tokens
    rings = [lax.rem(me + r, sp) for r in range(1, sp)]
    near = on_mesh(sp=rings[0])
    cross = [lax.rem(col + r, tp) for r in range(1, tp)]
    greet([on_mesh(sp=place) for place in rings] + [on_mesh(tp=place) for place in cross])

    def arrived(spot, sem):
        send(spot, spot, sem, sem, near).wait_recv()

    def left(spot, sem):
        send(spot, spot, sem, sem, near).wait_send()

    def fetch(n, src, dst):
        copy = pltpu.make_async_copy(src, dst, load.at[n])
        copy.start()
        return copy

    gates_rows = write_hbm.shape[0]
    mod_loads = [fetch(n, src, mod_w.at[n]) for n, src in enumerate((shift_hbm, scale_hbm, gate_hbm))]
    row_loads = [
        fetch(3, latent_hbm, rows_v.at[pl.ds(0, tokens)]),
        fetch(4, context_hbm, rows_v.at[pl.ds(tokens, ctx_tokens)]),
    ]
    weight_loads = [
        fetch(5, key_hbm, k_w),
        fetch(6, value_hbm, v_w),
        fetch(7, write_hbm, gate_w.at[pl.ds(0, gates_rows)]),
        fetch(8, decay_hbm, gate_w.at[pl.ds(gates_rows, gates_rows)]),
        fetch(9, query_hbm, q_w),
    ]
    out_load = fetch(10, out_hbm, out_w)

    def silu(ref):
        value = ref[...].astype(f32)
        return value / (1.0 + jnp.exp(-value))

    silus = (silu(cond_ref), silu(ctx_cond_ref))
    quarter = silus[0].shape[0]
    lefts = []
    for part in range(quarter):
        lefts.append(
            jnp.concatenate(
                [silus[0][part : part + 1], silus[1][part : part + 1], jnp.zeros((6, silus[0].shape[1]), f32)], axis=0
            ).astype(bf16)
        )
    silu_rows = jnp.concatenate(lefts, axis=1)
    for copy in mod_loads:
        copy.wait()
    shift = jnp.dot(silu_rows, mod_w[0], preferred_element_type=f32)
    scale = jnp.dot(silu_rows, mod_w[1], preferred_element_type=f32)
    gate = jnp.dot(silu_rows, mod_w[2], preferred_element_type=f32)
    partial = jnp.concatenate([shift[0:2], scale[0:2], gate[0:1], jnp.zeros((3, width), f32)], axis=0)
    got_p[me] = jnp.concatenate([partial[:, :half], partial[:, half:]], axis=0).astype(bf16)
    pl.semaphore_wait(pltpu.get_barrier_semaphore(), len(rings) + len(cross))
    for place in rings:
        send(got_p.at[me], got_p.at[me], sent_p, recv_p, on_mesh(sp=place)).start()

    gate_w[2 * gates_rows :, :] = jnp.zeros((gate_w.shape[0] - 2 * gates_rows, gate_w.shape[1]), bf16)
    for copy in row_loads:
        copy.wait()

    def measure_rows(i, unused):
        at = pl.ds(pl.multiple_of(i * 32, 32), 32)
        values = rows_v[at, :].astype(f32)
        mean = jnp.mean(values * values, axis=1, keepdims=True)
        stats[at, :] = jnp.broadcast_to(lax.rsqrt(mean + epsilon), (32, HEAD_DIM))
        return unused

    lax.fori_loop(0, total_tokens // 32, measure_rows, 0)

    arrived(got_p.at[pl.ds(0, sp - 1)], recv_p)
    total = got_p[0].astype(f32)
    for place in range(1, sp):
        total = total + got_p[place].astype(f32)
    blocks[col] = jnp.concatenate([total[0:4], total[8:12]], axis=0)
    gate_row[...] = jnp.concatenate([total[4:5], total[12:13]], axis=1)
    for place in cross:
        send(blocks.at[col], blocks.at[col], sent_t, recv_t, on_mesh(tp=place)).start()
    arrived(blocks.at[pl.ds(0, tp - 1)], recv_t)
    for place in range(tp):
        at = place * width
        for part in range(2):
            lanes = slice(at + part * half, at + (part + 1) * half)
            four = blocks[place, 4 * part : 4 * part + 4, :]
            scaled = (1.0 + four[2:4]) * gain_ref[:, lanes]
            for which in range(2):
                st[which, :, lanes] = jnp.broadcast_to(four[which : which + 1], (8, half))
                st[2 + which, :, lanes] = jnp.broadcast_to(scaled[which : which + 1], (8, half))

    def modulate(first, count, which):
        def step(i, unused):
            at = pl.ds(pl.multiple_of(first + i * 32, 32), 32)
            root = stats[at, :]
            for lane_at in range(0, rows_v.shape[1], HEAD_DIM):
                lanes = slice(lane_at, lane_at + HEAD_DIM)
                values = rows_v[at, lanes].astype(f32) * root
                shift, scale = st[which, :, lanes], st[2 + which, :, lanes]
                parts = [values[n : n + 8] * scale + shift for n in range(0, 32, 8)]
                mod_v[at, lanes] = jnp.concatenate(parts, axis=0).astype(bf16)
            return unused

        lax.fori_loop(0, count // 32, step, 0)

    modulate(tokens, ctx_tokens, 1)
    modulate(0, tokens, 0)
    for copy in weight_loads:
        copy.wait()
    pre = mm_t(mod_v[...], gate_w[...]).astype(bf16).astype(f32)
    k_v[...] = jnp.dot(mod_v[...], k_w[...], preferred_element_type=f32).astype(bf16)
    v_v[...] = jnp.dot(mod_v[...], v_w[...], preferred_element_type=f32).astype(bf16)

    all_heads = gates_rows // 2
    first_head = col * heads
    pre = pltpu.roll(pre, HEAD_DIM - first_head, 1)
    lane = lax.broadcasted_iota(jnp.int32, (1, HEAD_DIM), 1)
    write_bias = jnp.zeros((1, HEAD_DIM), f32)
    decay_bias = jnp.zeros((1, HEAD_DIM), f32)
    log_rate = jnp.zeros((1, HEAD_DIM), f32)
    for d in range(2):
        for head in range(heads):
            spot = d * all_heads + head
            write_bias = jnp.where(lane == spot, write_bias_ref[d, first_head + head], write_bias)
            decay_bias = jnp.where(lane == spot + gates_rows, decay_bias_ref[d, first_head + head], decay_bias)
            log_rate = jnp.where(lane == spot + gates_rows, log_rate_ref[d, first_head + head], log_rate)
    rate_v[...] = jax.nn.sigmoid(pre + write_bias)
    raised = pre + decay_bias
    soft = jnp.maximum(raised, 0.0) + jnp.log1p(jnp.exp(-jnp.abs(raised)))
    log_decay = -jnp.exp(log_rate) * soft
    lat, ctx = spans(tokens, ctx_tokens)
    for n, (at, size) in enumerate(lat + ctx):
        rows, cols = iotas(size)
        lower = (rows >= cols).astype(f32)
        upper = (rows <= cols).astype(f32)
        sums = jnp.dot(
            jnp.concatenate([lower, upper], axis=0).astype(bf16),
            split_three(log_decay[at : at + size]),
            preferred_element_type=f32,
        )
        sums = sums[:, :HEAD_DIM] + sums[:, HEAD_DIM : 2 * HEAD_DIM] + sums[:, 2 * HEAD_DIM :]
        running = jnp.where(lane < gates_rows + all_heads, sums[:size], sums[size:])
        run_v[at : at + size, :] = running
        run_t[n, :, :size] = running.T

    def group_of(n, at, size, head):
        lanes = slice(head * HEAD_DIM, (head + 1) * HEAD_DIM)
        gates = []
        for d in range(2):
            spot = d * all_heads + head
            deep = spot + gates_rows
            gates.append(
                (
                    rate_v[at : at + size, spot : spot + 1],
                    run_v[at : at + size, deep : deep + 1],
                    run_t[n, deep : deep + 1, :size],
                )
            )
        return dict(
            at=at,
            size=size,
            k=k_v[at : at + size, lanes],
            v=v_v[at : at + size, lanes],
            gates=gates,
        )

    def keep(part, item, carry):
        maps_b[part, item] = carry[:, :HEAD_DIM].T.astype(bf16)
        maps_m[part, item] = carry[:, HEAD_DIM:].T.astype(bf16)

    def owner_of(item, piece):
        return item * quads + 2 * piece + lax.rem(item + core, 2)

    my_item, my_part = me // quads, lax.rem(me, quads) // 2
    owning = lax.rem(me, 2) == lax.rem(my_item + core, 2)
    reverse = lax.rem(my_item, 2)

    def ship(part, item, piece):
        owner = owner_of(item, piece)

        @pl.when(owner != me)
        def _():
            send(
                maps_m.at[part, item], got_m.at[part, me], sent_m.at[part], recv_m.at[part], on_mesh(sp=owner)
            ).start()
            send(
                maps_b.at[part, item, pl.ds(piece * part_rows, part_rows)],
                got_b.at[part, me], sent_b.at[part], recv_b.at[part], on_mesh(sp=owner),
            ).start()

    def ship_head(part, head):
        for item in (2 * head, 2 * head + 1):
            for piece in range(split):
                ship(part, item, piece)

    def keep_own(part):
        got_m[part, me] = maps_m[part, my_item]
        got_b[part, me] = maps_b[part, my_item, pl.ds(pl.multiple_of(my_part * part_rows, part_rows), part_rows), :]

    ctx_groups = []
    for head in range(heads):
        for n, (at, size) in enumerate(ctx):
            ctx_groups.append(group_of(len(lat) + n, at, size, head))
    done = prepare(ctx_groups)
    each = 2 * len(ctx)
    for head in range(heads):
        for d in range(2):
            chosen = [i for i in done[head * each : (head + 1) * each] if i["d"] == d]
            keep(0, 2 * head + d, chain(chosen, d))
    for head in range(heads):
        ship_head(0, head)
    latents = []
    for head in range(heads):
        latents.append([group_of(n, at, size, head) for n, (at, size) in enumerate(lat)])
        solve_groups(latents[head])
        for d in range(2):
            keep(1, 2 * head + d, chain_groups(latents[head], d))
        ship_head(1, head)
    def arrive(part):
        arrived(got_m.at[part, pl.ds(0, sp - 1)], recv_m.at[part])
        arrived(got_b.at[part, pl.ds(0, sp - 1)], recv_b.at[part])

    def give_back(place):
        return send(
            starts.at[place], back.at[my_item * split + my_part], sent_s, recv_s.at[my_item // 2], on_mesh(sp=place)
        )

    def q_of(head):
        lanes = slice(head * HEAD_DIM, (head + 1) * HEAD_DIM)
        return lambda at, size: q_v[at : at + size, lanes]

    def run_chain():
        arrive(1)
        state = ctx_state[...]
        for step in range(sp):
            place = step + reverse * (sp - 1 - 2 * step)
            starts[place] = state.astype(bf16)
            if step < sp - 1:
                state = advance(state, got_m[1, place], got_b[1, place])
        for place in rings:
            give_back(place).start()
        back[my_item * split + my_part] = starts[me]

    q_v[...] = jnp.dot(mod_v[0:tokens, :], q_w[...], preferred_element_type=f32).astype(bf16)
    outputs(latents[0], q_of(0), o_v.at[0], e_v.at[0])

    @pl.when(owning)
    def _():
        keep_own(0)
        keep_own(1)
        arrive(0)
        state = jnp.zeros((part_rows, HEAD_DIM), f32)
        for step in range(sp):
            place = step + reverse * (sp - 1 - 2 * step)
            state = advance(state, got_m[0, place], got_b[0, place])
        ctx_state[...] = state

    for head in range(heads):
        if head > 0:
            outputs(latents[head], q_of(head), o_v.at[head], e_v.at[head])

        @pl.when(owning & (my_item // 2 == head))
        def _():
            run_chain()

    mid = tokens // 2

    def piece(head, place, part):
        return got_o.at[head, place, pl.ds(part * mid, mid)]

    def to_up(head, part):
        return send(
            piece(head, col, part), piece(head, col, part), sent_o.at[head], recv_dn.at[head, part],
            on_mesh(tp=up),
        )

    def to_down(head, part):
        return send(
            piece(head, col, part), piece(head, col, part), sent_o.at[head], recv_up.at[head, part],
            on_mesh(tp=down),
        )

    def forward(head, part):
        src, dst = (down, up) if part == 0 else (up, down)
        return send(
            piece(head, src, part), piece(head, src, part), sent_o.at[head], recv_f.at[head, part],
            on_mesh(tp=dst),
        )

    def relay(head, n, spot):
        return send(spot, spot, sent_o.at[head], recv_c.at[head, n], on_mesh(tp=partner))

    def finish_head(head):
        half_items = [2 * head, 2 * head + 1]
        mine = owning & (my_item // 2 == head)

        @pl.when(mine)
        def _():
            arrived(back.at[pl.ds(0, 2 * split - 1)], recv_s.at[head])

        @pl.when(jnp.logical_not(mine))
        def _():
            arrived(back.at[pl.ds(0, 2 * split)], recv_s.at[head])

        pair = [back[item * split : (item + 1) * split].reshape(HEAD_DIM, HEAD_DIM) for item in half_items]
        combined = o_v[head] + mm_t(e_v[head], jnp.concatenate(pair, axis=1))
        norm = lax.rsqrt(jnp.mean(combined * combined, axis=1, keepdims=True) + epsilon)
        got_o[head, col] = (combined * norm * head_gain_ref[...]).astype(bf16)
        for copy in (to_up(head, 0), to_down(head, 1), to_up(head, 1), to_down(head, 0)):
            copy.start()
        relay(head, 0, got_o.at[head, col]).start()

    def near_arrivals(head):
        waits = (
            (down, 0, recv_dn, 1, True),
            (up, 1, recv_up, 2, True),
            (down, 1, recv_dn, 1, False),
            (up, 0, recv_up, 2, False),
        )
        for place, part, sems, n, onward in waits:
            spot = piece(head, place, part)
            arrived(spot, sems.at[head, part])
            if onward:
                forward(head, part).start()
            relay(head, n, spot).start()

    def far_arrivals(head):
        for part in range(2):
            spot = piece(head, far, part)
            arrived(spot, recv_f.at[head, part])
            relay(head, 3, spot).start()

    def from_partner(head, n):
        arrived(got_o.at[head, 0], recv_c.at[head, n])

    def add(head, place, first=False):
        even = place - core
        lanes = jnp.concatenate([got_o[head, even], got_o[head, even + 1]], axis=1)
        depth = heads * HEAD_DIM
        weights = jnp.concatenate(
            [
                out_w[pl.ds(pl.multiple_of((even + n) * depth + head * HEAD_DIM, HEAD_DIM), HEAD_DIM), :]
                for n in range(2)
            ],
            axis=0,
        )
        part = jnp.dot(lanes, weights, preferred_element_type=f32)
        acc[...] = part if first else acc[...] + part

    out_load.wait()
    for head in range(heads):
        finish_head(head)
    near_arrivals(0)
    for head in range(heads):
        from_partner(head, 0)
        add(head, col, head == 0)
    for head in range(1, heads):
        near_arrivals(head)
    for head in range(heads):
        for n, place in ((1, down), (2, up)):
            from_partner(head, n)
            add(head, place)
        far_arrivals(head)
    for head in range(heads):
        from_partner(head, 3)
        add(head, far)
    lanes = pl.ds(pl.multiple_of(col * width, width), width)
    out_ref[...] = (rows_v[0:tokens, lanes].astype(f32) + gate_row[...] * acc[...]).astype(bf16)
    left(got_p.at[pl.ds(0, sp - 1)], sent_p)
    left(blocks.at[pl.ds(0, tp - 1)], sent_t)

    def sent_maps(count):
        for part in range(2):
            left(got_m.at[part, pl.ds(0, count)], sent_m.at[part])
            left(got_b.at[part, pl.ds(0, count)], sent_b.at[part])

    @pl.when(owning)
    def _():
        sent_maps(items * split - 1)
        left(starts.at[pl.ds(0, sp - 1)], sent_s)

    @pl.when(jnp.logical_not(owning))
    def _():
        sent_maps(items * split)

    for head in range(heads):
        left(got_o.at[head, pl.ds(0, tp - 1)], sent_o.at[head])


def deliver_kernel(src, dst, held, taken, given):
    rows = held.shape[0] // 4
    spots = [pl.ds(n * rows, rows) for n in range(4)]
    takes = [pltpu.make_async_copy(src.at[spot], held.at[spot], taken.at[n]) for n, spot in enumerate(spots)]
    gives = [pltpu.make_async_copy(held.at[spot], dst.at[spot], given.at[n]) for n, spot in enumerate(spots)]
    for take in takes:
        take.start()
    for take, give in zip(takes, gives):
        take.wait()
        give.start()
    for give in gives:
        give.wait()


def body(
    latent,
    context,
    condition,
    context_condition,
    shift_weight,
    scale_weight,
    gate_weight,
    norm_gain,
    query_weight,
    key_weight,
    value_weight,
    write_weight,
    decay_weight,
    write_bias,
    decay_bias,
    log_rate,
    head_gain,
    out_weight,
):
    sp, tp = lax.axis_size("sp"), lax.axis_size("tp")
    inner = query_weight.shape[1]
    heads = inner // HEAD_DIM
    tokens, ctx_tokens = latent.shape[0], context.shape[0]
    total = tokens + ctx_tokens
    features = latent.shape[1]
    width = shift_weight.shape[1]
    items = 2 * heads
    split = 2
    rows = HEAD_DIM // split
    chunks = sum(len(part) for part in spans(tokens, ctx_tokens))
    vmem = pl.BlockSpec(memory_space=pltpu.VMEM)
    smem = pl.BlockSpec(memory_space=pltpu.SMEM)
    anywhere = pl.BlockSpec(memory_space=pltpu.HBM)
    dma = pltpu.SemaphoreType.DMA
    flat = [jnp.transpose(w, (1, 2, 0)).reshape(-1, features) for w in (write_weight, decay_weight)]
    updated = pl.pallas_call(
        functools.partial(mixer_kernel, sp, tp, heads, tokens, ctx_tokens),
        in_specs=[vmem] * 4 + [smem] * 3 + [anywhere] * 11,
        out_specs=vmem,
        out_shape=jax.ShapeDtypeStruct((tokens, width), bf16),
        scratch_shapes=[
            pltpu.VMEM((total, features), bf16),
            pltpu.VMEM((3,) + shift_weight.shape, bf16),
            pltpu.VMEM(query_weight.shape, bf16),
            pltpu.VMEM(key_weight.shape, bf16),
            pltpu.VMEM(value_weight.shape, bf16),
            pltpu.VMEM((HEAD_DIM, features), bf16),
            pltpu.VMEM(out_weight.shape, bf16),
            pltpu.VMEM((4, 8, features), f32),
            pltpu.VMEM((total, HEAD_DIM), f32),
            pltpu.VMEM((total, features), bf16),
            pltpu.VMEM((tokens, inner), bf16),
            pltpu.VMEM((total, inner), bf16),
            pltpu.VMEM((total, inner), bf16),
            pltpu.VMEM((total, HEAD_DIM), f32),
            pltpu.VMEM((total, HEAD_DIM), f32),
            pltpu.VMEM((chunks, HEAD_DIM, CHUNK), f32),
            pltpu.VMEM((sp, 16, width // 2), bf16),
            pltpu.VMEM((tp, 8, width // 2), f32),
            pltpu.VMEM((1, width), f32),
            pltpu.VMEM((rows, HEAD_DIM), f32),
            pltpu.VMEM((heads, tokens, HEAD_DIM), f32),
            pltpu.VMEM((heads, tokens, 2 * HEAD_DIM), bf16),
            pltpu.VMEM((2, items, HEAD_DIM, HEAD_DIM), bf16),
            pltpu.VMEM((2, items, HEAD_DIM, HEAD_DIM), bf16),
            pltpu.VMEM((2, sp, HEAD_DIM, HEAD_DIM), bf16),
            pltpu.VMEM((2, sp, rows, HEAD_DIM), bf16),
            pltpu.VMEM((sp, rows, HEAD_DIM), bf16),
            pltpu.VMEM((items * split, rows, HEAD_DIM), bf16),
            pltpu.VMEM((heads, tp, tokens, HEAD_DIM), bf16),
            pltpu.VMEM((tokens, width), f32),
            dma((11,)),
            dma,
            dma,
            dma,
            dma,
            dma((2,)),
            dma((2,)),
            dma((2,)),
            dma((2,)),
            dma,
            dma((heads,)),
            dma((heads,)),
            dma((heads, 2)),
            dma((heads, 2)),
            dma((heads, 2)),
            dma((heads, 4)),
        ],
        compiler_params=pltpu.CompilerParams(
            collective_id=0, has_side_effects=True, vmem_limit_bytes=58 * 1024 * 1024
        ),
        name="mixer",
    )(
        condition.reshape(-1, HEAD_DIM),
        context_condition.reshape(-1, HEAD_DIM),
        norm_gain[None, :],
        head_gain[None, :],
        write_bias,
        decay_bias,
        log_rate,
        latent,
        context,
        shift_weight,
        scale_weight,
        gate_weight,
        query_weight,
        key_weight,
        value_weight,
        flat[0],
        flat[1],
        out_weight,
    )
    return pl.pallas_call(
        deliver_kernel,
        in_specs=[pl.BlockSpec(memory_space=pltpu.HBM)],
        out_specs=pl.BlockSpec(memory_space=pltpu.HBM),
        out_shape=jax.ShapeDtypeStruct((tokens, width), bf16),
        scratch_shapes=[pltpu.VMEM((tokens, width), bf16), dma((4,)), dma((4,))],
        compiler_params=pltpu.CompilerParams(vmem_limit_bytes=58 * 1024 * 1024),
        name="deliver",
    )(updated)


def solution(mesh):
    placed = (
        P("sp", None),
        P("sp", None),
        P("sp"),
        P("sp"),
        P("sp", "tp"),
        P("sp", "tp"),
        P("sp", "tp"),
        P(),
        P(None, "tp"),
        P(None, "tp"),
        P(None, "tp"),
        P(),
        P(),
        P(),
        P(),
        P(),
        P(),
        P(None, "tp"),
    )
    return jax.shard_map(body, mesh=mesh, in_specs=placed, out_specs=P("sp", "tp"), check_vma=False)
```

```python
import functools
import math

import jax
import jax.numpy as jnp
from jax import lax
from jax.experimental import pallas as pl
from jax.experimental.pallas import tpu as pltpu
from jax.sharding import PartitionSpec as P

HEAD_DIM = 128
CHUNK = 128
epsilon = 0.0001
bf16 = jnp.bfloat16
f32 = jnp.float32


def mm(a, b):
    return jnp.dot(a.astype(bf16), b.astype(bf16), preferred_element_type=f32)


def mm_t(a, b):
    return lax.dot_general(a, b, (((1,), (1,)), ((), ())), preferred_element_type=f32)


def spans(tokens, ctx_tokens):
    size = min(CHUNK, tokens)
    lat = [(at, size) for at in range(0, tokens, size)]
    ctx_size = min(CHUNK, ctx_tokens)
    ctx = [(tokens + at, ctx_size) for at in range(0, ctx_tokens, ctx_size)]
    return lat, ctx


def iotas(size):
    rows = lax.broadcasted_iota(jnp.int32, (size, size), 0)
    cols = lax.broadcasted_iota(jnp.int32, (size, size), 1)
    return rows, cols


def prepare(groups):
    items = []
    for group in groups:
        size = group["size"]
        rows, cols = iotas(size)
        keys = group["k"]
        keys_t = keys.astype(f32).T
        gram = jnp.dot(keys, keys_t.astype(bf16), preferred_element_type=f32)
        diag = jnp.where(rows == cols, gram, 0.0)
        s_col = lax.rsqrt(jnp.sum(diag, axis=1, keepdims=True) + epsilon)
        s_row = lax.rsqrt(jnp.sum(diag, axis=0, keepdims=True) + epsilon)
        gram = gram * s_col * s_row
        group["keys"] = keys.astype(f32) * s_col
        group["keys_t"] = keys_t * s_row
        group["values"] = group["v"].astype(f32)
        for d in range(2):
            rate_col, run_col, run_row = group["gates"][d]
            inside = rows >= cols if d == 0 else rows <= cols
            strict = rows > cols if d == 0 else rows < cols
            decay = jnp.where(inside, jnp.exp(jnp.minimum(run_col - run_row, 0.0)), 0.0)
            system = jnp.where(strict, gram * decay * rate_col, 0.0)
            item = dict(group=group, size=size, d=d, rate_col=rate_col, run_col=run_col, run_row=run_row)
            item["system"] = system
            near = (rows // 2) == (cols // 2)
            item["inv"] = jnp.where(rows == cols, 1.0, jnp.where(near, -system, 0.0))
            items.append(item)
    span = 2
    while span < max(item["size"] for item in items):
        firsts = []
        for item in items:
            if span >= item["size"]:
                firsts.append(None)
                continue
            rows, cols = iotas(item["size"])
            rows, cols = rows // span, cols // span
            if item["d"] == 0:
                mask = ((rows % 2) == 1) & (cols == rows - 1)
            else:
                mask = ((cols % 2) == 1) & (rows == cols - 1)
            firsts.append(mm(jnp.where(mask, item["system"], 0.0), item["inv"]))
        for item, first in zip(items, firsts):
            if first is not None:
                item["inv"] = item["inv"] - mm(item["inv"], first)
        span *= 2
    for item in items:
        group = item["group"]
        growth = jnp.exp(item["run_col"])
        both = jnp.concatenate(
            [group["values"] * item["rate_col"], group["keys"] * (item["rate_col"] * growth)], axis=1
        )
        item["solved"] = mm(item["inv"], both)
        last = item["run_row"][:, item["size"] - 1 :] if item["d"] == 0 else item["run_row"][:, :1]
        item["gate"] = jnp.exp(last)
        late_t = group["keys_t"] * jnp.exp(last - item["run_row"])
        item["late"] = mm(late_t, item["solved"])
    return items


def solve_groups(groups):
    size = groups[0]["size"]
    rows, cols = iotas(size)
    near = (rows // 2) == (cols // 2)
    for group in groups:
        keys = group["k"]
        keys_t = keys.astype(f32).T
        group["plain_t"] = keys_t.astype(bf16)
        gram = jnp.dot(keys, group["plain_t"], preferred_element_type=f32)
        diag = jnp.where(rows == cols, gram, 0.0)
        s_col = lax.rsqrt(jnp.sum(diag, axis=1, keepdims=True) + epsilon)
        s_row = lax.rsqrt(jnp.sum(diag, axis=0, keepdims=True) + epsilon)
        gram = gram * s_col * s_row
        group["s_row"] = s_row
        group["keys"] = keys.astype(f32) * s_col
        group["keys_t"] = keys_t * s_row
        group["decay"], group["system"], group["inv"] = [], [], []
        for d in range(2):
            rate_col, run_col, run_row = group["gates"][d]
            inside = rows >= cols if d == 0 else rows <= cols
            strict = rows > cols if d == 0 else rows < cols
            decay = jnp.where(inside, jnp.exp(jnp.minimum(run_col - run_row, 0.0)), 0.0)
            group["decay"].append(decay)
            system = jnp.where(strict, gram * decay * rate_col, 0.0)
            group["system"].append(system.astype(bf16))
            group["inv"].append(jnp.where(rows == cols, 1.0, jnp.where(near, -system, 0.0)))
    span = 2
    while span < size:
        row_block, col_block = rows // span, cols // span
        masks = (
            ((row_block % 2) == 1) & (col_block == row_block - 1),
            ((col_block % 2) == 1) & (row_block == col_block - 1),
        )
        masks = [jnp.where(mask, 1.0, 0.0).astype(bf16) for mask in masks]
        firsts = []
        for group in groups:
            group["packed"] = [inv.astype(bf16) for inv in group["inv"]]
            firsts.append([mm(group["system"][d] * masks[d], group["packed"][d]) for d in range(2)])
        for group, first in zip(groups, firsts):
            group["inv"] = [group["inv"][d] - mm(group["packed"][d], first[d]) for d in range(2)]
        span *= 2
    for group in groups:
        values = group["v"].astype(f32)
        group["growth"], group["solved"], group["late"], group["gate"] = [], [], [], []
        for d in range(2):
            rate_col, run_col, run_row = group["gates"][d]
            growth = jnp.exp(run_col)
            both = jnp.concatenate([values * rate_col, group["keys"] * (rate_col * growth)], axis=1)
            solved = mm(group["inv"][d], both).astype(bf16)
            last = run_row[:, size - 1 :] if d == 0 else run_row[:, :1]
            group["growth"].append(growth)
            group["solved"].append(solved)
            group["gate"].append(jnp.exp(last))
            group["late"].append(mm(group["keys_t"] * jnp.exp(last - run_row), solved))


def follow(carry, late, gate, eye):
    fresh = jnp.concatenate([late[:, :HEAD_DIM], (gate - 1.0) * eye - late[:, HEAD_DIM:]], axis=1)
    if carry is None:
        return fresh
    return gate * carry + fresh - mm(late[:, HEAD_DIM:], carry)


def identity():
    rows, cols = iotas(HEAD_DIM)
    return (rows == cols).astype(f32)


def chain(items, d):
    eye = identity()
    carry = None
    for item in items if d == 0 else items[::-1]:
        carry = follow(carry, item["late"], item["gate"], eye)
    return carry


def chain_groups(groups, d):
    eye = identity()
    carry = None
    for group in groups if d == 0 else groups[::-1]:
        group["before", d] = None if carry is None else carry.astype(bf16)
        carry = follow(carry, group["late"][d], group["gate"][d], eye)
    return carry


def outputs(groups, q_of, o_ref, e_ref):
    for group in groups:
        at, size = group["at"], group["size"]
        plain = q_of(at, size)
        queries = plain.astype(f32)
        q_scale = lax.rsqrt(jnp.sum(queries * queries, axis=1, keepdims=True) + epsilon) * HEAD_DIM**-0.5
        queries = queries * q_scale
        score = jnp.dot(plain, group["plain_t"], preferred_element_type=f32) * q_scale * group["s_row"]
        total = None
        for d in range(2):
            weighed = mm(score * group["decay"][d], group["solved"][d])
            out = weighed[:, :HEAD_DIM]
            early = queries * group["growth"][d] - weighed[:, HEAD_DIM:]
            before = group["before", d]
            if before is not None:
                moved = mm(early, before)
                out = out + moved[:, :HEAD_DIM]
                early = early + moved[:, HEAD_DIM:]
            e_ref[at : at + size, d * HEAD_DIM : (d + 1) * HEAD_DIM] = early.astype(bf16)
            total = out if total is None else total + out
        o_ref[at : at + size, :] = total


def on_mesh(sp=None, tp=None):
    return (lax.axis_index("sp") if sp is None else sp, lax.axis_index("tp") if tp is None else tp)


def send(src, dst, send_sem, recv_sem, device):
    return pltpu.make_async_remote_copy(
        src_ref=src,
        dst_ref=dst,
        send_sem=send_sem,
        recv_sem=recv_sem,
        device_id=device,
        device_id_type=pl.DeviceIdType.MESH,
    )


def greet(devices):
    barrier = pltpu.get_barrier_semaphore()
    for device in devices:
        pl.semaphore_signal(barrier, inc=1, device_id=device, device_id_type=pl.DeviceIdType.MESH)


def split_three(x):
    high = x.astype(bf16)
    rest = x - high.astype(f32)
    mid = rest.astype(bf16)
    low = (rest - mid.astype(f32)).astype(bf16)
    return jnp.concatenate([high, mid, low], axis=1)


def advance(state, move, add):
    high = state.astype(bf16)
    low = (state - high.astype(f32)).astype(bf16)
    both = jnp.concatenate([high, low], axis=0)
    moved = jnp.dot(both, move, preferred_element_type=f32)
    rows = state.shape[0]
    return state + add.astype(f32) + moved[:rows] + moved[rows:]


def mixer_kernel(
    sp, tp, heads, tokens, ctx_tokens,
    cond_ref, ctx_cond_ref, gain_ref, head_gain_ref, write_bias_ref, decay_bias_ref, log_rate_ref,
    latent_hbm, context_hbm, shift_hbm, scale_hbm, gate_hbm, query_hbm, key_hbm, value_hbm,
    write_hbm, decay_hbm, out_hbm,
    out_ref,
    rows_v, mod_w, q_w, k_w, v_w, gate_w, out_w, st, stats, mod_v, q_v, k_v, v_v, rate_v, run_v, run_t,
    got_p, blocks, gate_row, ctx_state, o_v, e_v, maps_m, maps_b, got_m, got_b, starts, back, got_o, acc,
    load, sent_p, recv_p, sent_t, recv_t, sent_m, recv_m, sent_b, recv_b, sent_s, recv_s,
    sent_o, recv_dn, recv_up, recv_f, recv_c,
):
    me, col = lax.axis_index("sp"), lax.axis_index("tp")
    items = 2 * heads
    quads = sp // items
    split = 2
    part_rows = HEAD_DIM // split
    core = lax.rem(col, 2)
    chips = tp // 2
    chip = col // 2
    partner = col + 1 - 2 * core
    up = lax.rem(chip + 1, chips) * 2 + core
    down = lax.rem(chip + chips - 1, chips) * 2 + core
    far = lax.rem(chip + 2, chips) * 2 + core
    width = mod_w.shape[2]
    half = width // 2
    total_tokens = tokens + ctx_tokens
    side = math.isqrt(sp)
    steps = [(dz, dx) for dz in range(side) for dx in range(side) if dz + dx > 0]
    steps.sort(key=lambda step: -sum(min(d, side - d) for d in step))
    rings = [lax.rem(me // side + dz, side) * side + lax.rem(lax.rem(me, side) + dx, side) for dz, dx in steps]
    near = on_mesh(sp=rings[0])
    cross = [lax.rem(col + r, tp) for r in range(1, tp)]
    greet([on_mesh(sp=place) for place in rings] + [on_mesh(tp=place) for place in cross])

    def arrived(spot, sem):
        send(spot, spot, sem, sem, near).wait_recv()

    def left(spot, sem):
        send(spot, spot, sem, sem, near).wait_send()

    def fetch(n, src, dst):
        copy = pltpu.make_async_copy(src, dst, load.at[n])
        copy.start()
        return copy

    gates_rows = write_hbm.shape[0]
    mod_loads = [fetch(n, src, mod_w.at[n]) for n, src in enumerate((shift_hbm, scale_hbm, gate_hbm))]
    row_loads = [
        fetch(3, latent_hbm, rows_v.at[pl.ds(0, tokens)]),
        fetch(4, context_hbm, rows_v.at[pl.ds(tokens, ctx_tokens)]),
    ]
    weight_loads = [
        fetch(5, key_hbm, k_w),
        fetch(6, value_hbm, v_w),
        fetch(7, write_hbm, gate_w.at[pl.ds(0, gates_rows)]),
        fetch(8, decay_hbm, gate_w.at[pl.ds(gates_rows, gates_rows)]),
        fetch(9, query_hbm, q_w),
    ]
    out_load = fetch(10, out_hbm, out_w)

    def silu(ref):
        value = ref[...].astype(f32)
        return value / (1.0 + jnp.exp(-value))

    silus = (silu(cond_ref), silu(ctx_cond_ref))
    quarter = silus[0].shape[0]
    lefts = []
    for part in range(quarter):
        lefts.append(
            jnp.concatenate(
                [silus[0][part : part + 1], silus[1][part : part + 1], jnp.zeros((6, silus[0].shape[1]), f32)], axis=0
            ).astype(bf16)
        )
    silu_rows = jnp.concatenate(lefts, axis=1)
    for copy in mod_loads:
        copy.wait()
    shift = jnp.dot(silu_rows, mod_w[0], preferred_element_type=f32)
    scale = jnp.dot(silu_rows, mod_w[1], preferred_element_type=f32)
    gate = jnp.dot(silu_rows, mod_w[2], preferred_element_type=f32)
    partial = jnp.concatenate([shift[0:2], scale[0:2], gate[0:1], jnp.zeros((3, width), f32)], axis=0)
    got_p[me] = jnp.concatenate([partial[:, :half], partial[:, half:]], axis=0).astype(bf16)
    pl.semaphore_wait(pltpu.get_barrier_semaphore(), len(rings) + len(cross))
    for place in rings:
        send(got_p.at[me], got_p.at[me], sent_p, recv_p, on_mesh(sp=place)).start()

    gate_w[2 * gates_rows :, :] = jnp.zeros((gate_w.shape[0] - 2 * gates_rows, gate_w.shape[1]), bf16)
    for copy in row_loads:
        copy.wait()

    def measure_rows(i, unused):
        at = pl.ds(pl.multiple_of(i * 32, 32), 32)
        values = rows_v[at, :].astype(f32)
        mean = jnp.mean(values * values, axis=1, keepdims=True)
        stats[at, :] = jnp.broadcast_to(lax.rsqrt(mean + epsilon), (32, HEAD_DIM))
        return unused

    lax.fori_loop(0, total_tokens // 32, measure_rows, 0)

    arrived(got_p.at[pl.ds(0, sp - 1)], recv_p)
    total = got_p[0].astype(f32)
    for place in range(1, sp):
        total = total + got_p[place].astype(f32)
    blocks[col] = jnp.concatenate([total[0:4], total[8:12]], axis=0)
    gate_row[...] = jnp.concatenate([total[4:5], total[12:13]], axis=1)
    for place in cross:
        send(blocks.at[col], blocks.at[col], sent_t, recv_t, on_mesh(tp=place)).start()
    arrived(blocks.at[pl.ds(0, tp - 1)], recv_t)
    for place in range(tp):
        at = place * width
        for part in range(2):
            lanes = slice(at + part * half, at + (part + 1) * half)
            four = blocks[place, 4 * part : 4 * part + 4, :]
            scaled = (1.0 + four[2:4]) * gain_ref[:, lanes]
            for which in range(2):
                st[which, :, lanes] = jnp.broadcast_to(four[which : which + 1], (8, half))
                st[2 + which, :, lanes] = jnp.broadcast_to(scaled[which : which + 1], (8, half))

    def modulate(first, count, which):
        def step(i, unused):
            at = pl.ds(pl.multiple_of(first + i * 32, 32), 32)
            root = stats[at, :]
            for lane_at in range(0, rows_v.shape[1], HEAD_DIM):
                lanes = slice(lane_at, lane_at + HEAD_DIM)
                values = rows_v[at, lanes].astype(f32) * root
                shift, scale = st[which, :, lanes], st[2 + which, :, lanes]
                parts = [values[n : n + 8] * scale + shift for n in range(0, 32, 8)]
                mod_v[at, lanes] = jnp.concatenate(parts, axis=0).astype(bf16)
            return unused

        lax.fori_loop(0, count // 32, step, 0)

    modulate(tokens, ctx_tokens, 1)
    modulate(0, tokens, 0)
    for copy in weight_loads:
        copy.wait()
    pre = mm_t(mod_v[...], gate_w[...]).astype(bf16).astype(f32)
    k_v[...] = jnp.dot(mod_v[...], k_w[...], preferred_element_type=f32).astype(bf16)
    v_v[...] = jnp.dot(mod_v[...], v_w[...], preferred_element_type=f32).astype(bf16)

    all_heads = gates_rows // 2
    first_head = col * heads
    pre = pltpu.roll(pre, HEAD_DIM - first_head, 1)
    lane = lax.broadcasted_iota(jnp.int32, (1, HEAD_DIM), 1)
    write_bias = jnp.zeros((1, HEAD_DIM), f32)
    decay_bias = jnp.zeros((1, HEAD_DIM), f32)
    log_rate = jnp.zeros((1, HEAD_DIM), f32)
    for d in range(2):
        for head in range(heads):
            spot = d * all_heads + head
            write_bias = jnp.where(lane == spot, write_bias_ref[d, first_head + head], write_bias)
            decay_bias = jnp.where(lane == spot + gates_rows, decay_bias_ref[d, first_head + head], decay_bias)
            log_rate = jnp.where(lane == spot + gates_rows, log_rate_ref[d, first_head + head], log_rate)
    rate_v[...] = jax.nn.sigmoid(pre + write_bias)
    raised = pre + decay_bias
    soft = jnp.maximum(raised, 0.0) + jnp.log1p(jnp.exp(-jnp.abs(raised)))
    log_decay = -jnp.exp(log_rate) * soft
    lat, ctx = spans(tokens, ctx_tokens)
    for n, (at, size) in enumerate(lat + ctx):
        rows, cols = iotas(size)
        lower = (rows >= cols).astype(f32)
        upper = (rows <= cols).astype(f32)
        sums = jnp.dot(
            jnp.concatenate([lower, upper], axis=0).astype(bf16),
            split_three(log_decay[at : at + size]),
            preferred_element_type=f32,
        )
        sums = sums[:, :HEAD_DIM] + sums[:, HEAD_DIM : 2 * HEAD_DIM] + sums[:, 2 * HEAD_DIM :]
        running = jnp.where(lane < gates_rows + all_heads, sums[:size], sums[size:])
        run_v[at : at + size, :] = running
        run_t[n, :, :size] = running.T

    def group_of(n, at, size, head):
        lanes = slice(head * HEAD_DIM, (head + 1) * HEAD_DIM)
        gates = []
        for d in range(2):
            spot = d * all_heads + head
            deep = spot + gates_rows
            gates.append(
                (
                    rate_v[at : at + size, spot : spot + 1],
                    run_v[at : at + size, deep : deep + 1],
                    run_t[n, deep : deep + 1, :size],
                )
            )
        return dict(
            at=at,
            size=size,
            k=k_v[at : at + size, lanes],
            v=v_v[at : at + size, lanes],
            gates=gates,
        )

    def keep(part, item, carry):
        maps_b[part, item] = carry[:, :HEAD_DIM].T.astype(bf16)
        maps_m[part, item] = carry[:, HEAD_DIM:].T.astype(bf16)

    def owner_of(item, piece):
        return item * quads + 2 * piece + lax.rem(item + core, 2)

    my_item, my_part = me // quads, lax.rem(me, quads) // 2
    owning = lax.rem(me, 2) == lax.rem(my_item + core, 2)
    reverse = lax.rem(my_item, 2)

    def ship(part, item, piece):
        owner = owner_of(item, piece)

        @pl.when(owner != me)
        def _():
            send(
                maps_m.at[part, item], got_m.at[part, me], sent_m.at[part], recv_m.at[part], on_mesh(sp=owner)
            ).start()
            send(
                maps_b.at[part, item, pl.ds(piece * part_rows, part_rows)],
                got_b.at[part, me], sent_b.at[part], recv_b.at[part], on_mesh(sp=owner),
            ).start()

    def ship_head(part, head):
        for item in (2 * head, 2 * head + 1):
            for piece in range(split):
                ship(part, item, piece)

    def keep_own(part):
        got_m[part, me] = maps_m[part, my_item]
        got_b[part, me] = maps_b[part, my_item, pl.ds(pl.multiple_of(my_part * part_rows, part_rows), part_rows), :]

    ctx_groups = []
    for head in range(heads):
        for n, (at, size) in enumerate(ctx):
            ctx_groups.append(group_of(len(lat) + n, at, size, head))
    done = prepare(ctx_groups)
    each = 2 * len(ctx)
    for head in range(heads):
        for d in range(2):
            chosen = [i for i in done[head * each : (head + 1) * each] if i["d"] == d]
            keep(0, 2 * head + d, chain(chosen, d))
    for head in range(heads):
        ship_head(0, head)
    latents = []
    for head in range(heads):
        latents.append([group_of(n, at, size, head) for n, (at, size) in enumerate(lat)])
        solve_groups(latents[head])
        for d in range(2):
            keep(1, 2 * head + d, chain_groups(latents[head], d))
        ship_head(1, head)
    def arrive(part):
        arrived(got_m.at[part, pl.ds(0, sp - 1)], recv_m.at[part])
        arrived(got_b.at[part, pl.ds(0, sp - 1)], recv_b.at[part])

    def give_back(place):
        return send(
            starts.at[place], back.at[my_item * split + my_part], sent_s, recv_s.at[my_item // 2], on_mesh(sp=place)
        )

    def q_of(head):
        lanes = slice(head * HEAD_DIM, (head + 1) * HEAD_DIM)
        return lambda at, size: q_v[at : at + size, lanes]

    def run_chain():
        arrive(1)
        state = ctx_state[...]
        for step in range(sp):
            place = step + reverse * (sp - 1 - 2 * step)
            starts[place] = state.astype(bf16)
            if step < sp - 1:
                state = advance(state, got_m[1, place], got_b[1, place])
        for place in rings:
            give_back(place).start()
        back[my_item * split + my_part] = starts[me]

    q_v[...] = jnp.dot(mod_v[0:tokens, :], q_w[...], preferred_element_type=f32).astype(bf16)
    outputs(latents[0], q_of(0), o_v.at[0], e_v.at[0])

    @pl.when(owning)
    def _():
        keep_own(0)
        keep_own(1)
        arrive(0)
        state = jnp.zeros((part_rows, HEAD_DIM), f32)
        for step in range(sp):
            place = step + reverse * (sp - 1 - 2 * step)
            state = advance(state, got_m[0, place], got_b[0, place])
        ctx_state[...] = state

    for head in range(heads):
        if head > 0:
            outputs(latents[head], q_of(head), o_v.at[head], e_v.at[head])

        @pl.when(owning & (my_item // 2 == head))
        def _():
            run_chain()

    parts = 2
    mid = tokens // parts

    def piece(head, place, part):
        return got_o.at[head, place, pl.ds(part * mid, mid)]

    def to_up(head, part):
        return send(
            piece(head, col, part), piece(head, col, part), sent_o.at[head], recv_dn.at[head, part],
            on_mesh(tp=up),
        )

    def to_down(head, part):
        return send(
            piece(head, col, part), piece(head, col, part), sent_o.at[head], recv_up.at[head, part],
            on_mesh(tp=down),
        )

    def forward(head, part):
        src, dst = (down, up) if part < parts // 2 else (up, down)
        return send(
            piece(head, src, part), piece(head, src, part), sent_o.at[head], recv_f.at[head, part],
            on_mesh(tp=dst),
        )

    def relay(head, n, spot):
        return send(spot, spot, sent_o.at[head], recv_c.at[head, n], on_mesh(tp=partner))

    def finish_head(head):
        half_items = [2 * head, 2 * head + 1]
        mine = owning & (my_item // 2 == head)

        @pl.when(mine)
        def _():
            arrived(back.at[pl.ds(0, 2 * split - 1)], recv_s.at[head])

        @pl.when(jnp.logical_not(mine))
        def _():
            arrived(back.at[pl.ds(0, 2 * split)], recv_s.at[head])

        pair = [back[item * split : (item + 1) * split].reshape(HEAD_DIM, HEAD_DIM) for item in half_items]
        combined = o_v[head] + mm_t(e_v[head], jnp.concatenate(pair, axis=1))
        norm = lax.rsqrt(jnp.mean(combined * combined, axis=1, keepdims=True) + epsilon)
        got_o[head, col] = (combined * norm * head_gain_ref[...]).astype(bf16)
        for part in range(parts):
            to_up(head, part).start()
            to_down(head, parts - 1 - part).start()
        relay(head, 0, got_o.at[head, col]).start()

    def near_arrivals(head):
        waits = []
        for part in range(parts):
            waits.append((down, part, recv_dn, 1, part < parts // 2))
            waits.append((up, parts - 1 - part, recv_up, 2, part < parts // 2))
        for place, part, sems, n, onward in waits:
            spot = piece(head, place, part)
            arrived(spot, sems.at[head, part])
            if onward:
                forward(head, part).start()
            relay(head, n, spot).start()

    def far_arrivals(head):
        for n in range(parts):
            part = n // 2 if n % 2 == 0 else parts - 1 - n // 2
            spot = piece(head, far, part)
            arrived(spot, recv_f.at[head, part])
            relay(head, 3, spot).start()

    def from_partner(head, n):
        arrived(got_o.at[head, 0], recv_c.at[head, n])

    def add(head, place, first=False):
        even = place - core
        lanes = jnp.concatenate([got_o[head, even], got_o[head, even + 1]], axis=1)
        depth = heads * HEAD_DIM
        weights = jnp.concatenate(
            [
                out_w[pl.ds(pl.multiple_of((even + n) * depth + head * HEAD_DIM, HEAD_DIM), HEAD_DIM), :]
                for n in range(2)
            ],
            axis=0,
        )
        part = jnp.dot(lanes, weights, preferred_element_type=f32)
        acc[...] = part if first else acc[...] + part

    out_load.wait()
    for head in range(heads):
        finish_head(head)
    near_arrivals(0)
    for head in range(heads):
        from_partner(head, 0)
        add(head, col, head == 0)
    for head in range(1, heads):
        near_arrivals(head)
    for head in range(heads):
        for n, place in ((1, down), (2, up)):
            from_partner(head, n)
            add(head, place)
        far_arrivals(head)
    for head in range(heads):
        from_partner(head, 3)
        add(head, far)
    lanes = pl.ds(pl.multiple_of(col * width, width), width)
    out_ref[...] = (rows_v[0:tokens, lanes].astype(f32) + gate_row[...] * acc[...]).astype(bf16)
    left(got_p.at[pl.ds(0, sp - 1)], sent_p)
    left(blocks.at[pl.ds(0, tp - 1)], sent_t)

    def sent_maps(count):
        for part in range(2):
            left(got_m.at[part, pl.ds(0, count)], sent_m.at[part])
            left(got_b.at[part, pl.ds(0, count)], sent_b.at[part])

    @pl.when(owning)
    def _():
        sent_maps(items * split - 1)
        left(starts.at[pl.ds(0, sp - 1)], sent_s)

    @pl.when(jnp.logical_not(owning))
    def _():
        sent_maps(items * split)

    for head in range(heads):
        left(got_o.at[head, pl.ds(0, tp - 1)], sent_o.at[head])


def deliver_kernel(src, dst, held, taken, given):
    rows = held.shape[0] // 4
    spots = [pl.ds(n * rows, rows) for n in range(4)]
    takes = [pltpu.make_async_copy(src.at[spot], held.at[spot], taken.at[n]) for n, spot in enumerate(spots)]
    gives = [pltpu.make_async_copy(held.at[spot], dst.at[spot], given.at[n]) for n, spot in enumerate(spots)]
    for take in takes:
        take.start()
    for take, give in zip(takes, gives):
        take.wait()
        give.start()
    for give in gives:
        give.wait()


def body(
    latent,
    context,
    condition,
    context_condition,
    shift_weight,
    scale_weight,
    gate_weight,
    norm_gain,
    query_weight,
    key_weight,
    value_weight,
    write_weight,
    decay_weight,
    write_bias,
    decay_bias,
    log_rate,
    head_gain,
    out_weight,
):
    sp, tp = lax.axis_size("sp"), lax.axis_size("tp")
    inner = query_weight.shape[1]
    heads = inner // HEAD_DIM
    tokens, ctx_tokens = latent.shape[0], context.shape[0]
    total = tokens + ctx_tokens
    features = latent.shape[1]
    width = shift_weight.shape[1]
    items = 2 * heads
    split = 2
    rows = HEAD_DIM // split
    chunks = sum(len(part) for part in spans(tokens, ctx_tokens))
    vmem = pl.BlockSpec(memory_space=pltpu.VMEM)
    smem = pl.BlockSpec(memory_space=pltpu.SMEM)
    anywhere = pl.BlockSpec(memory_space=pltpu.HBM)
    dma = pltpu.SemaphoreType.DMA
    flat = [jnp.transpose(w, (1, 2, 0)).reshape(-1, features) for w in (write_weight, decay_weight)]
    updated = pl.pallas_call(
        functools.partial(mixer_kernel, sp, tp, heads, tokens, ctx_tokens),
        in_specs=[vmem] * 4 + [smem] * 3 + [anywhere] * 11,
        out_specs=vmem,
        out_shape=jax.ShapeDtypeStruct((tokens, width), bf16),
        scratch_shapes=[
            pltpu.VMEM((total, features), bf16),
            pltpu.VMEM((3,) + shift_weight.shape, bf16),
            pltpu.VMEM(query_weight.shape, bf16),
            pltpu.VMEM(key_weight.shape, bf16),
            pltpu.VMEM(value_weight.shape, bf16),
            pltpu.VMEM((HEAD_DIM, features), bf16),
            pltpu.VMEM(out_weight.shape, bf16),
            pltpu.VMEM((4, 8, features), f32),
            pltpu.VMEM((total, HEAD_DIM), f32),
            pltpu.VMEM((total, features), bf16),
            pltpu.VMEM((tokens, inner), bf16),
            pltpu.VMEM((total, inner), bf16),
            pltpu.VMEM((total, inner), bf16),
            pltpu.VMEM((total, HEAD_DIM), f32),
            pltpu.VMEM((total, HEAD_DIM), f32),
            pltpu.VMEM((chunks, HEAD_DIM, CHUNK), f32),
            pltpu.VMEM((sp, 16, width // 2), bf16),
            pltpu.VMEM((tp, 8, width // 2), f32),
            pltpu.VMEM((1, width), f32),
            pltpu.VMEM((rows, HEAD_DIM), f32),
            pltpu.VMEM((heads, tokens, HEAD_DIM), f32),
            pltpu.VMEM((heads, tokens, 2 * HEAD_DIM), bf16),
            pltpu.VMEM((2, items, HEAD_DIM, HEAD_DIM), bf16),
            pltpu.VMEM((2, items, HEAD_DIM, HEAD_DIM), bf16),
            pltpu.VMEM((2, sp, HEAD_DIM, HEAD_DIM), bf16),
            pltpu.VMEM((2, sp, rows, HEAD_DIM), bf16),
            pltpu.VMEM((sp, rows, HEAD_DIM), bf16),
            pltpu.VMEM((items * split, rows, HEAD_DIM), bf16),
            pltpu.VMEM((heads, tp, tokens, HEAD_DIM), bf16),
            pltpu.VMEM((tokens, width), f32),
            dma((11,)),
            dma,
            dma,
            dma,
            dma,
            dma((2,)),
            dma((2,)),
            dma((2,)),
            dma((2,)),
            dma,
            dma((heads,)),
            dma((heads,)),
            dma((heads, 2)),
            dma((heads, 2)),
            dma((heads, 2)),
            dma((heads, 4)),
        ],
        compiler_params=pltpu.CompilerParams(
            collective_id=0, has_side_effects=True, vmem_limit_bytes=58 * 1024 * 1024
        ),
        name="mixer",
    )(
        condition.reshape(-1, HEAD_DIM),
        context_condition.reshape(-1, HEAD_DIM),
        norm_gain[None, :],
        head_gain[None, :],
        write_bias,
        decay_bias,
        log_rate,
        latent,
        context,
        shift_weight,
        scale_weight,
        gate_weight,
        query_weight,
        key_weight,
        value_weight,
        flat[0],
        flat[1],
        out_weight,
    )
    return pl.pallas_call(
        deliver_kernel,
        in_specs=[pl.BlockSpec(memory_space=pltpu.HBM)],
        out_specs=pl.BlockSpec(memory_space=pltpu.HBM),
        out_shape=jax.ShapeDtypeStruct((tokens, width), bf16),
        scratch_shapes=[pltpu.VMEM((tokens, width), bf16), dma((4,)), dma((4,))],
        compiler_params=pltpu.CompilerParams(vmem_limit_bytes=58 * 1024 * 1024),
        name="deliver",
    )(updated)


def solution(mesh):
    placed = (
        P("sp", None),
        P("sp", None),
        P("sp"),
        P("sp"),
        P("sp", "tp"),
        P("sp", "tp"),
        P("sp", "tp"),
        P(),
        P(None, "tp"),
        P(None, "tp"),
        P(None, "tp"),
        P(),
        P(),
        P(),
        P(),
        P(),
        P(),
        P(None, "tp"),
    )
    return jax.shard_map(body, mesh=mesh, in_specs=placed, out_specs=P("sp", "tp"), check_vma=False)
```

```python
import functools
import math

import jax
import jax.numpy as jnp
from jax import lax
from jax.experimental import pallas as pl
from jax.experimental.pallas import tpu as pltpu
from jax.sharding import PartitionSpec as P

HEAD_DIM = 128
CHUNK = 128
epsilon = 0.0001
bf16 = jnp.bfloat16
f32 = jnp.float32


def mm(a, b):
    return jnp.dot(a.astype(bf16), b.astype(bf16), preferred_element_type=f32)


def mm_t(a, b):
    return lax.dot_general(a, b, (((1,), (1,)), ((), ())), preferred_element_type=f32)


def spans(tokens, ctx_tokens):
    size = min(CHUNK, tokens)
    lat = [(at, size) for at in range(0, tokens, size)]
    ctx_size = min(CHUNK, ctx_tokens)
    ctx = [(tokens + at, ctx_size) for at in range(0, ctx_tokens, ctx_size)]
    return lat, ctx


def iotas(size):
    rows = lax.broadcasted_iota(jnp.int32, (size, size), 0)
    cols = lax.broadcasted_iota(jnp.int32, (size, size), 1)
    return rows, cols


def prepare(groups):
    items = []
    for group in groups:
        size = group["size"]
        rows, cols = iotas(size)
        keys = group["k"]
        keys_t = keys.astype(f32).T
        gram = jnp.dot(keys, keys_t.astype(bf16), preferred_element_type=f32)
        diag = jnp.where(rows == cols, gram, 0.0)
        s_col = lax.rsqrt(jnp.sum(diag, axis=1, keepdims=True) + epsilon)
        s_row = lax.rsqrt(jnp.sum(diag, axis=0, keepdims=True) + epsilon)
        gram = gram * s_col * s_row
        group["keys"] = keys.astype(f32) * s_col
        group["keys_t"] = keys_t * s_row
        group["values"] = group["v"].astype(f32)
        for d in range(2):
            rate_col, run_col, run_row = group["gates"][d]
            inside = rows >= cols if d == 0 else rows <= cols
            strict = rows > cols if d == 0 else rows < cols
            decay = jnp.where(inside, jnp.exp(jnp.minimum(run_col - run_row, 0.0)), 0.0)
            system = jnp.where(strict, gram * decay * rate_col, 0.0)
            item = dict(group=group, size=size, d=d, rate_col=rate_col, run_col=run_col, run_row=run_row)
            item["system"] = system
            near = (rows // 2) == (cols // 2)
            item["inv"] = jnp.where(rows == cols, 1.0, jnp.where(near, -system, 0.0))
            items.append(item)
    span = 2
    while span < max(item["size"] for item in items):
        firsts = []
        for item in items:
            if span >= item["size"]:
                firsts.append(None)
                continue
            rows, cols = iotas(item["size"])
            rows, cols = rows // span, cols // span
            if item["d"] == 0:
                mask = ((rows % 2) == 1) & (cols == rows - 1)
            else:
                mask = ((cols % 2) == 1) & (rows == cols - 1)
            firsts.append(mm(jnp.where(mask, item["system"], 0.0), item["inv"]))
        for item, first in zip(items, firsts):
            if first is not None:
                item["inv"] = item["inv"] - mm(item["inv"], first)
        span *= 2
    for item in items:
        group = item["group"]
        growth = jnp.exp(item["run_col"])
        both = jnp.concatenate(
            [group["values"] * item["rate_col"], group["keys"] * (item["rate_col"] * growth)], axis=1
        )
        item["solved"] = mm(item["inv"], both)
        last = item["run_row"][:, item["size"] - 1 :] if item["d"] == 0 else item["run_row"][:, :1]
        item["gate"] = jnp.exp(last)
        late_t = group["keys_t"] * jnp.exp(last - item["run_row"])
        item["late"] = mm(late_t, item["solved"])
    return items


def solve_groups(groups):
    size = groups[0]["size"]
    rows, cols = iotas(size)
    near = (rows // 2) == (cols // 2)
    for group in groups:
        keys = group["k"]
        keys_t = keys.astype(f32).T
        group["plain_t"] = keys_t.astype(bf16)
        gram = jnp.dot(keys, group["plain_t"], preferred_element_type=f32)
        diag = jnp.where(rows == cols, gram, 0.0)
        s_col = lax.rsqrt(jnp.sum(diag, axis=1, keepdims=True) + epsilon)
        s_row = lax.rsqrt(jnp.sum(diag, axis=0, keepdims=True) + epsilon)
        gram = gram * s_col * s_row
        group["s_row"] = s_row
        group["keys"] = keys.astype(f32) * s_col
        group["keys_t"] = keys_t * s_row
        group["decay"], group["system"], group["inv"] = [], [], []
        for d in range(2):
            rate_col, run_col, run_row = group["gates"][d]
            inside = rows >= cols if d == 0 else rows <= cols
            strict = rows > cols if d == 0 else rows < cols
            decay = jnp.where(inside, jnp.exp(jnp.minimum(run_col - run_row, 0.0)), 0.0)
            group["decay"].append(decay)
            system = jnp.where(strict, gram * decay * rate_col, 0.0)
            group["system"].append(system.astype(bf16))
            group["inv"].append(jnp.where(rows == cols, 1.0, jnp.where(near, -system, 0.0)))
    span = 2
    while span < size:
        row_block, col_block = rows // span, cols // span
        masks = (
            ((row_block % 2) == 1) & (col_block == row_block - 1),
            ((col_block % 2) == 1) & (row_block == col_block - 1),
        )
        masks = [jnp.where(mask, 1.0, 0.0).astype(bf16) for mask in masks]
        firsts = []
        for group in groups:
            group["packed"] = [inv.astype(bf16) for inv in group["inv"]]
            firsts.append([mm(group["system"][d] * masks[d], group["packed"][d]) for d in range(2)])
        for group, first in zip(groups, firsts):
            group["inv"] = [group["inv"][d] - mm(group["packed"][d], first[d]) for d in range(2)]
        span *= 2
    for group in groups:
        values = group["v"].astype(f32)
        group["growth"], group["solved"], group["late"], group["gate"] = [], [], [], []
        for d in range(2):
            rate_col, run_col, run_row = group["gates"][d]
            growth = jnp.exp(run_col)
            both = jnp.concatenate([values * rate_col, group["keys"] * (rate_col * growth)], axis=1)
            solved = mm(group["inv"][d], both).astype(bf16)
            last = run_row[:, size - 1 :] if d == 0 else run_row[:, :1]
            group["growth"].append(growth)
            group["solved"].append(solved)
            group["gate"].append(jnp.exp(last))
            group["late"].append(mm(group["keys_t"] * jnp.exp(last - run_row), solved))


def follow(carry, late, gate, eye):
    fresh = jnp.concatenate([late[:, :HEAD_DIM], (gate - 1.0) * eye - late[:, HEAD_DIM:]], axis=1)
    if carry is None:
        return fresh
    return gate * carry + fresh - mm(late[:, HEAD_DIM:], carry)


def identity():
    rows, cols = iotas(HEAD_DIM)
    return (rows == cols).astype(f32)


def chain(items, d):
    eye = identity()
    carry = None
    for item in items if d == 0 else items[::-1]:
        carry = follow(carry, item["late"], item["gate"], eye)
    return carry


def chain_groups(groups, d):
    eye = identity()
    carry = None
    for group in groups if d == 0 else groups[::-1]:
        group["before", d] = None if carry is None else carry.astype(bf16)
        carry = follow(carry, group["late"][d], group["gate"][d], eye)
    return carry


def outputs(groups, q_of, o_ref, e_ref):
    for group in groups:
        at, size = group["at"], group["size"]
        plain = q_of(at, size)
        queries = plain.astype(f32)
        q_scale = lax.rsqrt(jnp.sum(queries * queries, axis=1, keepdims=True) + epsilon) * HEAD_DIM**-0.5
        queries = queries * q_scale
        score = jnp.dot(plain, group["plain_t"], preferred_element_type=f32) * q_scale * group["s_row"]
        total = None
        for d in range(2):
            weighed = mm(score * group["decay"][d], group["solved"][d])
            out = weighed[:, :HEAD_DIM]
            early = queries * group["growth"][d] - weighed[:, HEAD_DIM:]
            before = group["before", d]
            if before is not None:
                moved = mm(early, before)
                out = out + moved[:, :HEAD_DIM]
                early = early + moved[:, HEAD_DIM:]
            e_ref[at : at + size, d * HEAD_DIM : (d + 1) * HEAD_DIM] = early.astype(bf16)
            total = out if total is None else total + out
        o_ref[at : at + size, :] = total


def on_mesh(sp=None, tp=None):
    return (lax.axis_index("sp") if sp is None else sp, lax.axis_index("tp") if tp is None else tp)


def send(src, dst, send_sem, recv_sem, device):
    return pltpu.make_async_remote_copy(
        src_ref=src,
        dst_ref=dst,
        send_sem=send_sem,
        recv_sem=recv_sem,
        device_id=device,
        device_id_type=pl.DeviceIdType.MESH,
    )


def greet(devices):
    barrier = pltpu.get_barrier_semaphore()
    for device in devices:
        pl.semaphore_signal(barrier, inc=1, device_id=device, device_id_type=pl.DeviceIdType.MESH)


def split_three(x):
    high = x.astype(bf16)
    rest = x - high.astype(f32)
    mid = rest.astype(bf16)
    low = (rest - mid.astype(f32)).astype(bf16)
    return jnp.concatenate([high, mid, low], axis=1)


def advance(state, move, add):
    high = state.astype(bf16)
    low = (state - high.astype(f32)).astype(bf16)
    both = jnp.concatenate([high, low], axis=0)
    moved = jnp.dot(both, move, preferred_element_type=f32)
    rows = state.shape[0]
    return state + add.astype(f32) + moved[:rows] + moved[rows:]


def mixer_kernel(
    sp, tp, heads, tokens, ctx_tokens,
    cond_hbm, ctx_cond_hbm, gain_hbm, head_gain_hbm, write_bias_hbm, decay_bias_hbm, log_rate_hbm,
    latent_hbm, context_hbm, shift_hbm, scale_hbm, gate_hbm, query_hbm, key_hbm, value_hbm,
    write_hbm, decay_hbm, out_hbm,
    out_ref,
    cond_ref, ctx_cond_ref, gain_ref, head_gain_ref, write_bias_ref, decay_bias_ref, log_rate_ref,
    rows_v, mod_w, q_w, k_w, v_w, gate_w, out_w, st, stats, mod_v, q_v, k_v, v_v, rate_v, run_v, run_t,
    got_p, blocks, gate_row, ctx_state, o_v, e_v, maps_m, maps_b, got_m, got_b, starts, back, got_o, acc,
    load, sent_p, recv_p, sent_t, recv_t, sent_m, recv_m, sent_b, recv_b, sent_s, recv_s,
    sent_o, recv_dn, recv_up, recv_f, recv_c,
):
    me, col = lax.axis_index("sp"), lax.axis_index("tp")
    items = 2 * heads
    quads = sp // items
    split = 2
    part_rows = HEAD_DIM // split
    core = lax.rem(col, 2)
    chips = tp // 2
    chip = col // 2
    partner = col + 1 - 2 * core
    up = lax.rem(chip + 1, chips) * 2 + core
    down = lax.rem(chip + chips - 1, chips) * 2 + core
    far = lax.rem(chip + 2, chips) * 2 + core
    width = mod_w.shape[2]
    half = width // 2
    total_tokens = tokens + ctx_tokens
    side = math.isqrt(sp)
    steps = [(dz, dx) for dz in range(side) for dx in range(side) if dz + dx > 0]
    steps.sort(key=lambda step: -sum(min(d, side - d) for d in step))
    rings = [lax.rem(me // side + dz, side) * side + lax.rem(lax.rem(me, side) + dx, side) for dz, dx in steps]
    near = on_mesh(sp=rings[0])
    cross = [
        lax.rem(col // 2 + dc, tp // 2) * 2 + lax.rem(col + dk, 2)
        for dc in (2, 1, 3, 0)
        for dk in range(2)
        if dc + dk > 0
    ]
    greet([on_mesh(sp=place) for place in rings] + [on_mesh(tp=place) for place in cross])

    def arrived(spot, sem):
        send(spot, spot, sem, sem, near).wait_recv()

    def left(spot, sem):
        send(spot, spot, sem, sem, near).wait_send()

    def fetch(n, src, dst):
        copy = pltpu.make_async_copy(src, dst, load.at[n])
        copy.start()
        return copy

    gates_rows = write_hbm.shape[0]
    mod_loads = [fetch(11, cond_hbm, cond_ref), fetch(12, ctx_cond_hbm, ctx_cond_ref)]
    mod_loads += [fetch(n, src, mod_w.at[n]) for n, src in enumerate((shift_hbm, scale_hbm, gate_hbm))]
    row_loads = [
        fetch(3, latent_hbm, rows_v.at[pl.ds(0, tokens)]),
        fetch(4, context_hbm, rows_v.at[pl.ds(tokens, ctx_tokens)]),
    ]
    weight_loads = [
        fetch(5, key_hbm, k_w),
        fetch(6, value_hbm, v_w),
        fetch(7, write_hbm, gate_w.at[pl.ds(0, gates_rows)]),
        fetch(8, decay_hbm, gate_w.at[pl.ds(gates_rows, gates_rows)]),
        fetch(9, query_hbm, q_w),
    ]
    out_load = fetch(10, out_hbm, out_w)
    small_loads = [
        fetch(13, gain_hbm, gain_ref),
        fetch(14, head_gain_hbm, head_gain_ref),
        fetch(15, write_bias_hbm, write_bias_ref),
        fetch(16, decay_bias_hbm, decay_bias_ref),
        fetch(17, log_rate_hbm, log_rate_ref),
    ]
    for copy in mod_loads:
        copy.wait()

    def silu(ref):
        value = ref[...].astype(f32)
        return value / (1.0 + jnp.exp(-value))

    silus = (silu(cond_ref), silu(ctx_cond_ref))
    quarter = silus[0].shape[0]
    lefts = []
    for part in range(quarter):
        lefts.append(
            jnp.concatenate(
                [silus[0][part : part + 1], silus[1][part : part + 1], jnp.zeros((6, silus[0].shape[1]), f32)], axis=0
            ).astype(bf16)
        )
    silu_rows = jnp.concatenate(lefts, axis=1)
    shift = jnp.dot(silu_rows, mod_w[0], preferred_element_type=f32)
    scale = jnp.dot(silu_rows, mod_w[1], preferred_element_type=f32)
    gate = jnp.dot(silu_rows, mod_w[2], preferred_element_type=f32)
    partial = jnp.concatenate([shift[0:2], scale[0:2], gate[0:1], jnp.zeros((3, width), f32)], axis=0)
    got_p[me] = jnp.concatenate([partial[:, :half], partial[:, half:]], axis=0).astype(bf16)
    pl.semaphore_wait(pltpu.get_barrier_semaphore(), len(rings) + len(cross))
    for place in rings:
        send(got_p.at[me], got_p.at[me], sent_p, recv_p, on_mesh(sp=place)).start()

    gate_w[2 * gates_rows :, :] = jnp.zeros((gate_w.shape[0] - 2 * gates_rows, gate_w.shape[1]), bf16)
    for copy in row_loads + small_loads:
        copy.wait()

    def measure_rows(i, unused):
        at = pl.ds(pl.multiple_of(i * 32, 32), 32)
        values = rows_v[at, :].astype(f32)
        mean = jnp.mean(values * values, axis=1, keepdims=True)
        stats[at, :] = jnp.broadcast_to(lax.rsqrt(mean + epsilon), (32, HEAD_DIM))
        return unused

    lax.fori_loop(0, total_tokens // 32, measure_rows, 0)

    arrived(got_p.at[pl.ds(0, sp - 1)], recv_p)
    total = got_p[0].astype(f32)
    for place in range(1, sp):
        total = total + got_p[place].astype(f32)
    blocks[col] = jnp.concatenate([total[0:4], total[8:12]], axis=0)
    gate_row[...] = jnp.concatenate([total[4:5], total[12:13]], axis=1)
    for place in cross:
        send(blocks.at[col], blocks.at[col], sent_t, recv_t, on_mesh(tp=place)).start()
    arrived(blocks.at[pl.ds(0, tp - 1)], recv_t)
    for place in range(tp):
        at = place * width
        for part in range(2):
            lanes = slice(at + part * half, at + (part + 1) * half)
            four = blocks[place, 4 * part : 4 * part + 4, :]
            scaled = (1.0 + four[2:4]) * gain_ref[:, lanes]
            for which in range(2):
                st[which, :, lanes] = jnp.broadcast_to(four[which : which + 1], (8, half))
                st[2 + which, :, lanes] = jnp.broadcast_to(scaled[which : which + 1], (8, half))

    def modulate(first, count, which):
        def step(i, unused):
            at = pl.ds(pl.multiple_of(first + i * 32, 32), 32)
            root = stats[at, :]
            for lane_at in range(0, rows_v.shape[1], HEAD_DIM):
                lanes = slice(lane_at, lane_at + HEAD_DIM)
                values = rows_v[at, lanes].astype(f32) * root
                shift, scale = st[which, :, lanes], st[2 + which, :, lanes]
                parts = [values[n : n + 8] * scale + shift for n in range(0, 32, 8)]
                mod_v[at, lanes] = jnp.concatenate(parts, axis=0).astype(bf16)
            return unused

        lax.fori_loop(0, count // 32, step, 0)

    modulate(tokens, ctx_tokens, 1)
    modulate(0, tokens, 0)
    for copy in weight_loads:
        copy.wait()
    pre = mm_t(mod_v[...], gate_w[...]).astype(bf16).astype(f32)
    k_v[...] = jnp.dot(mod_v[...], k_w[...], preferred_element_type=f32).astype(bf16)
    v_v[...] = jnp.dot(mod_v[...], v_w[...], preferred_element_type=f32).astype(bf16)

    all_heads = gates_rows // 2
    first_head = col * heads
    pre = pltpu.roll(pre, HEAD_DIM - first_head, 1)
    lane = lax.broadcasted_iota(jnp.int32, (1, HEAD_DIM), 1)
    write_bias = jnp.zeros((1, HEAD_DIM), f32)
    decay_bias = jnp.zeros((1, HEAD_DIM), f32)
    log_rate = jnp.zeros((1, HEAD_DIM), f32)
    for d in range(2):
        for head in range(heads):
            spot = d * all_heads + head
            write_bias = jnp.where(lane == spot, write_bias_ref[d, first_head + head], write_bias)
            decay_bias = jnp.where(lane == spot + gates_rows, decay_bias_ref[d, first_head + head], decay_bias)
            log_rate = jnp.where(lane == spot + gates_rows, log_rate_ref[d, first_head + head], log_rate)
    rate_v[...] = jax.nn.sigmoid(pre + write_bias)
    raised = pre + decay_bias
    soft = jnp.maximum(raised, 0.0) + jnp.log1p(jnp.exp(-jnp.abs(raised)))
    log_decay = -jnp.exp(log_rate) * soft
    lat, ctx = spans(tokens, ctx_tokens)
    for n, (at, size) in enumerate(lat + ctx):
        rows, cols = iotas(size)
        lower = (rows >= cols).astype(f32)
        upper = (rows <= cols).astype(f32)
        sums = jnp.dot(
            jnp.concatenate([lower, upper], axis=0).astype(bf16),
            split_three(log_decay[at : at + size]),
            preferred_element_type=f32,
        )
        sums = sums[:, :HEAD_DIM] + sums[:, HEAD_DIM : 2 * HEAD_DIM] + sums[:, 2 * HEAD_DIM :]
        running = jnp.where(lane < gates_rows + all_heads, sums[:size], sums[size:])
        run_v[at : at + size, :] = running
        run_t[n, :, :size] = running.T

    def group_of(n, at, size, head):
        lanes = slice(head * HEAD_DIM, (head + 1) * HEAD_DIM)
        gates = []
        for d in range(2):
            spot = d * all_heads + head
            deep = spot + gates_rows
            gates.append(
                (
                    rate_v[at : at + size, spot : spot + 1],
                    run_v[at : at + size, deep : deep + 1],
                    run_t[n, deep : deep + 1, :size],
                )
            )
        return dict(
            at=at,
            size=size,
            k=k_v[at : at + size, lanes],
            v=v_v[at : at + size, lanes],
            gates=gates,
        )

    def keep(part, item, carry):
        maps_b[part, item] = carry[:, :HEAD_DIM].T.astype(bf16)
        maps_m[part, item] = carry[:, HEAD_DIM:].T.astype(bf16)

    def owner_of(item, piece):
        return item * quads + 2 * piece + lax.rem(item + core, 2)

    my_item, my_part = me // quads, lax.rem(me, quads) // 2
    owning = lax.rem(me, 2) == lax.rem(my_item + core, 2)
    reverse = lax.rem(my_item, 2)

    def ship(part, item, piece):
        owner = owner_of(item, piece)

        @pl.when(owner != me)
        def _():
            send(
                maps_m.at[part, item], got_m.at[part, me], sent_m.at[part], recv_m.at[part], on_mesh(sp=owner)
            ).start()
            send(
                maps_b.at[part, item, pl.ds(piece * part_rows, part_rows)],
                got_b.at[part, me], sent_b.at[part], recv_b.at[part], on_mesh(sp=owner),
            ).start()

    def ship_head(part, head):
        for item in (2 * head, 2 * head + 1):
            for piece in range(split):
                ship(part, item, piece)

    def keep_own(part):
        got_m[part, me] = maps_m[part, my_item]
        got_b[part, me] = maps_b[part, my_item, pl.ds(pl.multiple_of(my_part * part_rows, part_rows), part_rows), :]

    ctx_groups = []
    for head in range(heads):
        for n, (at, size) in enumerate(ctx):
            ctx_groups.append(group_of(len(lat) + n, at, size, head))
    done = prepare(ctx_groups)
    each = 2 * len(ctx)
    for head in range(heads):
        for d in range(2):
            chosen = [i for i in done[head * each : (head + 1) * each] if i["d"] == d]
            keep(0, 2 * head + d, chain(chosen, d))
    for head in range(heads):
        ship_head(0, head)
    latents = []
    for head in range(heads):
        latents.append([group_of(n, at, size, head) for n, (at, size) in enumerate(lat)])
        solve_groups(latents[head])
        for d in range(2):
            keep(1, 2 * head + d, chain_groups(latents[head], d))
        ship_head(1, head)
    def arrive(part):
        arrived(got_m.at[part, pl.ds(0, sp - 1)], recv_m.at[part])
        arrived(got_b.at[part, pl.ds(0, sp - 1)], recv_b.at[part])

    def give_back(place):
        return send(
            starts.at[place], back.at[my_item * split + my_part], sent_s, recv_s.at[my_item // 2], on_mesh(sp=place)
        )

    def q_of(head):
        lanes = slice(head * HEAD_DIM, (head + 1) * HEAD_DIM)
        return lambda at, size: q_v[at : at + size, lanes]

    def run_chain():
        arrive(1)
        state = ctx_state[...]
        for step in range(sp):
            place = step + reverse * (sp - 1 - 2 * step)
            starts[place] = state.astype(bf16)
            if step < sp - 1:
                state = advance(state, got_m[1, place], got_b[1, place])
        for place in rings:
            give_back(place).start()
        back[my_item * split + my_part] = starts[me]

    q_v[...] = jnp.dot(mod_v[0:tokens, :], q_w[...], preferred_element_type=f32).astype(bf16)
    outputs(latents[0], q_of(0), o_v.at[0], e_v.at[0])

    @pl.when(owning)
    def _():
        keep_own(0)
        keep_own(1)
        arrive(0)
        state = jnp.zeros((part_rows, HEAD_DIM), f32)
        for step in range(sp):
            place = step + reverse * (sp - 1 - 2 * step)
            state = advance(state, got_m[0, place], got_b[0, place])
        ctx_state[...] = state

    for head in range(heads):
        if head > 0:
            outputs(latents[head], q_of(head), o_v.at[head], e_v.at[head])

        @pl.when(owning & (my_item // 2 == head))
        def _():
            run_chain()

    parts = 2
    mid = tokens // parts

    def piece(head, place, part):
        return got_o.at[head, place, pl.ds(part * mid, mid)]

    def to_up(head, part):
        return send(
            piece(head, col, part), piece(head, col, part), sent_o.at[head], recv_dn.at[head, part],
            on_mesh(tp=up),
        )

    def to_down(head, part):
        return send(
            piece(head, col, part), piece(head, col, part), sent_o.at[head], recv_up.at[head, part],
            on_mesh(tp=down),
        )

    def forward(head, part):
        src, dst = (down, up) if part < parts // 2 else (up, down)
        return send(
            piece(head, src, part), piece(head, src, part), sent_o.at[head], recv_f.at[head, part],
            on_mesh(tp=dst),
        )

    def relay(head, n, spot):
        return send(spot, spot, sent_o.at[head], recv_c.at[head, n], on_mesh(tp=partner))

    def finish_head(head):
        half_items = [2 * head, 2 * head + 1]
        mine = owning & (my_item // 2 == head)

        @pl.when(mine)
        def _():
            arrived(back.at[pl.ds(0, 2 * split - 1)], recv_s.at[head])

        @pl.when(jnp.logical_not(mine))
        def _():
            arrived(back.at[pl.ds(0, 2 * split)], recv_s.at[head])

        pair = [back[item * split : (item + 1) * split].reshape(HEAD_DIM, HEAD_DIM) for item in half_items]
        combined = o_v[head] + mm_t(e_v[head], jnp.concatenate(pair, axis=1))
        norm = lax.rsqrt(jnp.mean(combined * combined, axis=1, keepdims=True) + epsilon)
        got_o[head, col] = (combined * norm * head_gain_ref[...]).astype(bf16)
        for part in range(parts):
            to_up(head, part).start()
            to_down(head, parts - 1 - part).start()
        relay(head, 0, got_o.at[head, col]).start()

    def near_arrivals(head):
        waits = []
        for part in range(parts):
            waits.append((down, part, recv_dn, 1, part < parts // 2))
            waits.append((up, parts - 1 - part, recv_up, 2, part < parts // 2))
        for place, part, sems, n, onward in waits:
            spot = piece(head, place, part)
            arrived(spot, sems.at[head, part])
            if onward:
                forward(head, part).start()
            relay(head, n, spot).start()

    def far_arrivals(head):
        for n in range(parts):
            part = n // 2 if n % 2 == 0 else parts - 1 - n // 2
            spot = piece(head, far, part)
            arrived(spot, recv_f.at[head, part])
            relay(head, 3, spot).start()

    def from_partner(head, n):
        arrived(got_o.at[head, 0], recv_c.at[head, n])

    def add(head, place, first=False):
        even = place - core
        lanes = jnp.concatenate([got_o[head, even], got_o[head, even + 1]], axis=1)
        depth = heads * HEAD_DIM
        weights = jnp.concatenate(
            [
                out_w[pl.ds(pl.multiple_of((even + n) * depth + head * HEAD_DIM, HEAD_DIM), HEAD_DIM), :]
                for n in range(2)
            ],
            axis=0,
        )
        part = jnp.dot(lanes, weights, preferred_element_type=f32)
        acc[...] = part if first else acc[...] + part

    out_load.wait()
    for head in range(heads):
        finish_head(head)
    near_arrivals(0)
    for head in range(heads):
        from_partner(head, 0)
        add(head, col, head == 0)
    for head in range(1, heads):
        near_arrivals(head)
    for head in range(heads):
        for n, place in ((1, down), (2, up)):
            from_partner(head, n)
            add(head, place)
        far_arrivals(head)
    for head in range(heads):
        from_partner(head, 3)
        add(head, far)
    lanes = pl.ds(pl.multiple_of(col * width, width), width)
    out_ref[...] = (rows_v[0:tokens, lanes].astype(f32) + gate_row[...] * acc[...]).astype(bf16)
    left(got_p.at[pl.ds(0, sp - 1)], sent_p)
    left(blocks.at[pl.ds(0, tp - 1)], sent_t)

    def sent_maps(count):
        for part in range(2):
            left(got_m.at[part, pl.ds(0, count)], sent_m.at[part])
            left(got_b.at[part, pl.ds(0, count)], sent_b.at[part])

    @pl.when(owning)
    def _():
        sent_maps(items * split - 1)
        left(starts.at[pl.ds(0, sp - 1)], sent_s)

    @pl.when(jnp.logical_not(owning))
    def _():
        sent_maps(items * split)

    for head in range(heads):
        left(got_o.at[head, pl.ds(0, tp - 1)], sent_o.at[head])


def deliver_kernel(src, dst, held, taken, given):
    rows = held.shape[0] // 4
    spots = [pl.ds(n * rows, rows) for n in range(4)]
    takes = [pltpu.make_async_copy(src.at[spot], held.at[spot], taken.at[n]) for n, spot in enumerate(spots)]
    gives = [pltpu.make_async_copy(held.at[spot], dst.at[spot], given.at[n]) for n, spot in enumerate(spots)]
    for take in takes:
        take.start()
    for take, give in zip(takes, gives):
        take.wait()
        give.start()
    for give in gives:
        give.wait()


def body(
    latent,
    context,
    condition,
    context_condition,
    shift_weight,
    scale_weight,
    gate_weight,
    norm_gain,
    query_weight,
    key_weight,
    value_weight,
    write_weight,
    decay_weight,
    write_bias,
    decay_bias,
    log_rate,
    head_gain,
    out_weight,
):
    sp, tp = lax.axis_size("sp"), lax.axis_size("tp")
    inner = query_weight.shape[1]
    heads = inner // HEAD_DIM
    tokens, ctx_tokens = latent.shape[0], context.shape[0]
    total = tokens + ctx_tokens
    features = latent.shape[1]
    width = shift_weight.shape[1]
    items = 2 * heads
    split = 2
    rows = HEAD_DIM // split
    chunks = sum(len(part) for part in spans(tokens, ctx_tokens))
    vmem = pl.BlockSpec(memory_space=pltpu.VMEM)
    anywhere = pl.BlockSpec(memory_space=pltpu.HBM)
    dma = pltpu.SemaphoreType.DMA
    flat = [jnp.transpose(w, (1, 2, 0)).reshape(-1, features) for w in (write_weight, decay_weight)]
    updated = pl.pallas_call(
        functools.partial(mixer_kernel, sp, tp, heads, tokens, ctx_tokens),
        in_specs=[anywhere] * 18,
        out_specs=vmem,
        out_shape=jax.ShapeDtypeStruct((tokens, width), bf16),
        scratch_shapes=[
            pltpu.VMEM((condition.shape[0] // HEAD_DIM, HEAD_DIM), bf16),
            pltpu.VMEM((condition.shape[0] // HEAD_DIM, HEAD_DIM), bf16),
            pltpu.VMEM((1, features), f32),
            pltpu.VMEM((1, HEAD_DIM), f32),
            pltpu.SMEM(write_bias.shape, f32),
            pltpu.SMEM(decay_bias.shape, f32),
            pltpu.SMEM(log_rate.shape, f32),
            pltpu.VMEM((total, features), bf16),
            pltpu.VMEM((3,) + shift_weight.shape, bf16),
            pltpu.VMEM(query_weight.shape, bf16),
            pltpu.VMEM(key_weight.shape, bf16),
            pltpu.VMEM(value_weight.shape, bf16),
            pltpu.VMEM((HEAD_DIM, features), bf16),
            pltpu.VMEM(out_weight.shape, bf16),
            pltpu.VMEM((4, 8, features), f32),
            pltpu.VMEM((total, HEAD_DIM), f32),
            pltpu.VMEM((total, features), bf16),
            pltpu.VMEM((tokens, inner), bf16),
            pltpu.VMEM((total, inner), bf16),
            pltpu.VMEM((total, inner), bf16),
            pltpu.VMEM((total, HEAD_DIM), f32),
            pltpu.VMEM((total, HEAD_DIM), f32),
            pltpu.VMEM((chunks, HEAD_DIM, CHUNK), f32),
            pltpu.VMEM((sp, 16, width // 2), bf16),
            pltpu.VMEM((tp, 8, width // 2), f32),
            pltpu.VMEM((1, width), f32),
            pltpu.VMEM((rows, HEAD_DIM), f32),
            pltpu.VMEM((heads, tokens, HEAD_DIM), f32),
            pltpu.VMEM((heads, tokens, 2 * HEAD_DIM), bf16),
            pltpu.VMEM((2, items, HEAD_DIM, HEAD_DIM), bf16),
            pltpu.VMEM((2, items, HEAD_DIM, HEAD_DIM), bf16),
            pltpu.VMEM((2, sp, HEAD_DIM, HEAD_DIM), bf16),
            pltpu.VMEM((2, sp, rows, HEAD_DIM), bf16),
            pltpu.VMEM((sp, rows, HEAD_DIM), bf16),
            pltpu.VMEM((items * split, rows, HEAD_DIM), bf16),
            pltpu.VMEM((heads, tp, tokens, HEAD_DIM), bf16),
            pltpu.VMEM((tokens, width), f32),
            dma((18,)),
            dma,
            dma,
            dma,
            dma,
            dma((2,)),
            dma((2,)),
            dma((2,)),
            dma((2,)),
            dma,
            dma((heads,)),
            dma((heads,)),
            dma((heads, 2)),
            dma((heads, 2)),
            dma((heads, 2)),
            dma((heads, 4)),
        ],
        compiler_params=pltpu.CompilerParams(
            collective_id=0, has_side_effects=True, vmem_limit_bytes=58 * 1024 * 1024
        ),
        name="mixer",
    )(
        condition.reshape(-1, HEAD_DIM),
        context_condition.reshape(-1, HEAD_DIM),
        norm_gain[None, :],
        head_gain[None, :],
        write_bias,
        decay_bias,
        log_rate,
        latent,
        context,
        shift_weight,
        scale_weight,
        gate_weight,
        query_weight,
        key_weight,
        value_weight,
        flat[0],
        flat[1],
        out_weight,
    )
    return pl.pallas_call(
        deliver_kernel,
        in_specs=[pl.BlockSpec(memory_space=pltpu.HBM)],
        out_specs=pl.BlockSpec(memory_space=pltpu.HBM),
        out_shape=jax.ShapeDtypeStruct((tokens, width), bf16),
        scratch_shapes=[pltpu.VMEM((tokens, width), bf16), dma((4,)), dma((4,))],
        compiler_params=pltpu.CompilerParams(vmem_limit_bytes=58 * 1024 * 1024),
        name="deliver",
    )(updated)


def solution(mesh):
    placed = (
        P("sp", None),
        P("sp", None),
        P("sp"),
        P("sp"),
        P("sp", "tp"),
        P("sp", "tp"),
        P("sp", "tp"),
        P(),
        P(None, "tp"),
        P(None, "tp"),
        P(None, "tp"),
        P(),
        P(),
        P(),
        P(),
        P(),
        P(),
        P(None, "tp"),
    )
    return jax.shard_map(body, mesh=mesh, in_specs=placed, out_specs=P("sp", "tp"), check_vma=False)
```

```python
import functools
import math

import jax
import jax.numpy as jnp
from jax import lax
from jax.experimental import pallas as pl
from jax.experimental.pallas import tpu as pltpu
from jax.sharding import PartitionSpec as P

HEAD_DIM = 128
CHUNK = 128
epsilon = 0.0001
bf16 = jnp.bfloat16
f32 = jnp.float32


def mm(a, b):
    return jnp.dot(a.astype(bf16), b.astype(bf16), preferred_element_type=f32)


def mm_t(a, b):
    return lax.dot_general(a, b, (((1,), (1,)), ((), ())), preferred_element_type=f32)


def spans(tokens, ctx_tokens):
    size = min(CHUNK, tokens)
    lat = [(at, size) for at in range(0, tokens, size)]
    ctx_size = min(CHUNK, ctx_tokens)
    ctx = [(tokens + at, ctx_size) for at in range(0, ctx_tokens, ctx_size)]
    return lat, ctx


def iotas(size):
    rows = lax.broadcasted_iota(jnp.int32, (size, size), 0)
    cols = lax.broadcasted_iota(jnp.int32, (size, size), 1)
    return rows, cols


def prepare(groups):
    items = []
    for group in groups:
        size = group["size"]
        rows, cols = iotas(size)
        keys = group["k"]
        keys_t = keys.astype(f32).T
        gram = jnp.dot(keys, keys_t.astype(bf16), preferred_element_type=f32)
        diag = jnp.where(rows == cols, gram, 0.0)
        s_col = lax.rsqrt(jnp.sum(diag, axis=1, keepdims=True) + epsilon)
        s_row = lax.rsqrt(jnp.sum(diag, axis=0, keepdims=True) + epsilon)
        gram = gram * s_col * s_row
        group["keys"] = keys.astype(f32) * s_col
        group["keys_t"] = keys_t * s_row
        group["values"] = group["v"].astype(f32)
        for d in range(2):
            rate_col, run_col, run_row = group["gates"][d]
            inside = rows >= cols if d == 0 else rows <= cols
            strict = rows > cols if d == 0 else rows < cols
            decay = jnp.where(inside, jnp.exp(jnp.minimum(run_col - run_row, 0.0)), 0.0)
            system = jnp.where(strict, gram * decay * rate_col, 0.0)
            item = dict(group=group, size=size, d=d, rate_col=rate_col, run_col=run_col, run_row=run_row)
            item["system"] = system
            near = (rows // 2) == (cols // 2)
            item["inv"] = jnp.where(rows == cols, 1.0, jnp.where(near, -system, 0.0))
            items.append(item)
    span = 2
    while span < max(item["size"] for item in items):
        firsts = []
        for item in items:
            if span >= item["size"]:
                firsts.append(None)
                continue
            rows, cols = iotas(item["size"])
            rows, cols = rows // span, cols // span
            if item["d"] == 0:
                mask = ((rows % 2) == 1) & (cols == rows - 1)
            else:
                mask = ((cols % 2) == 1) & (rows == cols - 1)
            firsts.append(mm(jnp.where(mask, item["system"], 0.0), item["inv"]))
        for item, first in zip(items, firsts):
            if first is not None:
                item["inv"] = item["inv"] - mm(item["inv"], first)
        span *= 2
    for item in items:
        group = item["group"]
        growth = jnp.exp(item["run_col"])
        both = jnp.concatenate(
            [group["values"] * item["rate_col"], group["keys"] * (item["rate_col"] * growth)], axis=1
        )
        item["solved"] = mm(item["inv"], both)
        last = item["run_row"][:, item["size"] - 1 :] if item["d"] == 0 else item["run_row"][:, :1]
        item["gate"] = jnp.exp(last)
        late_t = group["keys_t"] * jnp.exp(last - item["run_row"])
        item["late"] = mm(late_t, item["solved"])
    return items


def solve_groups(groups):
    size = groups[0]["size"]
    rows, cols = iotas(size)
    near = (rows // 2) == (cols // 2)
    for group in groups:
        keys = group["k"]
        keys_t = keys.astype(f32).T
        group["plain_t"] = keys_t.astype(bf16)
        gram = jnp.dot(keys, group["plain_t"], preferred_element_type=f32)
        diag = jnp.where(rows == cols, gram, 0.0)
        s_col = lax.rsqrt(jnp.sum(diag, axis=1, keepdims=True) + epsilon)
        s_row = lax.rsqrt(jnp.sum(diag, axis=0, keepdims=True) + epsilon)
        gram = gram * s_col * s_row
        group["s_row"] = s_row
        group["keys"] = keys.astype(f32) * s_col
        group["keys_t"] = keys_t * s_row
        group["decay"], group["system"], group["inv"] = [], [], []
        for d in range(2):
            rate_col, run_col, run_row = group["gates"][d]
            inside = rows >= cols if d == 0 else rows <= cols
            strict = rows > cols if d == 0 else rows < cols
            decay = jnp.where(inside, jnp.exp(jnp.minimum(run_col - run_row, 0.0)), 0.0)
            group["decay"].append(decay)
            system = jnp.where(strict, gram * decay * rate_col, 0.0)
            group["system"].append(system.astype(bf16))
            group["inv"].append(jnp.where(rows == cols, 1.0, jnp.where(near, -system, 0.0)))
    span = 2
    while span < size:
        row_block, col_block = rows // span, cols // span
        masks = (
            ((row_block % 2) == 1) & (col_block == row_block - 1),
            ((col_block % 2) == 1) & (row_block == col_block - 1),
        )
        masks = [jnp.where(mask, 1.0, 0.0).astype(bf16) for mask in masks]
        firsts = []
        for group in groups:
            group["packed"] = [inv.astype(bf16) for inv in group["inv"]]
            firsts.append([mm(group["system"][d] * masks[d], group["packed"][d]) for d in range(2)])
        for group, first in zip(groups, firsts):
            group["inv"] = [group["inv"][d] - mm(group["packed"][d], first[d]) for d in range(2)]
        span *= 2
    for group in groups:
        values = group["v"].astype(f32)
        group["growth"], group["solved"], group["late"], group["gate"] = [], [], [], []
        for d in range(2):
            rate_col, run_col, run_row = group["gates"][d]
            growth = jnp.exp(run_col)
            both = jnp.concatenate([values * rate_col, group["keys"] * (rate_col * growth)], axis=1)
            solved = mm(group["inv"][d], both).astype(bf16)
            last = run_row[:, size - 1 :] if d == 0 else run_row[:, :1]
            group["growth"].append(growth)
            group["solved"].append(solved)
            group["gate"].append(jnp.exp(last))
            group["late"].append(mm(group["keys_t"] * jnp.exp(last - run_row), solved))


def follow(carry, late, gate, eye):
    fresh = jnp.concatenate([late[:, :HEAD_DIM], (gate - 1.0) * eye - late[:, HEAD_DIM:]], axis=1)
    if carry is None:
        return fresh
    return gate * carry + fresh - mm(late[:, HEAD_DIM:], carry)


def identity():
    rows, cols = iotas(HEAD_DIM)
    return (rows == cols).astype(f32)


def chain(items, d):
    eye = identity()
    carry = None
    for item in items if d == 0 else items[::-1]:
        carry = follow(carry, item["late"], item["gate"], eye)
    return carry


def chain_groups(groups, d):
    eye = identity()
    carry = None
    for group in groups if d == 0 else groups[::-1]:
        group["before", d] = None if carry is None else carry.astype(bf16)
        carry = follow(carry, group["late"][d], group["gate"][d], eye)
    return carry


def outputs(groups, q_of, o_ref, e_ref):
    for group in groups:
        at, size = group["at"], group["size"]
        plain = q_of(at, size)
        queries = plain.astype(f32)
        q_scale = lax.rsqrt(jnp.sum(queries * queries, axis=1, keepdims=True) + epsilon) * HEAD_DIM**-0.5
        queries = queries * q_scale
        score = jnp.dot(plain, group["plain_t"], preferred_element_type=f32) * q_scale * group["s_row"]
        total = None
        for d in range(2):
            weighed = mm(score * group["decay"][d], group["solved"][d])
            out = weighed[:, :HEAD_DIM]
            early = queries * group["growth"][d] - weighed[:, HEAD_DIM:]
            before = group["before", d]
            if before is not None:
                moved = mm(early, before)
                out = out + moved[:, :HEAD_DIM]
                early = early + moved[:, HEAD_DIM:]
            e_ref[at : at + size, d * HEAD_DIM : (d + 1) * HEAD_DIM] = early.astype(bf16)
            total = out if total is None else total + out
        o_ref[at : at + size, :] = total


def on_mesh(sp=None, tp=None):
    return (lax.axis_index("sp") if sp is None else sp, lax.axis_index("tp") if tp is None else tp)


def send(src, dst, send_sem, recv_sem, device):
    return pltpu.make_async_remote_copy(
        src_ref=src,
        dst_ref=dst,
        send_sem=send_sem,
        recv_sem=recv_sem,
        device_id=device,
        device_id_type=pl.DeviceIdType.MESH,
    )


def greet(devices):
    barrier = pltpu.get_barrier_semaphore()
    for device in devices:
        pl.semaphore_signal(barrier, inc=1, device_id=device, device_id_type=pl.DeviceIdType.MESH)


def split_three(x):
    high = x.astype(bf16)
    rest = x - high.astype(f32)
    mid = rest.astype(bf16)
    low = (rest - mid.astype(f32)).astype(bf16)
    return jnp.concatenate([high, mid, low], axis=1)


def advance(state, move, add):
    high = state.astype(bf16)
    low = (state - high.astype(f32)).astype(bf16)
    both = jnp.concatenate([high, low], axis=0)
    moved = jnp.dot(both, move, preferred_element_type=f32)
    rows = state.shape[0]
    return state + add.astype(f32) + moved[:rows] + moved[rows:]


def mixer_kernel(
    sp, tp, heads, tokens, ctx_tokens,
    cond_hbm, ctx_cond_hbm, gain_hbm, head_gain_hbm, write_bias_hbm, decay_bias_hbm, log_rate_hbm,
    latent_hbm, context_hbm, shift_hbm, scale_hbm, gate_hbm, query_hbm, key_hbm, value_hbm,
    write_hbm, decay_hbm, out_hbm,
    out_ref,
    cond_ref, ctx_cond_ref, gain_ref, head_gain_ref, write_bias_ref, decay_bias_ref, log_rate_ref,
    rows_v, mod_w, q_w, k_w, v_w, gate_w, out_w, st, stats, mod_v, q_v, k_v, v_v, rate_v, run_v, run_t,
    got_p, blocks, gate_row, ctx_state, o_v, e_v, maps_m, maps_b, got_m, got_b, starts, back, got_o, acc,
    load, sent_p, recv_p, sent_t, recv_t, sent_m, recv_m, sent_b, recv_b, sent_s, recv_s,
    sent_o, recv_dn, recv_up, recv_f, recv_c,
):
    me, col = lax.axis_index("sp"), lax.axis_index("tp")
    items = 2 * heads
    quads = sp // items
    split = 2
    part_rows = HEAD_DIM // split
    core = lax.rem(col, 2)
    chips = tp // 2
    chip = col // 2
    partner = col + 1 - 2 * core
    up = lax.rem(chip + 1, chips) * 2 + core
    down = lax.rem(chip + chips - 1, chips) * 2 + core
    far = lax.rem(chip + 2, chips) * 2 + core
    width = mod_w.shape[2]
    half = width // 2
    total_tokens = tokens + ctx_tokens
    side = math.isqrt(sp)
    steps = [(dz, dx) for dz in range(side) for dx in range(side) if dz + dx > 0]
    steps.sort(key=lambda step: -sum(min(d, side - d) for d in step))
    rings = [lax.rem(me // side + dz, side) * side + lax.rem(lax.rem(me, side) + dx, side) for dz, dx in steps]
    near = on_mesh(sp=rings[0])
    cross = [
        lax.rem(col // 2 + dc, tp // 2) * 2 + lax.rem(col + dk, 2)
        for dc in (2, 1, 3, 0)
        for dk in range(2)
        if dc + dk > 0
    ]
    greet([on_mesh(sp=place) for place in rings] + [on_mesh(tp=place) for place in cross])

    def arrived(spot, sem):
        send(spot, spot, sem, sem, near).wait_recv()

    def left(spot, sem):
        send(spot, spot, sem, sem, near).wait_send()

    def fetch(n, src, dst):
        copy = pltpu.make_async_copy(src, dst, load.at[n])
        copy.start()
        return copy

    gates_rows = write_hbm.shape[0]
    mod_loads = [fetch(11, cond_hbm, cond_ref), fetch(12, ctx_cond_hbm, ctx_cond_ref)]
    mod_loads += [fetch(n, src, mod_w.at[n]) for n, src in enumerate((shift_hbm, scale_hbm, gate_hbm))]
    row_loads = [
        fetch(3, latent_hbm, rows_v.at[pl.ds(0, tokens)]),
        fetch(4, context_hbm, rows_v.at[pl.ds(tokens, ctx_tokens)]),
    ]
    weight_loads = [
        fetch(5, key_hbm, k_w),
        fetch(6, value_hbm, v_w),
        fetch(7, write_hbm, gate_w.at[pl.ds(0, gates_rows)]),
        fetch(8, decay_hbm, gate_w.at[pl.ds(gates_rows, gates_rows)]),
        fetch(9, query_hbm, q_w),
    ]
    out_load = fetch(10, out_hbm, out_w)
    small_loads = [
        fetch(13, gain_hbm, gain_ref),
        fetch(14, head_gain_hbm, head_gain_ref),
        fetch(15, write_bias_hbm, write_bias_ref),
        fetch(16, decay_bias_hbm, decay_bias_ref),
        fetch(17, log_rate_hbm, log_rate_ref),
    ]
    for copy in mod_loads:
        copy.wait()

    def silu(ref):
        value = ref[...].astype(f32)
        return value / (1.0 + jnp.exp(-value))

    silus = (silu(cond_ref), silu(ctx_cond_ref))
    quarter = silus[0].shape[0]
    lefts = []
    for part in range(quarter):
        lefts.append(
            jnp.concatenate(
                [silus[0][part : part + 1], silus[1][part : part + 1], jnp.zeros((6, silus[0].shape[1]), f32)], axis=0
            ).astype(bf16)
        )
    silu_rows = jnp.concatenate(lefts, axis=1)
    shift = jnp.dot(silu_rows, mod_w[0], preferred_element_type=f32)
    scale = jnp.dot(silu_rows, mod_w[1], preferred_element_type=f32)
    gate = jnp.dot(silu_rows, mod_w[2], preferred_element_type=f32)
    partial = jnp.concatenate([shift[0:2], scale[0:2], gate[0:1], jnp.zeros((3, width), f32)], axis=0)
    got_p[me] = jnp.concatenate([partial[:, :half], partial[:, half:]], axis=0).astype(bf16)
    pl.semaphore_wait(pltpu.get_barrier_semaphore(), len(rings) + len(cross))
    for place in rings:
        send(got_p.at[me], got_p.at[me], sent_p, recv_p, on_mesh(sp=place)).start()

    gate_w[2 * gates_rows :, :] = jnp.zeros((gate_w.shape[0] - 2 * gates_rows, gate_w.shape[1]), bf16)
    for copy in row_loads + small_loads:
        copy.wait()

    def measure_rows(i, unused):
        at = pl.ds(pl.multiple_of(i * 32, 32), 32)
        values = rows_v[at, :].astype(f32)
        mean = jnp.mean(values * values, axis=1, keepdims=True)
        stats[at, :] = jnp.broadcast_to(lax.rsqrt(mean + epsilon), (32, HEAD_DIM))
        return unused

    lax.fori_loop(0, total_tokens // 32, measure_rows, 0)

    arrived(got_p.at[pl.ds(0, sp - 1)], recv_p)
    total = got_p[0].astype(f32)
    for place in range(1, sp):
        total = total + got_p[place].astype(f32)
    blocks[col] = jnp.concatenate([total[0:4], total[8:12]], axis=0)
    gate_row[...] = jnp.concatenate([total[4:5], total[12:13]], axis=1)
    for place in cross:
        send(blocks.at[col], blocks.at[col], sent_t, recv_t, on_mesh(tp=place)).start()
    arrived(blocks.at[pl.ds(0, tp - 1)], recv_t)
    for place in range(tp):
        at = place * width
        for part in range(2):
            lanes = slice(at + part * half, at + (part + 1) * half)
            four = blocks[place, 4 * part : 4 * part + 4, :]
            scaled = (1.0 + four[2:4]) * gain_ref[:, lanes]
            for which in range(2):
                st[which, :, lanes] = jnp.broadcast_to(four[which : which + 1], (8, half))
                st[2 + which, :, lanes] = jnp.broadcast_to(scaled[which : which + 1], (8, half))

    def modulate(first, count, which):
        def step(i, unused):
            at = pl.ds(pl.multiple_of(first + i * 32, 32), 32)
            root = stats[at, :]
            for lane_at in range(0, rows_v.shape[1], HEAD_DIM):
                lanes = slice(lane_at, lane_at + HEAD_DIM)
                values = rows_v[at, lanes].astype(f32) * root
                shift, scale = st[which, :, lanes], st[2 + which, :, lanes]
                parts = [values[n : n + 8] * scale + shift for n in range(0, 32, 8)]
                mod_v[at, lanes] = jnp.concatenate(parts, axis=0).astype(bf16)
            return unused

        lax.fori_loop(0, count // 32, step, 0)

    modulate(tokens, ctx_tokens, 1)
    modulate(0, tokens, 0)
    for copy in weight_loads:
        copy.wait()
    pre = mm_t(mod_v[...], gate_w[...]).astype(bf16).astype(f32)
    k_v[...] = jnp.dot(mod_v[...], k_w[...], preferred_element_type=f32).astype(bf16)
    v_v[...] = jnp.dot(mod_v[...], v_w[...], preferred_element_type=f32).astype(bf16)

    all_heads = gates_rows // 2
    first_head = col * heads
    pre = pltpu.roll(pre, HEAD_DIM - first_head, 1)
    lane = lax.broadcasted_iota(jnp.int32, (1, HEAD_DIM), 1)
    write_bias = jnp.zeros((1, HEAD_DIM), f32)
    decay_bias = jnp.zeros((1, HEAD_DIM), f32)
    log_rate = jnp.zeros((1, HEAD_DIM), f32)
    for d in range(2):
        for head in range(heads):
            spot = d * all_heads + head
            write_bias = jnp.where(lane == spot, write_bias_ref[d, first_head + head], write_bias)
            decay_bias = jnp.where(lane == spot + gates_rows, decay_bias_ref[d, first_head + head], decay_bias)
            log_rate = jnp.where(lane == spot + gates_rows, log_rate_ref[d, first_head + head], log_rate)
    rate_v[...] = jax.nn.sigmoid(pre + write_bias)
    raised = pre + decay_bias
    soft = jnp.maximum(raised, 0.0) + jnp.log1p(jnp.exp(-jnp.abs(raised)))
    log_decay = -jnp.exp(log_rate) * soft
    lat, ctx = spans(tokens, ctx_tokens)
    for n, (at, size) in enumerate(lat + ctx):
        rows, cols = iotas(size)
        lower = (rows >= cols).astype(f32)
        upper = (rows <= cols).astype(f32)
        sums = jnp.dot(
            jnp.concatenate([lower, upper], axis=0).astype(bf16),
            split_three(log_decay[at : at + size]),
            preferred_element_type=f32,
        )
        sums = sums[:, :HEAD_DIM] + sums[:, HEAD_DIM : 2 * HEAD_DIM] + sums[:, 2 * HEAD_DIM :]
        running = jnp.where(lane < gates_rows + all_heads, sums[:size], sums[size:])
        run_v[at : at + size, :] = running
        run_t[n, :, :size] = running.T

    def group_of(n, at, size, head):
        lanes = slice(head * HEAD_DIM, (head + 1) * HEAD_DIM)
        gates = []
        for d in range(2):
            spot = d * all_heads + head
            deep = spot + gates_rows
            gates.append(
                (
                    rate_v[at : at + size, spot : spot + 1],
                    run_v[at : at + size, deep : deep + 1],
                    run_t[n, deep : deep + 1, :size],
                )
            )
        return dict(
            at=at,
            size=size,
            k=k_v[at : at + size, lanes],
            v=v_v[at : at + size, lanes],
            gates=gates,
        )

    def keep(part, item, carry):
        maps_b[part, item] = carry[:, :HEAD_DIM].T.astype(bf16)
        maps_m[part, item] = carry[:, HEAD_DIM:].T.astype(bf16)

    def owner_of(item, piece):
        return item * quads + 2 * piece + lax.rem(item + core, 2)

    my_item, my_part = me // quads, lax.rem(me, quads) // 2
    owning = lax.rem(me, 2) == lax.rem(my_item + core, 2)
    reverse = lax.rem(my_item, 2)

    def ship(part, item, piece):
        owner = owner_of(item, piece)

        @pl.when(owner != me)
        def _():
            send(
                maps_m.at[part, item], got_m.at[part, me], sent_m.at[part], recv_m.at[part], on_mesh(sp=owner)
            ).start()
            send(
                maps_b.at[part, item, pl.ds(piece * part_rows, part_rows)],
                got_b.at[part, me], sent_b.at[part], recv_b.at[part], on_mesh(sp=owner),
            ).start()

    def ship_head(part, head):
        for item in (2 * head, 2 * head + 1):
            for piece in range(split):
                ship(part, item, piece)

    def keep_own(part):
        got_m[part, me] = maps_m[part, my_item]
        got_b[part, me] = maps_b[part, my_item, pl.ds(pl.multiple_of(my_part * part_rows, part_rows), part_rows), :]

    ctx_groups = []
    for head in range(heads):
        for n, (at, size) in enumerate(ctx):
            ctx_groups.append(group_of(len(lat) + n, at, size, head))
    done = prepare(ctx_groups)
    each = 2 * len(ctx)
    for head in range(heads):
        for d in range(2):
            chosen = [i for i in done[head * each : (head + 1) * each] if i["d"] == d]
            keep(0, 2 * head + d, chain(chosen, d))
    for head in range(heads):
        ship_head(0, head)
    latents = []
    for head in range(heads):
        latents.append([group_of(n, at, size, head) for n, (at, size) in enumerate(lat)])
        solve_groups(latents[head])
        for d in range(2):
            keep(1, 2 * head + d, chain_groups(latents[head], d))
        ship_head(1, head)
    def arrive(part):
        arrived(got_m.at[part, pl.ds(0, sp - 1)], recv_m.at[part])
        arrived(got_b.at[part, pl.ds(0, sp - 1)], recv_b.at[part])

    def give_back(place):
        return send(
            starts.at[place], back.at[my_item * split + my_part], sent_s, recv_s.at[my_item // 2], on_mesh(sp=place)
        )

    def q_of(head):
        lanes = slice(head * HEAD_DIM, (head + 1) * HEAD_DIM)
        return lambda at, size: q_v[at : at + size, lanes]

    def run_chain():
        arrive(1)
        state = ctx_state[...]
        for step in range(sp):
            place = step + reverse * (sp - 1 - 2 * step)
            starts[place] = state.astype(bf16)
            if step < sp - 1:
                state = advance(state, got_m[1, place], got_b[1, place])
        for place in rings:
            give_back(place).start()
        back[my_item * split + my_part] = starts[me]

    q_v[...] = jnp.dot(mod_v[0:tokens, :], q_w[...], preferred_element_type=f32).astype(bf16)
    outputs(latents[0], q_of(0), o_v.at[0], e_v.at[0])

    @pl.when(owning)
    def _():
        keep_own(0)
        keep_own(1)
        arrive(0)
        state = jnp.zeros((part_rows, HEAD_DIM), f32)
        for step in range(sp):
            place = step + reverse * (sp - 1 - 2 * step)
            state = advance(state, got_m[0, place], got_b[0, place])
        ctx_state[...] = state

    for head in range(heads):
        if head > 0:
            outputs(latents[head], q_of(head), o_v.at[head], e_v.at[head])

        @pl.when(owning & (my_item // 2 == head))
        def _():
            run_chain()

    parts = 2
    mid = tokens // parts

    def piece(head, place, part):
        return got_o.at[head, place, pl.ds(part * mid, mid)]

    def to_up(head, part):
        return send(
            piece(head, col, part), piece(head, col, part), sent_o.at[head], recv_dn.at[head, part],
            on_mesh(tp=up),
        )

    def to_down(head, part):
        return send(
            piece(head, col, part), piece(head, col, part), sent_o.at[head], recv_up.at[head, part],
            on_mesh(tp=down),
        )

    def forward(head, part):
        src, dst = (down, up) if part < parts // 2 else (up, down)
        return send(
            piece(head, src, part), piece(head, src, part), sent_o.at[head], recv_f.at[head, part],
            on_mesh(tp=dst),
        )

    def relay(head, n, spot):
        return send(spot, spot, sent_o.at[head], recv_c.at[head, n], on_mesh(tp=partner))

    def finish_head(head):
        half_items = [2 * head, 2 * head + 1]
        mine = owning & (my_item // 2 == head)

        @pl.when(mine)
        def _():
            arrived(back.at[pl.ds(0, 2 * split - 1)], recv_s.at[head])

        @pl.when(jnp.logical_not(mine))
        def _():
            arrived(back.at[pl.ds(0, 2 * split)], recv_s.at[head])

        pair = [back[item * split : (item + 1) * split].reshape(HEAD_DIM, HEAD_DIM) for item in half_items]
        combined = o_v[head] + mm_t(e_v[head], jnp.concatenate(pair, axis=1))
        norm = lax.rsqrt(jnp.mean(combined * combined, axis=1, keepdims=True) + epsilon)
        got_o[head, col] = (combined * norm * head_gain_ref[...]).astype(bf16)
        for part in range(parts):
            to_up(head, part).start()
            to_down(head, parts - 1 - part).start()
        relay(head, 0, got_o.at[head, col]).start()

    def near_arrivals(head):
        waits = []
        for part in range(parts):
            waits.append((down, part, recv_dn, 1, part < parts // 2))
            waits.append((up, parts - 1 - part, recv_up, 2, part < parts // 2))
        for place, part, sems, n, onward in waits:
            spot = piece(head, place, part)
            arrived(spot, sems.at[head, part])
            if onward:
                forward(head, part).start()
            relay(head, n, spot).start()

    def far_arrivals(head):
        for n in range(parts):
            part = n
            spot = piece(head, far, part)
            arrived(spot, recv_f.at[head, part])
            relay(head, 3 + n // (parts // 2), spot).start()

    def from_partner(head, n):
        arrived(got_o.at[head, 0], recv_c.at[head, n])

    def product(head, place, rows):
        even = place - core
        lanes = jnp.concatenate([got_o[head, even, rows, :], got_o[head, even + 1, rows, :]], axis=1)
        depth = heads * HEAD_DIM
        weights = jnp.concatenate(
            [
                out_w[pl.ds(pl.multiple_of((even + n) * depth + head * HEAD_DIM, HEAD_DIM), HEAD_DIM), :]
                for n in range(2)
            ],
            axis=0,
        )
        return jnp.dot(lanes, weights, preferred_element_type=f32)

    def add(head, place, first=False):
        part = product(head, place, slice(0, tokens))
        acc[...] = part if first else acc[...] + part

    out_load.wait()
    for head in range(heads):
        finish_head(head)
    near_arrivals(0)
    for head in range(heads):
        from_partner(head, 0)
        add(head, col, head == 0)
    for head in range(1, heads):
        near_arrivals(head)
    for head in range(heads):
        for n, place in ((1, down), (2, up)):
            from_partner(head, n)
            add(head, place)
        far_arrivals(head)
    for head in range(heads - 1):
        for n in range(parts):
            arrived(piece(head, 0, 0), recv_c.at[head, 3 + n])
        add(head, far)
    lanes = pl.ds(pl.multiple_of(col * width, width), width)
    for n in range(parts):
        arrived(piece(heads - 1, 0, 0), recv_c.at[heads - 1, 3 + n])
        rows = slice(n * mid, (n + 1) * mid)
        part = acc[rows, :] + product(heads - 1, far, rows)
        out_ref[rows, :] = (rows_v[rows, lanes].astype(f32) + gate_row[...] * part).astype(bf16)
    left(got_p.at[pl.ds(0, sp - 1)], sent_p)
    left(blocks.at[pl.ds(0, tp - 1)], sent_t)

    def sent_maps(count):
        for part in range(2):
            left(got_m.at[part, pl.ds(0, count)], sent_m.at[part])
            left(got_b.at[part, pl.ds(0, count)], sent_b.at[part])

    @pl.when(owning)
    def _():
        sent_maps(items * split - 1)
        left(starts.at[pl.ds(0, sp - 1)], sent_s)

    @pl.when(jnp.logical_not(owning))
    def _():
        sent_maps(items * split)

    for head in range(heads):
        left(got_o.at[head, pl.ds(0, tp - 1)], sent_o.at[head])


def deliver_kernel(src, dst, held, taken, given):
    rows = held.shape[0] // 4
    spots = [pl.ds(n * rows, rows) for n in range(4)]
    takes = [pltpu.make_async_copy(src.at[spot], held.at[spot], taken.at[n]) for n, spot in enumerate(spots)]
    gives = [pltpu.make_async_copy(held.at[spot], dst.at[spot], given.at[n]) for n, spot in enumerate(spots)]
    for take in takes:
        take.start()
    for take, give in zip(takes, gives):
        take.wait()
        give.start()
    for give in gives:
        give.wait()


def body(
    latent,
    context,
    condition,
    context_condition,
    shift_weight,
    scale_weight,
    gate_weight,
    norm_gain,
    query_weight,
    key_weight,
    value_weight,
    write_weight,
    decay_weight,
    write_bias,
    decay_bias,
    log_rate,
    head_gain,
    out_weight,
):
    sp, tp = lax.axis_size("sp"), lax.axis_size("tp")
    inner = query_weight.shape[1]
    heads = inner // HEAD_DIM
    tokens, ctx_tokens = latent.shape[0], context.shape[0]
    total = tokens + ctx_tokens
    features = latent.shape[1]
    width = shift_weight.shape[1]
    items = 2 * heads
    split = 2
    rows = HEAD_DIM // split
    chunks = sum(len(part) for part in spans(tokens, ctx_tokens))
    vmem = pl.BlockSpec(memory_space=pltpu.VMEM)
    anywhere = pl.BlockSpec(memory_space=pltpu.HBM)
    dma = pltpu.SemaphoreType.DMA
    flat = [jnp.transpose(w, (1, 2, 0)).reshape(-1, features) for w in (write_weight, decay_weight)]
    updated = pl.pallas_call(
        functools.partial(mixer_kernel, sp, tp, heads, tokens, ctx_tokens),
        in_specs=[anywhere] * 18,
        out_specs=vmem,
        out_shape=jax.ShapeDtypeStruct((tokens, width), bf16),
        scratch_shapes=[
            pltpu.VMEM((condition.shape[0] // HEAD_DIM, HEAD_DIM), bf16),
            pltpu.VMEM((condition.shape[0] // HEAD_DIM, HEAD_DIM), bf16),
            pltpu.VMEM((1, features), f32),
            pltpu.VMEM((1, HEAD_DIM), f32),
            pltpu.SMEM(write_bias.shape, f32),
            pltpu.SMEM(decay_bias.shape, f32),
            pltpu.SMEM(log_rate.shape, f32),
            pltpu.VMEM((total, features), bf16),
            pltpu.VMEM((3,) + shift_weight.shape, bf16),
            pltpu.VMEM(query_weight.shape, bf16),
            pltpu.VMEM(key_weight.shape, bf16),
            pltpu.VMEM(value_weight.shape, bf16),
            pltpu.VMEM((HEAD_DIM, features), bf16),
            pltpu.VMEM(out_weight.shape, bf16),
            pltpu.VMEM((4, 8, features), f32),
            pltpu.VMEM((total, HEAD_DIM), f32),
            pltpu.VMEM((total, features), bf16),
            pltpu.VMEM((tokens, inner), bf16),
            pltpu.VMEM((total, inner), bf16),
            pltpu.VMEM((total, inner), bf16),
            pltpu.VMEM((total, HEAD_DIM), f32),
            pltpu.VMEM((total, HEAD_DIM), f32),
            pltpu.VMEM((chunks, HEAD_DIM, CHUNK), f32),
            pltpu.VMEM((sp, 16, width // 2), bf16),
            pltpu.VMEM((tp, 8, width // 2), f32),
            pltpu.VMEM((1, width), f32),
            pltpu.VMEM((rows, HEAD_DIM), f32),
            pltpu.VMEM((heads, tokens, HEAD_DIM), f32),
            pltpu.VMEM((heads, tokens, 2 * HEAD_DIM), bf16),
            pltpu.VMEM((2, items, HEAD_DIM, HEAD_DIM), bf16),
            pltpu.VMEM((2, items, HEAD_DIM, HEAD_DIM), bf16),
            pltpu.VMEM((2, sp, HEAD_DIM, HEAD_DIM), bf16),
            pltpu.VMEM((2, sp, rows, HEAD_DIM), bf16),
            pltpu.VMEM((sp, rows, HEAD_DIM), bf16),
            pltpu.VMEM((items * split, rows, HEAD_DIM), bf16),
            pltpu.VMEM((heads, tp, tokens, HEAD_DIM), bf16),
            pltpu.VMEM((tokens, width), f32),
            dma((18,)),
            dma,
            dma,
            dma,
            dma,
            dma((2,)),
            dma((2,)),
            dma((2,)),
            dma((2,)),
            dma,
            dma((heads,)),
            dma((heads,)),
            dma((heads, 2)),
            dma((heads, 2)),
            dma((heads, 2)),
            dma((heads, 5)),
        ],
        compiler_params=pltpu.CompilerParams(
            collective_id=0, has_side_effects=True, vmem_limit_bytes=58 * 1024 * 1024
        ),
        name="mixer",
    )(
        condition.reshape(-1, HEAD_DIM),
        context_condition.reshape(-1, HEAD_DIM),
        norm_gain[None, :],
        head_gain[None, :],
        write_bias,
        decay_bias,
        log_rate,
        latent,
        context,
        shift_weight,
        scale_weight,
        gate_weight,
        query_weight,
        key_weight,
        value_weight,
        flat[0],
        flat[1],
        out_weight,
    )
    return pl.pallas_call(
        deliver_kernel,
        in_specs=[pl.BlockSpec(memory_space=pltpu.HBM)],
        out_specs=pl.BlockSpec(memory_space=pltpu.HBM),
        out_shape=jax.ShapeDtypeStruct((tokens, width), bf16),
        scratch_shapes=[pltpu.VMEM((tokens, width), bf16), dma((4,)), dma((4,))],
        compiler_params=pltpu.CompilerParams(vmem_limit_bytes=58 * 1024 * 1024),
        name="deliver",
    )(updated)


def solution(mesh):
    placed = (
        P("sp", None),
        P("sp", None),
        P("sp"),
        P("sp"),
        P("sp", "tp"),
        P("sp", "tp"),
        P("sp", "tp"),
        P(),
        P(None, "tp"),
        P(None, "tp"),
        P(None, "tp"),
        P(),
        P(),
        P(),
        P(),
        P(),
        P(),
        P(None, "tp"),
    )
    return jax.shard_map(body, mesh=mesh, in_specs=placed, out_specs=P("sp", "tp"), check_vma=False)
```
